32 devices in a mesh: rep: 2 (over x), fs: 8 (over z, y), tp: 2 (over core).
Axes of the slice: x: 2, y: 2, z: 4, core: 2. Of those that a mesh axis runs over, the one named last changes fastest.
Arguments:
- tokens: bfloat16 [16, 384, 2048], P(('rep', 'fs')), may hold values from -6 to 6
- mix_gain: float32 [2048], replicated, may hold values from 0.1 to 1.9
- value_weight: float32 [2048, 2048], P('fs', 'tp'), may hold values from -0.125 to 0.125
- value_scale: float32 [2048], P(('tp', 'fs')), may hold values from 0.5 to 2
- inner_weight: float32 [2048, 2048], P('fs', 'tp'), may hold values from -0.125 to 0.125
- inner_scale: float32 [2048], P(('tp', 'fs')), may hold values from 0.5 to 2
- outer_weight: float32 [2048, 2048], P('fs', 'tp'), may hold values from -0.125 to 0.125
- outer_scale: float32 [2048], P(('tp', 'fs')), may hold values from 0.5 to 2
- conv_taps: float32 [3, 2048], P(None, 'tp'), may hold values from -3 to 3
- out_weight: float32 [2048, 2048], P('tp', 'fs'), may hold values from -0.125 to 0.125
- out_scale: float32 [2048], P('fs'), may hold values from 0.5 to 2
- mlp_gain: float32 [2048], replicated, may hold values from 0.1 to 1.9
- up_weight: float32 [2048, 6144], P('fs', 'tp'), may hold values from -0.125 to 0.125
- up_scale: float32 [6144], P(('tp', 'fs')), may hold values from 0.5 to 2
- down_weight: float32 [6144, 2048], P('tp', 'fs'), may hold values from -0.078125 to 0.078125
- down_scale: float32 [2048], P('fs'), may hold values from 0.5 to 2
Outputs:
- layer_out: bfloat16 [16, 384, 2048], P(('rep', 'fs'))
The draws below stay inside these ranges and needn't reach their ends.
All inputs are finite; a program needn't handle non-finite values.
Results may differ from the reference program's by a relative error of at most 0.02.
Values may be sent and summed in bfloat16 or wider, within the bound.
A program may use at most 128 MiB of HBM per device.

```python
import math
import jax
import jax.numpy as jnp
from jax import lax

D = 2048
FF = 6144
TOK_DEV = 384
SEQS = 16
N_TP = 2


def block_scale(rng, dims, shards, low, high):
    def one(axis_at, shards_of):
        heights = jax.random.uniform(jax.random.fold_in(jax.random.fold_in(rng, 6), axis_at), (shards_of,), jnp.float32, low / len(shards), high / len(shards))
        return jnp.repeat(jnp.exp(heights), dims[axis_at] // shards_of).reshape((-1,) + (1,) * (len(dims) - axis_at - 1))

    level = one(*shards[0])
    for cut in shards[1:]:
        level = level * one(*cut)
    return level


def scatter_about(key, shape, scale, limit, cuts=(), kind=jnp.bfloat16):
    values = scale * jax.random.normal(key, shape, jnp.float32)
    if cuts:
        values = values * block_scale(key, shape, cuts, -0.22, 0.18)
    return jnp.clip(values, -limit, limit).astype(kind)


def setup_inputs(seed: int = 0) -> dict:
    key_of = jax.random.split(jax.random.key(seed), 17)
    return {
        "tokens": scatter_about(key_of[0], (SEQS, TOK_DEV, D), 1.0, 6.0, ((0, 16),)),
        "mix_gain": jnp.clip(1.0 + 0.18 * jax.random.normal(key_of[1], (D,), jnp.float32), 0.1, 1.9),
        "value_weight": scatter_about(key_of[2], (D, D), D ** -0.5, 0.125, ((0, 8), (1, 2)), jnp.float32),
        "value_scale": jnp.clip(jnp.exp(math.log(2.0) - 1.3862944 * jax.random.uniform(key_of[3], (D,), jnp.float32) ** block_scale(key_of[3], (D,), ((0, 16),), -0.2, 0.2)), 0.5, 2.0),
        "inner_weight": scatter_about(key_of[4], (D, D), D ** -0.5, 0.125, ((0, 8), (1, 2)), jnp.float32),
        "inner_scale": jnp.clip(jnp.exp(math.log(2.0) - 1.3862944 * jax.random.uniform(key_of[5], (D,), jnp.float32) ** block_scale(key_of[5], (D,), ((0, 16),), -0.2, 0.2)), 0.5, 2.0),
        "outer_weight": scatter_about(key_of[6], (D, D), D ** -0.5, 0.125, ((0, 8), (1, 2)), jnp.float32),
        "outer_scale": jnp.clip(jnp.exp(math.log(2.0) - 1.3862944 * jax.random.uniform(key_of[7], (D,), jnp.float32) ** block_scale(key_of[7], (D,), ((0, 16),), -0.2, 0.2)), 0.5, 2.0),
        "conv_taps": scatter_about(key_of[8], (3, D), 0.6, 3.0, ((1, 2),), jnp.float32),
        "out_weight": scatter_about(key_of[9], (D, D), D ** -0.5, 0.125, ((0, 2), (1, 8)), jnp.float32),
        "out_scale": jnp.clip(jnp.exp(math.log(2.0) - 1.3862944 * jax.random.uniform(key_of[10], (D,), jnp.float32) ** block_scale(key_of[10], (D,), ((0, 8),), -0.2, 0.2)), 0.5, 2.0),
        "mlp_gain": jnp.clip(1.0 + 0.18 * jax.random.normal(key_of[11], (D,), jnp.float32), 0.1, 1.9),
        "up_weight": scatter_about(key_of[12], (D, FF), D ** -0.5, 0.125, ((0, 8), (1, 2)), jnp.float32),
        "up_scale": jnp.clip(jnp.exp(math.log(2.0) - 1.3862944 * jax.random.uniform(key_of[13], (FF,), jnp.float32) ** block_scale(key_of[13], (FF,), ((0, 16),), -0.2, 0.2)), 0.5, 2.0),
        "down_weight": scatter_about(key_of[14], (FF, D), FF ** -0.5, 0.078125, ((0, 2), (1, 8)), jnp.float32),
        "down_scale": jnp.clip(jnp.exp(math.log(2.0) - 1.3862944 * jax.random.uniform(key_of[15], (D,), jnp.float32) ** block_scale(key_of[15], (D,), ((0, 8),), -0.2, 0.2)), 0.5, 2.0),
    }


norm_eps = 1e-06

def normalize(values, gain):
    return values * lax.rsqrt(lax.optimization_barrier(jnp.mean(values * values, axis=-1, keepdims=True)) + norm_eps) * gain

def block_sum(left, right, blocks):
    rows = left.shape[0]
    width = left.shape[1] // blocks
    left_blocks = left.reshape(rows, blocks, width).astype(jnp.float32)
    right_blocks = right.reshape(blocks, width, right.shape[1]).astype(jnp.float32)
    parts = jnp.einsum('lnk,nkd->nld', left_blocks, right_blocks).astype(jnp.bfloat16)
    parts = lax.optimization_barrier(parts)
    return lax.optimization_barrier(jnp.sum(parts.astype(jnp.float32), axis=0))

def reference(tokens, mix_gain, value_weight, value_scale, inner_weight, inner_scale, outer_weight, outer_scale, conv_taps, out_weight, out_scale, mlp_gain, up_weight, up_scale, down_weight, down_scale):
    value_b = value_weight.astype(jnp.bfloat16)
    inner_b = inner_weight.astype(jnp.bfloat16)
    outer_b = outer_weight.astype(jnp.bfloat16)
    out_b = out_weight.astype(jnp.bfloat16)
    up_b = up_weight.astype(jnp.bfloat16)
    down_b = down_weight.astype(jnp.bfloat16)

    def one_sequence(sequence):
        start = sequence.astype(jnp.float32)
        normed = normalize(start, mix_gain).astype(jnp.bfloat16)
        value = jnp.dot(normed, value_b, preferred_element_type=jnp.float32) * value_scale
        inner = jnp.dot(normed, inner_b, preferred_element_type=jnp.float32) * inner_scale
        outer = jnp.dot(normed, outer_b, preferred_element_type=jnp.float32) * outer_scale
        gated = inner * value
        padded = jnp.pad(gated, ((1, 1), (0, 0)))
        conv = conv_taps[0] * padded[:-2] + conv_taps[1] * padded[1:-1] + conv_taps[2] * padded[2:]
        hidden = (outer * conv).astype(jnp.bfloat16)
        middle = start + block_sum(hidden, out_b, N_TP) * out_scale
        normed_mid = normalize(middle, mlp_gain).astype(jnp.bfloat16)
        upper = jnp.dot(normed_mid, up_b, preferred_element_type=jnp.float32) * up_scale
        act = jnp.square(jax.nn.relu(upper)).astype(jnp.bfloat16)
        return (middle + block_sum(act, down_b, N_TP) * down_scale).astype(jnp.bfloat16)
    return lax.map(one_sequence, tokens)
```

```python
import functools

import jax
import jax.numpy as jnp
from jax import lax
from jax.experimental import pallas as pl
from jax.experimental.pallas import tpu as pltpu
from jax.sharding import PartitionSpec as P

MESH = pl.DeviceIdType.MESH
norm_eps = 1e-06
HALO = 16
TILE = 16
f32 = jnp.float32
bf16 = jnp.bfloat16

def kernel(
    nz, G, T, win, rows, inside,
    tok, g1, g2, vectors, weights,
    out,
    WA, WO, WU, WD, nrm, hid, p1, q1, mid32, mid, act, p2, q2,
    staged, leaving, gathered,
    rz, rd, sz, sd, sy, loc, rn, sn, r1, s1, ra, sa, r2, s2, ro, so,
):
    if inside:
        packed, table, asc, taps, usc, oc, dc = gathered
    else:
        asc, taps, usc, oc, dc = vectors
    D = tok.shape[1]
    pw = D // nz
    cw = pw // 2
    r, f, t = lax.axis_index("rep"), lax.axis_index("fs"), lax.axis_index("tp")
    z, y = f // 2, f % 2
    fy = z * 2 + 1 - y
    g = r * 2 + y
    ka, ko, ku, kd = (w.shape[0] for w in leaving)
    stages = range(5 if inside else 4)
    has_lo, has_hi = z > 0, z < nz - 1
    if T == 2:
        start, off = t * (rows - HALO), t * HALO
    else:
        start = jnp.clip(t * rows - HALO, 0, tok.shape[0] - win)
        off = t * rows - start
    start, off = pl.multiple_of(start, HALO), pl.multiple_of(off, HALO)

    def member(m):
        return (m // 2, z * 2 + m % 2, t)

    def others():
        return [(g + d) % G for d in range(1, G)]

    def siblings():
        return [(t + d) % T for d in range(1, T)]

    def copy(src, dst, ssem, rsem, dev):
        return pltpu.make_async_remote_copy(
            src_ref=src, dst_ref=dst, send_sem=ssem, recv_sem=rsem, device_id=dev, device_id_type=MESH
        )

    def arrived(ref, sem):
        pltpu.make_async_copy(ref, ref, sem).wait()

    def slot(s, ff, tt):
        if s == 0:
            return WA.at[tt, pl.ds(pl.multiple_of(ff * ka, ka), ka)]
        if s == 1:
            return WO.at[ff, pl.ds(pl.multiple_of(tt * ko, ko), ko)]
        if s == 2:
            return WU.at[tt, pl.ds(pl.multiple_of(ff * ku, ku), ku)]
        if s == 3:
            return WD.at[ff, pl.ds(pl.multiple_of(tt * kd, kd), kd)]
        return table.at[ff, tt]

    def to_siblings(s, ff, src):
        for tt in siblings():
            copy(src, slot(s, ff, t), sd.at[s, ff], rd.at[s, ff], (r, f, tt)).start()

    def both_ways(s, ff, src):
        @pl.when(has_lo)
        def _():
            copy(src, slot(s, ff, t), sz.at[s, ff, 0], rz.at[s, ff], (r, f - 2, t)).start()

        @pl.when(has_hi)
        def _():
            copy(src, slot(s, ff, t), sz.at[s, ff, 1], rz.at[s, ff], (r, f + 2, t)).start()

    def fetches():
        for i, w in enumerate(weights):
            src, dst = weights[i], staged[i]
            if w.shape[1] > dst.shape[1]:
                n = dst.shape[1]
                src = src.at[:, pl.ds(pl.multiple_of(r * n, n), n)]
            elif w.shape[0] > dst.shape[0]:
                n = dst.shape[0]
                src = src.at[pl.ds(pl.multiple_of(r * n, n), n)]
            yield pltpu.make_async_copy(src, dst, loc.at[i])

    def round_stage(s):
        parts = {0: (0, 1, 2), 1: (3,), 2: (4,), 3: (5,)}[s]
        high = leaving[s].shape[0]
        for i in parts:
            pltpu.make_async_copy(staged[i], staged[i], loc.at[i]).wait()
        for yy in range(2):

            @pl.when(y == yy)
            def _():
                @pl.loop(0, high // 32)
                def _(k):
                    at = pl.ds(pl.multiple_of(k * 32, 32), 32)
                    for n, i in enumerate(parts):
                        if s in (0, 2):
                            wide = staged[i].shape[1] // 2
                            mine = staged[i][at, yy * wide : (yy + 1) * wide]
                            theirs = staged[i][at, (1 - yy) * wide : (2 - yy) * wide]
                        else:
                            wide = staged[i].shape[1]
                            mine = staged[i][pl.ds(pl.multiple_of(yy * high + k * 32, 32), 32), :]
                            theirs = staged[i][pl.ds(pl.multiple_of((1 - yy) * high + k * 32, 32), 32), :]
                        cols = slice(n * wide, (n + 1) * wide)
                        leaving[s][at, cols] = theirs.astype(bf16)
                        if s == 0:
                            WA[t, pl.ds(pl.multiple_of(f * ka + k * 32, 32), 32), cols] = mine.astype(bf16)
                        elif s == 1:
                            WO[f, pl.ds(pl.multiple_of(t * ko + k * 32, 32), 32), :] = mine.astype(bf16)
                        elif s == 2:
                            WU[t, pl.ds(pl.multiple_of(f * ku + k * 32, 32), 32), :] = mine.astype(bf16)
                        else:
                            WD[f, pl.ds(pl.multiple_of(t * kd + k * 32, 32), 32), :] = mine.astype(bf16)

    def kick(s):
        own = slot(s, f, t)
        copy(leaving[s] if s < 4 else own, own, sy.at[s], rz.at[s, f], (r, fy, t)).start()
        both_ways(s, f, own)
        to_siblings(s, f, own)

    def kick2(s):
        arrived(slot(s, fy, t), rz.at[s, fy])
        both_ways(s, fy, slot(s, fy, t))
        to_siblings(s, fy, slot(s, fy, t))

    def place(j):
        k = (j + 1) // 2
        sg = 1 - 2 * (j % 2)
        return z + sg * k, z - sg

    def step(s, j):
        zs, nxt = place(j)

        @pl.when(jnp.logical_and(zs >= 0, zs < nz))
        def _():
            for yy in range(2):
                ff = 2 * zs + yy
                arrived(slot(s, ff, t), rz.at[s, ff])

                @pl.when(jnp.logical_and(nxt >= 0, nxt < nz))
                def _():
                    copy(
                        slot(s, ff, t), slot(s, ff, t), sz.at[s, ff, 0], rz.at[s, ff], (r, 2 * nxt + y, t)
                    ).start()

                to_siblings(s, ff, slot(s, ff, t))

    def steps(s, lo, hi):
        @pl.loop(lo, hi)
        def _(j):
            step(s, j)

    def from_siblings(s, ff):
        for tt in siblings():
            arrived(slot(s, ff, tt), rd.at[s, ff])

    def all_from_siblings(s):
        @pl.loop(0, 2 * nz)
        def _(ff):
            from_siblings(s, ff)

    last = 2 * nz - 1

    for fetch in fetches():
        fetch.start()
    if inside:
        at_col = 0
        for v in vectors[:3]:
            packed[:, at_col : at_col + v.shape[1]] = v[...]
            at_col += v.shape[1]
        few = vectors[0].shape[1]
        for k in range(3):
            packed[:, at_col : at_col + few] = vectors[6][k : k + 1, pl.ds(pl.multiple_of(f * few, few), few)]
            at_col += few
        for v in vectors[3:6]:
            packed[:, at_col : at_col + v.shape[1]] = v[...]
            at_col += v.shape[1]
        table[f, t] = packed[...]

    barrier = pltpu.get_barrier_semaphore()
    for m in others():
        pl.semaphore_signal(barrier, inc=1, device_id=member(m), device_id_type=MESH)
    for tt in siblings():
        pl.semaphore_signal(barrier, inc=1, device_id=(r, f, tt), device_id_type=MESH)

    @pl.when(has_lo)
    def _():
        pl.semaphore_signal(barrier, inc=1, device_id=(r, f - 2, t), device_id_type=MESH)

    @pl.when(has_hi)
    def _():
        pl.semaphore_signal(barrier, inc=1, device_id=(r, f + 2, t), device_id_type=MESH)

    pl.semaphore_wait(barrier, G + T - 2 + (z + nz - 1) // nz + (2 * nz - 2 - z) // nz)

    round_stage(0)
    round_stage(1)
    kick(0)
    if inside:
        kick(4)
    kick(1)
    round_stage(2)
    round_stage(3)

    @pl.loop(0, win // TILE)
    def _(i):
        at = pl.ds(pl.multiple_of(i * TILE, TILE), TILE)
        x = tok[pl.ds(pl.multiple_of(start + i * TILE, TILE), TILE), :].astype(f32)
        x = x * lax.rsqrt(jnp.mean(x * x, axis=-1, keepdims=True) + norm_eps) * g1[...]
        nrm[g, at, :] = x.astype(bf16)

    kick2(0)
    if inside:
        kick2(4)
    for m in others():
        copy(nrm.at[g], nrm.at[g], sn.at[m], rn.at[g], member(m)).start()
    kick(2)
    kick2(1)
    steps(0, 1, last)
    if inside:
        steps(4, 1, last)
    kick(3)
    kick2(2)
    steps(1, 1, last)

    all_from_siblings(0)
    for m in others():
        arrived(nrm.at[m], rn.at[m])
    if inside:
        all_from_siblings(4)
        few, ups, outs = vectors[0].shape[1], vectors[3].shape[1], vectors[4].shape[1]
        wide = 3 * vectors[0].shape[1] * 2
        near = 2 * nz // G
        for tt in range(T):
            for j in range(near):
                row_of = table[g * near + j, tt]
                for k in range(3):
                    at_col = (k * near + j) * few
                    asc[tt, :, at_col : at_col + few] = row_of[:, k * few : (k + 1) * few]
                    taps[tt, k : k + 1, j * few : (j + 1) * few] = row_of[:, (3 + k) * few : (4 + k) * few]
                usc[tt, :, j * ups : (j + 1) * ups] = row_of[:, wide : wide + ups]
        for zs in range(nz):
            for yy in range(2):
                row_of = table[2 * zs + yy, 0]
                cols = slice(yy * outs, (yy + 1) * outs)
                oc[zs, :, cols] = row_of[:, wide + ups : wide + ups + outs]
                dc[zs, :, cols] = row_of[:, wide + ups + outs :]
    c = taps.shape[2]

    @pl.loop(0, G)
    def _(gs):
        x = nrm[gs]
        row = lax.broadcasted_iota(jnp.int32, (win, c), 0)
        for tt in range(T):
            prod = jnp.dot(x, WA[tt], preferred_element_type=f32) * asc[tt]
            gated = prod[:, c : 2 * c] * prod[:, :c]
            before = jnp.where(row == 0, 0.0, pltpu.roll(gated, 1, 0))
            after = jnp.where(row == win - 1, 0.0, pltpu.roll(gated, win - 1, 0))
            conv = taps[tt, 0:1] * before + taps[tt, 1:2] * gated + taps[tt, 2:3] * after
            hid[gs, :, tt * c : (tt + 1) * c] = (prod[:, 2 * c :] * conv).astype(bf16)

    all_from_siblings(1)

    @pl.loop(0, nz)
    def _(zs):
        @pl.loop(0, G)
        def _(gs):
            h = hid[gs, pl.ds(off, rows), :]
            for yy in range(2):
                p1[gs, zs, :, yy * cw : (yy + 1) * cw] = jnp.dot(
                    h, WO[2 * zs + yy], preferred_element_type=f32
                ).astype(bf16)

    kick2(3)
    for m in others():
        copy(p1.at[m], q1.at[g], s1.at[m], r1.at[g], member(m)).start()
    cut = (2 * last) // 3
    steps(2, 1, cut)

    for m in others():
        arrived(q1.at[m], r1.at[m])

    def total(p, q, zs, at):
        acc = p[g, zs, at, :].astype(f32)
        for m in others():
            acc = acc + q[m, zs, at, :].astype(f32)
        return acc

    @pl.loop(0, rows // TILE)
    def _(i):
        at = pl.ds(pl.multiple_of(i * TILE, TILE), TILE)
        here = pl.ds(pl.multiple_of(t * rows + i * TILE, TILE), TILE)
        ssq = jnp.zeros((TILE, 1), f32)
        for zs in range(nz):
            m = tok[here, zs * pw : (zs + 1) * pw].astype(f32) + total(p1, q1, zs, at) * oc[zs]
            mid32[zs, at, :] = m
            ssq = ssq + jnp.sum(m * m, axis=-1, keepdims=True)
        inv = lax.rsqrt(ssq / D + norm_eps)
        for zs in range(nz):
            cols = slice(zs * pw, (zs + 1) * pw)
            mid[g, at, cols] = (mid32[zs, at, :] * inv * g2[:, cols]).astype(bf16)

    steps(2, cut, cut + 1)
    for m in others():
        copy(mid.at[g], mid.at[g], sa.at[m], ra.at[g], member(m)).start()
    steps(2, cut + 1, last)
    cut2 = (last + 1) // 2
    steps(3, 1, cut2)

    all_from_siblings(2)
    for m in others():
        arrived(mid.at[m], ra.at[m])
    u = usc.shape[2]

    @pl.loop(0, G)
    def _(gs):
        x = mid[gs]
        for tt in range(T):
            upper = jnp.dot(x, WU[tt], preferred_element_type=f32) * usc[tt]
            act[gs, :, tt * u : (tt + 1) * u] = jnp.square(jnp.maximum(upper, 0.0)).astype(bf16)

    def down(j):
        zs, _ = place(j)

        @pl.when(jnp.logical_and(zs >= 0, zs < nz))
        def _():
            for yy in range(2):
                from_siblings(3, 2 * zs + yy)

            @pl.loop(0, G)
            def _(gs):
                x = act[gs]
                for yy in range(2):
                    p2[gs, zs, :, yy * cw : (yy + 1) * cw] = jnp.dot(
                        x, WD[2 * zs + yy], preferred_element_type=f32
                    ).astype(bf16)

            for m in others():
                copy(p2.at[m, zs], q2.at[g, zs], s2.at[m, zs], r2.at[g, zs], member(m)).start()

    @pl.loop(0, last)
    def _(j):
        @pl.when(j >= cut2)
        def _():
            step(3, j)

        down(j)

    @pl.loop(0, nz)
    def _(zs):
        for m in others():
            arrived(q2.at[m, zs], r2.at[m, zs])

    @pl.loop(0, rows // TILE)
    def _(i):
        at = pl.ds(pl.multiple_of(i * TILE, TILE), TILE)
        here = pl.ds(pl.multiple_of(t * rows + i * TILE, TILE), TILE)
        for zs in range(nz):
            out[here, zs * pw : (zs + 1) * pw] = (
                mid32[zs, at, :] + total(p2, q2, zs, at) * dc[zs]
            ).astype(bf16)

    def half(tt):
        return out.at[pl.ds(pl.multiple_of(tt * rows, rows), rows)]

    for tt in siblings():
        copy(half(t), half(t), so.at[tt], ro.at[t], (r, f, tt)).start()

    for s in stages:
        own = slot(s, f, t)
        arrived(own, sy.at[s])

        def gone(ff, k, s=s, own=own):
            arrived(own, sz.at[s, ff, k])

        for ff in (f, fy):
            pl.when(has_lo)(functools.partial(gone, ff, 0))
            pl.when(has_hi)(functools.partial(gone, ff, 1))

        @pl.loop(1, last)
        def _(j):
            zs, nxt = place(j)
            ok = jnp.logical_and(zs >= 0, zs < nz)

            @pl.when(jnp.logical_and(ok, jnp.logical_and(nxt >= 0, nxt < nz)))
            def _():
                for yy in range(2):
                    gone(2 * zs + yy, 0)

        @pl.loop(0, 2 * nz)
        def _(ff):
            for _ in siblings():
                arrived(own, sd.at[s, ff])

    for m in others():
        arrived(nrm.at[m], sn.at[m])
        arrived(p1.at[m], s1.at[m])
        arrived(mid.at[m], sa.at[m])

        @pl.loop(0, nz)
        def _(zs):
            arrived(p2.at[m, zs], s2.at[m, zs])

    for tt in siblings():
        arrived(half(tt), ro.at[tt])
        arrived(half(tt), so.at[tt])

def line_kernel(
    nz, G, T, win, rows, inside,
    tok, g1, g2, vectors, weights,
    out,
    WA, WO, WU, WD, nrm, hid, p1, q1, mid32, mid, act, p2, q2,
    staged, leaving, gathered,
    rz, rd, sz, sd, sy, loc, rn, sn, r1, s1, ra, sa, r2, s2, ro, so,
):
    if inside:
        packed, table, asc, taps, usc, oc, dc = gathered
    else:
        asc, taps, usc, oc, dc = vectors
    D = tok.shape[1]
    pw = D // nz
    cw = pw // 2
    r, f, t = lax.axis_index("rep"), lax.axis_index("fs"), lax.axis_index("tp")
    z, y = f // 2, f % 2
    fy = z * 2 + 1 - y
    g = r * 2 + y
    ka, ko, ku, kd = (w.shape[0] for w in leaving)
    stages = range(5 if inside else 4)
    has_lo, has_hi = z > 0, z < nz - 1
    outer = jnp.logical_or(z == 0, z == nz - 1)
    inner = jnp.logical_not(outer)
    inward = jnp.where(2 * z < nz, 1, -1)
    across = z + 2 * inward
    if T == 2:
        start, off = t * (rows - HALO), t * HALO
    else:
        start = jnp.clip(t * rows - HALO, 0, tok.shape[0] - win)
        off = t * rows - start
    start, off = pl.multiple_of(start, HALO), pl.multiple_of(off, HALO)

    def member(m):
        return (m // 2, z * 2 + m % 2, t)

    def others():
        return [(g + d) % G for d in range(1, G)]

    gx, gy, gd = (1 - r) * 2 + y, r * 2 + 1 - y, (1 - r) * 2 + 1 - y

    def peers():
        return [gd, gx, gy]

    def siblings():
        return [(t + d) % T for d in range(1, T)]

    def copy(src, dst, ssem, rsem, dev):
        return pltpu.make_async_remote_copy(
            src_ref=src, dst_ref=dst, send_sem=ssem, recv_sem=rsem, device_id=dev, device_id_type=MESH
        )

    def arrived(ref, sem):
        pltpu.make_async_copy(ref, ref, sem).wait()

    def slot(s, ff, tt):
        if s == 0:
            return WA.at[tt, pl.ds(pl.multiple_of(ff * ka, ka), ka)]
        if s == 1:
            return WO.at[ff, pl.ds(pl.multiple_of(tt * ko, ko), ko)]
        if s == 2:
            return WU.at[tt, pl.ds(pl.multiple_of(ff * ku, ku), ku)]
        if s == 3:
            return WD.at[ff, pl.ds(pl.multiple_of(tt * kd, kd), kd)]
        return table.at[ff, tt]

    def to_siblings(s, ff, src):
        for tt in siblings():
            copy(src, slot(s, ff, t), sd.at[s, ff], rd.at[s, ff], (r, f, tt)).start()

    def both_ways(s, ff, src):
        @pl.when(has_lo)
        def _():
            copy(src, slot(s, ff, t), sz.at[s, ff, 0], rz.at[s, ff], (r, f - 2, t)).start()

        @pl.when(has_hi)
        def _():
            copy(src, slot(s, ff, t), sz.at[s, ff, 1], rz.at[s, ff], (r, f + 2, t)).start()

        @pl.when(outer)
        def _():
            copy(src, slot(s, ff, t), sz.at[s, ff, 2], rz.at[s, ff], (r, 2 * across + y, t)).start()

    def fetches():
        for i, w in enumerate(weights):
            src, dst = weights[i], staged[i]
            if w.shape[1] > dst.shape[1]:
                n = dst.shape[1]
                src = src.at[:, pl.ds(pl.multiple_of(r * n, n), n)]
            elif w.shape[0] > dst.shape[0]:
                n = dst.shape[0]
                src = src.at[pl.ds(pl.multiple_of(r * n, n), n)]
            yield pltpu.make_async_copy(src, dst, loc.at[i])

    def round_stage(s):
        parts = {0: (0, 1, 2), 1: (3,), 2: (4,), 3: (5,)}[s]
        high = leaving[s].shape[0]
        for i in parts:
            pltpu.make_async_copy(staged[i], staged[i], loc.at[i]).wait()
        for yy in range(2):

            @pl.when(y == yy)
            def _():
                @pl.loop(0, high // 32)
                def _(k):
                    at = pl.ds(pl.multiple_of(k * 32, 32), 32)
                    for n, i in enumerate(parts):
                        if s in (0, 2):
                            wide = staged[i].shape[1] // 2
                            mine = staged[i][at, yy * wide : (yy + 1) * wide]
                            theirs = staged[i][at, (1 - yy) * wide : (2 - yy) * wide]
                        else:
                            wide = staged[i].shape[1]
                            mine = staged[i][pl.ds(pl.multiple_of(yy * high + k * 32, 32), 32), :]
                            theirs = staged[i][pl.ds(pl.multiple_of((1 - yy) * high + k * 32, 32), 32), :]
                        cols = slice(n * wide, (n + 1) * wide)
                        leaving[s][at, cols] = theirs.astype(bf16)
                        if s == 0:
                            WA[t, pl.ds(pl.multiple_of(f * ka + k * 32, 32), 32), cols] = mine.astype(bf16)
                        elif s == 1:
                            WO[f, pl.ds(pl.multiple_of(t * ko + k * 32, 32), 32), :] = mine.astype(bf16)
                        elif s == 2:
                            WU[t, pl.ds(pl.multiple_of(f * ku + k * 32, 32), 32), :] = mine.astype(bf16)
                        else:
                            WD[f, pl.ds(pl.multiple_of(t * kd + k * 32, 32), 32), :] = mine.astype(bf16)

    def swap(s):
        own = slot(s, f, t)
        copy(leaving[s] if s < 4 else own, own, sy.at[s], rz.at[s, f], (r, fy, t)).start()
        to_siblings(s, f, own)

    def spread(s):
        both_ways(s, f, slot(s, f, t))

    def kick2(s):
        arrived(slot(s, fy, t), rz.at[s, fy])
        both_ways(s, fy, slot(s, fy, t))
        to_siblings(s, fy, slot(s, fy, t))

    def place(j):
        return (z + inward * j + nz) % nz

    def relayed(zs):
        return jnp.logical_and(inner, zs != z - inward)

    blocks = 2 * (nz - 1)

    def block(i):
        first, rest = i < 2, jnp.maximum(i - 2, 0)
        near_out, late_out = jnp.where(first, 1, 2 + rest % 2), jnp.where(first, i, rest // 2)
        near_in, late_in = jnp.where(i < 4, 1 + i % 2, nz - 1), jnp.where(i < 4, i // 2, i % 2)
        near, late = jnp.where(inner, near_in, near_out), jnp.where(inner, late_in, late_out)
        return place(near), (y + late) % 2

    def step(s, i):
        zs, yy = block(i)
        ff = 2 * zs + yy
        arrived(slot(s, ff, t), rz.at[s, ff])

        @pl.when(relayed(zs))
        def _():
            copy(
                slot(s, ff, t), slot(s, ff, t), sz.at[s, ff, 0], rz.at[s, ff], (r, 2 * (z - inward) + y, t)
            ).start()

        to_siblings(s, ff, slot(s, ff, t))

    def steps(s, lo, hi):
        @pl.loop(lo, hi)
        def _(j):
            step(s, j)

    def from_siblings(s, ff):
        for tt in siblings():
            arrived(slot(s, ff, tt), rd.at[s, ff])

    def all_from_siblings(s):
        @pl.loop(0, 2 * nz)
        def _(ff):
            from_siblings(s, ff)

    for fetch in fetches():
        fetch.start()
    if inside:
        at_col = 0
        for v in vectors[:3]:
            packed[:, at_col : at_col + v.shape[1]] = v[...]
            at_col += v.shape[1]
        few = vectors[0].shape[1]
        for k in range(3):
            packed[:, at_col : at_col + few] = vectors[6][k : k + 1, pl.ds(pl.multiple_of(f * few, few), few)]
            at_col += few
        for v in vectors[3:6]:
            packed[:, at_col : at_col + v.shape[1]] = v[...]
            at_col += v.shape[1]
        table[f, t] = packed[...]

    barrier = pltpu.get_barrier_semaphore()
    for m in others():
        pl.semaphore_signal(barrier, inc=1, device_id=member(m), device_id_type=MESH)
    for tt in siblings():
        pl.semaphore_signal(barrier, inc=1, device_id=(r, f, tt), device_id_type=MESH)

    for zs in (z - 1, z + 1, across):
        near = jnp.logical_and(zs >= 0, zs < nz)

        @pl.when(jnp.logical_and(near, zs != z))
        def _():
            pl.semaphore_signal(barrier, inc=1, device_id=(r, 2 * zs + y, t), device_id_type=MESH)

    pl.semaphore_wait(barrier, G + T - 2 + jnp.where(outer, 2, 3))

    round_stage(0)
    round_stage(1)
    early = (0, 4, 1) if inside else (0, 1)
    for s in early:
        swap(s)
        spread(s)
    round_stage(2)
    round_stage(3)

    @pl.loop(0, win // TILE)
    def _(i):
        at = pl.ds(pl.multiple_of(i * TILE, TILE), TILE)
        x = tok[pl.ds(pl.multiple_of(start + i * TILE, TILE), TILE), :].astype(f32)
        x = x * lax.rsqrt(jnp.mean(x * x, axis=-1, keepdims=True) + norm_eps) * g1[...]
        nrm[g, at, :] = x.astype(bf16)

    for s in early:
        kick2(s)
    for m in (gx, gy):
        copy(nrm.at[g], nrm.at[g], sn.at[m], rn.at[g], member(m)).start()
    for s in (2, 3):
        swap(s)

    @pl.when(outer)
    def _():
        spread(2)
        spread(3)

    steps(0, 0, 2)

    arrived(nrm.at[gy], rn.at[gy])
    copy(nrm.at[gy], nrm.at[gy], sn.at[gd], rn.at[gy], member(gx)).start()

    steps(0, 2, blocks)
    if inside:
        steps(4, 0, blocks)

    @pl.when(inner)
    def _():
        spread(2)
        kick2(2)

    all_from_siblings(0)
    if inside:
        all_from_siblings(4)

    for m in (gx, gd):
        arrived(nrm.at[m], rn.at[m])
    if inside:
        few, ups, outs = vectors[0].shape[1], vectors[3].shape[1], vectors[4].shape[1]
        wide = 3 * vectors[0].shape[1] * 2
        near = 2 * nz // G
        for tt in range(T):
            for j in range(near):
                row_of = table[g * near + j, tt]
                for k in range(3):
                    at_col = (k * near + j) * few
                    asc[tt, :, at_col : at_col + few] = row_of[:, k * few : (k + 1) * few]
                    taps[tt, k : k + 1, j * few : (j + 1) * few] = row_of[:, (3 + k) * few : (4 + k) * few]
                usc[tt, :, j * ups : (j + 1) * ups] = row_of[:, wide : wide + ups]
        for zs in range(nz):
            for yy in range(2):
                row_of = table[2 * zs + yy, 0]
                cols = slice(yy * outs, (yy + 1) * outs)
                oc[zs, :, cols] = row_of[:, wide + ups : wide + ups + outs]
                dc[zs, :, cols] = row_of[:, wide + ups + outs :]
    c = taps.shape[2]

    @pl.loop(0, G)
    def _(gs):
        x = nrm[gs]
        row = lax.broadcasted_iota(jnp.int32, (win, c), 0)
        for tt in range(T):
            prod = jnp.dot(x, WA[tt], preferred_element_type=f32) * asc[tt]
            gated = prod[:, c : 2 * c] * prod[:, :c]
            before = jnp.where(row == 0, 0.0, pltpu.roll(gated, 1, 0))
            after = jnp.where(row == win - 1, 0.0, pltpu.roll(gated, win - 1, 0))
            conv = taps[tt, 0:1] * before + taps[tt, 1:2] * gated + taps[tt, 2:3] * after
            hid[gs, :, tt * c : (tt + 1) * c] = (prod[:, 2 * c :] * conv).astype(bf16)

    @pl.loop(0, nz)
    def _(j):
        zs = place(j)

        @pl.when(jnp.logical_and(j > 0, j < nz - 1))
        def _():
            steps(1, jnp.where(j == 1, 0, 3), jnp.where(j == 1, 3, blocks))

        for yy in range(2):
            from_siblings(1, 2 * zs + yy)

        @pl.loop(0, G)
        def _(gs):
            h = hid[gs, pl.ds(off, rows), :]
            for yy in range(2):
                p1[gs, zs, :, yy * cw : (yy + 1) * cw] = jnp.dot(
                    h, WO[2 * zs + yy], preferred_element_type=f32
                ).astype(bf16)

        for m in peers():
            copy(p1.at[m, zs], q1.at[g, zs], s1.at[m, zs], r1.at[g, zs], member(m)).start()

    @pl.when(outer)
    def _():
        kick2(2)
        kick2(3)

    cut = jnp.where(inner, blocks, 2)
    steps(2, 0, cut)

    @pl.when(inner)
    def _():
        spread(3)
        kick2(3)

    @pl.loop(0, nz)
    def _(zs):
        for m in others():
            arrived(q1.at[m, zs], r1.at[m, zs])

    def total(p, q, zs, at):
        acc = p[g, zs, at, :].astype(f32)
        for m in others():
            acc = acc + q[m, zs, at, :].astype(f32)
        return acc

    @pl.loop(0, rows // TILE)
    def _(i):
        at = pl.ds(pl.multiple_of(i * TILE, TILE), TILE)
        here = pl.ds(pl.multiple_of(t * rows + i * TILE, TILE), TILE)
        ssq = jnp.zeros((TILE, 1), f32)
        for zs in range(nz):
            m = tok[here, zs * pw : (zs + 1) * pw].astype(f32) + total(p1, q1, zs, at) * oc[zs]
            mid32[zs, at, :] = m
            ssq = ssq + jnp.sum(m * m, axis=-1, keepdims=True)
        inv = lax.rsqrt(ssq / D + norm_eps)
        for zs in range(nz):
            cols = slice(zs * pw, (zs + 1) * pw)
            mid[g, at, cols] = (mid32[zs, at, :] * inv * g2[:, cols]).astype(bf16)

    for m in (gx, gy):
        copy(mid.at[g], mid.at[g], sa.at[m], ra.at[g], member(m)).start()

    cut1 = jnp.where(inner, blocks, 4)
    steps(2, cut, cut1)

    part = rows // 2
    for m, n, lo in ((gx, gy, part), (gy, gx, 0)):
        arrived(mid.at[m], ra.at[m])
        some = mid.at[m, pl.ds(lo, part)]
        copy(some, some, sa.at[gd if lo else g], ra.at[m] if lo else ra.at[G], member(n)).start()

    steps(2, cut1, blocks)

    cut2 = jnp.where(inner, blocks, 0)
    steps(3, 0, cut2)

    all_from_siblings(2)

    some = mid.at[gd, pl.ds(0, part)]
    arrived(some, ra.at[gd])
    arrived(some, ra.at[G])

    u = usc.shape[2]

    @pl.loop(0, G)
    def _(gs):
        x = mid[gs]
        for tt in range(T):
            upper = jnp.dot(x, WU[tt], preferred_element_type=f32) * usc[tt]
            act[gs, :, tt * u : (tt + 1) * u] = jnp.square(jnp.maximum(upper, 0.0)).astype(bf16)

    @pl.loop(0, nz)
    def _(j):
        zs = place(j)

        @pl.when(outer & (j > 0) & (j < nz - 1))
        def _():
            steps(3, jnp.where(j == 1, 0, 2), jnp.where(j == 1, 2, blocks - 1))

        @pl.when(outer & (j == nz - 1))
        def _():
            steps(3, blocks - 1, blocks)

        for yy in range(2):
            from_siblings(3, 2 * zs + yy)

        @pl.loop(0, G)
        def _(gs):
            x = act[gs]
            for yy in range(2):
                p2[gs, zs, :, yy * cw : (yy + 1) * cw] = jnp.dot(
                    x, WD[2 * zs + yy], preferred_element_type=f32
                ).astype(bf16)

        for m in peers():
            copy(p2.at[m, zs], q2.at[g, zs], s2.at[m, zs], r2.at[g, zs], member(m)).start()

    @pl.loop(0, nz)
    def _(zs):
        for m in others():
            arrived(q2.at[m, zs], r2.at[m, zs])

    @pl.loop(0, rows // TILE)
    def _(i):
        at = pl.ds(pl.multiple_of(i * TILE, TILE), TILE)
        here = pl.ds(pl.multiple_of(t * rows + i * TILE, TILE), TILE)
        for zs in range(nz):
            out[here, zs * pw : (zs + 1) * pw] = (
                mid32[zs, at, :] + total(p2, q2, zs, at) * dc[zs]
            ).astype(bf16)

    def half(tt):
        return out.at[pl.ds(pl.multiple_of(tt * rows, rows), rows)]

    for tt in siblings():
        copy(half(t), half(t), so.at[tt], ro.at[t], (r, f, tt)).start()

    for s in stages:
        own = slot(s, f, t)
        arrived(own, sy.at[s])

        def gone(ff, k, s=s, own=own):
            arrived(own, sz.at[s, ff, k])

        for ff in (f, fy):
            pl.when(has_lo)(functools.partial(gone, ff, 0))
            pl.when(has_hi)(functools.partial(gone, ff, 1))
            pl.when(outer)(functools.partial(gone, ff, 2))

        @pl.loop(1, nz)
        def _(j):
            zs = place(j)

            @pl.when(relayed(zs))
            def _():
                for yy in range(2):
                    gone(2 * zs + yy, 0)

        @pl.loop(0, 2 * nz)
        def _(ff):
            for _ in siblings():
                arrived(own, sd.at[s, ff])

    for m in others():
        arrived(nrm.at[m], sn.at[m])

    for m in (gx, gy):
        arrived(mid.at[m], sa.at[m])
    for m in (g, gd):
        arrived(mid.at[g, pl.ds(0, part)], sa.at[m])

    for m in others():

        @pl.loop(0, nz)
        def _(zs):
            arrived(p1.at[m, zs], s1.at[m, zs])
            arrived(p2.at[m, zs], s2.at[m, zs])

    for tt in siblings():
        arrived(half(tt), ro.at[tt])
        arrived(half(tt), so.at[tt])

def body(
    R, n_fs, T,
    tokens, mix_gain, value_weight, value_scale, inner_weight, inner_scale, outer_weight, outer_scale,
    conv_taps, out_weight, out_scale, mlp_gain, up_weight, up_scale, down_weight, down_scale,
):
    G, nz = 2 * R, n_fs // 2
    TOK, D = tokens.shape[1:]
    rows = TOK // T
    win = TOK if T == 1 else rows + HALO if T == 2 else rows + 2 * HALO
    r, f = lax.axis_index("rep"), lax.axis_index("fs")
    g = r * 2 + f % 2

    vs, us, os = value_scale.shape[0], up_scale.shape[0], out_scale.shape[0]
    inside = all(n % 128 == 0 for n in (vs, us, os))
    c, u = conv_taps.shape[1] // G, up_weight.shape[1] // G
    if inside:
        scales = (value_scale, inner_scale, outer_scale, up_scale, out_scale, down_scale)
        vectors = tuple(v[None] for v in scales) + (conv_taps,)
    else:
        tap = lax.dynamic_slice_in_dim(conv_taps, f * vs, vs, axis=1)
        packed = jnp.concatenate(
            [value_scale, inner_scale, outer_scale, tap[0], tap[1], tap[2], up_scale, out_scale, down_scale]
        )
        every = lax.all_gather(packed, ("tp", "fs"), axis=0, tiled=False).reshape(T, n_fs, -1)

        def block(v):
            return lax.dynamic_index_in_dim(v.reshape(T, G, -1), g, axis=1, keepdims=True)

        small = [block(every[:, :, i * vs : (i + 1) * vs]) for i in range(6)]
        asc = jnp.concatenate(small[:3], axis=2)
        taps = jnp.concatenate(small[3:], axis=1)
        usc = block(every[:, :, 6 * vs : 6 * vs + us])
        oc = every[0, :, 6 * vs + us : 6 * vs + us + os].reshape(nz, 1, -1)
        dc = every[0, :, 6 * vs + us + os :].reshape(nz, 1, -1)
        vectors = (asc, taps, usc, oc, dc)
    weights = (value_weight, inner_weight, outer_weight, out_weight, up_weight, down_weight)
    ka, ko, kd = value_weight.shape[0], out_weight.shape[0] // G, down_weight.shape[0] // G
    cw = out_weight.shape[1]
    rounded = [(ka, 3 * c), (ko, cw), (ka, u), (kd, cw)]
    staged = [(ka, 2 * c)] * 3 + [(2 * ko, cw), (ka, 2 * u), (2 * kd, cw)]
    gathered = ()
    if inside:
        L = 6 * vs + us + 2 * os
        small = [(1, L), (n_fs, T, 1, L), (T, 1, 3 * c), (T, 3, c), (T, 1, u), (nz, 1, 2 * cw), (nz, 1, 2 * cw)]
        gathered = tuple(pltpu.VMEM(shape, f32) for shape in small)
    pw = D // nz
    lined = T == 2 and nz == 4 and R == 2
    dma = pltpu.SemaphoreType.DMA
    vmem = pl.BlockSpec(memory_space=pltpu.VMEM)
    hbm = pl.BlockSpec(memory_space=pl.ANY)
    result = pl.pallas_call(
        functools.partial(line_kernel if lined else kernel, nz, G, T, win, rows, inside),
        out_shape=jax.ShapeDtypeStruct((TOK, D), bf16),
        in_specs=[vmem] * 3 + [(vmem,) * len(vectors), (hbm,) * 6],
        out_specs=vmem,
        scratch_shapes=[
            pltpu.VMEM((T, D, 3 * c), bf16),
            pltpu.VMEM((n_fs, T * ko, cw), bf16),
            pltpu.VMEM((T, D, u), bf16),
            pltpu.VMEM((n_fs, T * kd, cw), bf16),
            pltpu.VMEM((G, win, D), bf16),
            pltpu.VMEM((G, win, T * ko), bf16),
            pltpu.VMEM((G, nz, rows, pw), bf16),
            pltpu.VMEM((G, nz, rows, pw), bf16),
            pltpu.VMEM((nz, rows, pw), f32),
            pltpu.VMEM((G, rows, D), bf16),
            pltpu.VMEM((G, rows, T * kd), bf16),
            pltpu.VMEM((G, nz, rows, pw), bf16),
            pltpu.VMEM((G, nz, rows, pw), bf16),
            tuple(pltpu.VMEM(shape, f32) for shape in staged),
            tuple(pltpu.VMEM(shape, bf16) for shape in rounded),
            gathered,
            dma((5, n_fs)),
            dma((5, n_fs)),
            dma((5, n_fs, 3)),
            dma((5, n_fs)),
            dma((5,)),
            dma((6,)),
            dma((G,)),
            dma((G,)),
            dma((G, nz) if lined else (G,)),
            dma((G, nz) if lined else (G,)),
            dma((G + 1,)),
            dma((G + 1,)),
            dma((G, nz)),
            dma((G, nz)),
            dma((T,)),
            dma((T,)),
        ],
        compiler_params=pltpu.CompilerParams(
            collective_id=0, has_side_effects=True, vmem_limit_bytes=65000000
        ),
    )(tokens[0], mix_gain[None], mlp_gain[None], vectors, weights)
    return result[None]

def solution(mesh):
    placed = (
        P(("rep", "fs"), None, None),
        P(),
        P("fs", "tp"),
        P(("tp", "fs")),
        P("fs", "tp"),
        P(("tp", "fs")),
        P("fs", "tp"),
        P(("tp", "fs")),
        P(None, "tp"),
        P("tp", "fs"),
        P("fs"),
        P(),
        P("fs", "tp"),
        P(("tp", "fs")),
        P("tp", "fs"),
        P("fs"),
    )
    sizes = (mesh.shape["rep"], mesh.shape["fs"], mesh.shape["tp"])
    return jax.shard_map(
        functools.partial(body, *sizes),
        mesh=mesh,
        in_specs=placed,
        out_specs=P(("rep", "fs"), None, None),
        check_vma=False,
    )
```

```python
import functools

import jax
import jax.numpy as jnp
from jax import lax
from jax.experimental import pallas as pl
from jax.experimental.pallas import tpu as pltpu
from jax.sharding import PartitionSpec as P

MESH = pl.DeviceIdType.MESH
norm_eps = 1e-06
HALO = 16
TILE = 16
f32 = jnp.float32
bf16 = jnp.bfloat16

def kernel(
    nz, G, T, win, rows, inside,
    tok, g1, g2, vectors, weights,
    out,
    WA, WO, WU, WD, nrm, hid, p1, q1, mid32, mid, act, p2, q2,
    staged, leaving, gathered,
    rz, rd, sz, sd, sy, loc, rn, sn, r1, s1, ra, sa, r2, s2, ro, so,
):
    if inside:
        packed, table, asc, taps, usc, oc, dc = gathered
    else:
        asc, taps, usc, oc, dc = vectors
    D = tok.shape[1]
    pw = D // nz
    cw = pw // 2
    r, f, t = lax.axis_index("rep"), lax.axis_index("fs"), lax.axis_index("tp")
    z, y = f // 2, f % 2
    fy = z * 2 + 1 - y
    g = r * 2 + y
    ka, ko, ku, kd = (w.shape[0] for w in leaving)
    stages = range(5 if inside else 4)
    has_lo, has_hi = z > 0, z < nz - 1
    if T == 2:
        start, off = t * (rows - HALO), t * HALO
    else:
        start = jnp.clip(t * rows - HALO, 0, tok.shape[0] - win)
        off = t * rows - start
    start, off = pl.multiple_of(start, HALO), pl.multiple_of(off, HALO)

    def member(m):
        return (m // 2, z * 2 + m % 2, t)

    def others():
        return [(g + d) % G for d in range(1, G)]

    def siblings():
        return [(t + d) % T for d in range(1, T)]

    def copy(src, dst, ssem, rsem, dev):
        return pltpu.make_async_remote_copy(
            src_ref=src, dst_ref=dst, send_sem=ssem, recv_sem=rsem, device_id=dev, device_id_type=MESH
        )

    def arrived(ref, sem):
        pltpu.make_async_copy(ref, ref, sem).wait()

    def slot(s, ff, tt):
        if s == 0:
            return WA.at[tt, pl.ds(pl.multiple_of(ff * ka, ka), ka)]
        if s == 1:
            return WO.at[ff, pl.ds(pl.multiple_of(tt * ko, ko), ko)]
        if s == 2:
            return WU.at[tt, pl.ds(pl.multiple_of(ff * ku, ku), ku)]
        if s == 3:
            return WD.at[ff, pl.ds(pl.multiple_of(tt * kd, kd), kd)]
        return table.at[ff, tt]

    def to_siblings(s, ff, src):
        for tt in siblings():
            copy(src, slot(s, ff, t), sd.at[s, ff], rd.at[s, ff], (r, f, tt)).start()

    def both_ways(s, ff, src):
        @pl.when(has_lo)
        def _():
            copy(src, slot(s, ff, t), sz.at[s, ff, 0], rz.at[s, ff], (r, f - 2, t)).start()

        @pl.when(has_hi)
        def _():
            copy(src, slot(s, ff, t), sz.at[s, ff, 1], rz.at[s, ff], (r, f + 2, t)).start()

    def fetches():
        for i, w in enumerate(weights):
            src, dst = weights[i], staged[i]
            if w.shape[1] > dst.shape[1]:
                n = dst.shape[1]
                src = src.at[:, pl.ds(pl.multiple_of(r * n, n), n)]
            elif w.shape[0] > dst.shape[0]:
                n = dst.shape[0]
                src = src.at[pl.ds(pl.multiple_of(r * n, n), n)]
            yield pltpu.make_async_copy(src, dst, loc.at[i])

    def round_stage(s):
        parts = {0: (0, 1, 2), 1: (3,), 2: (4,), 3: (5,)}[s]
        high = leaving[s].shape[0]
        for i in parts:
            pltpu.make_async_copy(staged[i], staged[i], loc.at[i]).wait()
        for yy in range(2):

            @pl.when(y == yy)
            def _():
                @pl.loop(0, high // 32)
                def _(k):
                    at = pl.ds(pl.multiple_of(k * 32, 32), 32)
                    for n, i in enumerate(parts):
                        if s in (0, 2):
                            wide = staged[i].shape[1] // 2
                            mine = staged[i][at, yy * wide : (yy + 1) * wide]
                            theirs = staged[i][at, (1 - yy) * wide : (2 - yy) * wide]
                        else:
                            wide = staged[i].shape[1]
                            mine = staged[i][pl.ds(pl.multiple_of(yy * high + k * 32, 32), 32), :]
                            theirs = staged[i][pl.ds(pl.multiple_of((1 - yy) * high + k * 32, 32), 32), :]
                        cols = slice(n * wide, (n + 1) * wide)
                        leaving[s][at, cols] = theirs.astype(bf16)
                        if s == 0:
                            WA[t, pl.ds(pl.multiple_of(f * ka + k * 32, 32), 32), cols] = mine.astype(bf16)
                        elif s == 1:
                            WO[f, pl.ds(pl.multiple_of(t * ko + k * 32, 32), 32), :] = mine.astype(bf16)
                        elif s == 2:
                            WU[t, pl.ds(pl.multiple_of(f * ku + k * 32, 32), 32), :] = mine.astype(bf16)
                        else:
                            WD[f, pl.ds(pl.multiple_of(t * kd + k * 32, 32), 32), :] = mine.astype(bf16)

    def kick(s):
        own = slot(s, f, t)
        copy(leaving[s] if s < 4 else own, own, sy.at[s], rz.at[s, f], (r, fy, t)).start()
        both_ways(s, f, own)
        to_siblings(s, f, own)

    def kick2(s):
        arrived(slot(s, fy, t), rz.at[s, fy])
        both_ways(s, fy, slot(s, fy, t))
        to_siblings(s, fy, slot(s, fy, t))

    def place(j):
        k = (j + 1) // 2
        sg = 1 - 2 * (j % 2)
        return z + sg * k, z - sg

    def step(s, j):
        zs, nxt = place(j)

        @pl.when(jnp.logical_and(zs >= 0, zs < nz))
        def _():
            for yy in range(2):
                ff = 2 * zs + yy
                arrived(slot(s, ff, t), rz.at[s, ff])

                @pl.when(jnp.logical_and(nxt >= 0, nxt < nz))
                def _():
                    copy(
                        slot(s, ff, t), slot(s, ff, t), sz.at[s, ff, 0], rz.at[s, ff], (r, 2 * nxt + y, t)
                    ).start()

                to_siblings(s, ff, slot(s, ff, t))

    def steps(s, lo, hi):
        @pl.loop(lo, hi)
        def _(j):
            step(s, j)

    def from_siblings(s, ff):
        for tt in siblings():
            arrived(slot(s, ff, tt), rd.at[s, ff])

    def all_from_siblings(s):
        @pl.loop(0, 2 * nz)
        def _(ff):
            from_siblings(s, ff)

    last = 2 * nz - 1

    for fetch in fetches():
        fetch.start()
    if inside:
        at_col = 0
        for v in vectors[:3]:
            packed[:, at_col : at_col + v.shape[1]] = v[...]
            at_col += v.shape[1]
        few = vectors[0].shape[1]
        for k in range(3):
            packed[:, at_col : at_col + few] = vectors[6][k : k + 1, pl.ds(pl.multiple_of(f * few, few), few)]
            at_col += few
        for v in vectors[3:6]:
            packed[:, at_col : at_col + v.shape[1]] = v[...]
            at_col += v.shape[1]
        table[f, t] = packed[...]

    barrier = pltpu.get_barrier_semaphore()
    for m in others():
        pl.semaphore_signal(barrier, inc=1, device_id=member(m), device_id_type=MESH)
    for tt in siblings():
        pl.semaphore_signal(barrier, inc=1, device_id=(r, f, tt), device_id_type=MESH)

    @pl.when(has_lo)
    def _():
        pl.semaphore_signal(barrier, inc=1, device_id=(r, f - 2, t), device_id_type=MESH)

    @pl.when(has_hi)
    def _():
        pl.semaphore_signal(barrier, inc=1, device_id=(r, f + 2, t), device_id_type=MESH)

    pl.semaphore_wait(barrier, G + T - 2 + (z + nz - 1) // nz + (2 * nz - 2 - z) // nz)

    round_stage(0)
    round_stage(1)
    kick(0)
    if inside:
        kick(4)
    kick(1)
    round_stage(2)
    round_stage(3)

    @pl.loop(0, win // TILE)
    def _(i):
        at = pl.ds(pl.multiple_of(i * TILE, TILE), TILE)
        x = tok[pl.ds(pl.multiple_of(start + i * TILE, TILE), TILE), :].astype(f32)
        x = x * lax.rsqrt(jnp.mean(x * x, axis=-1, keepdims=True) + norm_eps) * g1[...]
        nrm[g, at, :] = x.astype(bf16)

    kick2(0)
    if inside:
        kick2(4)
    for m in others():
        copy(nrm.at[g], nrm.at[g], sn.at[m], rn.at[g], member(m)).start()
    kick(2)
    kick2(1)
    steps(0, 1, last)
    if inside:
        steps(4, 1, last)
    kick(3)
    kick2(2)
    steps(1, 1, last)

    all_from_siblings(0)
    for m in others():
        arrived(nrm.at[m], rn.at[m])
    if inside:
        all_from_siblings(4)
        few, ups, outs = vectors[0].shape[1], vectors[3].shape[1], vectors[4].shape[1]
        wide = 3 * vectors[0].shape[1] * 2
        near = 2 * nz // G
        for tt in range(T):
            for j in range(near):
                row_of = table[g * near + j, tt]
                for k in range(3):
                    at_col = (k * near + j) * few
                    asc[tt, :, at_col : at_col + few] = row_of[:, k * few : (k + 1) * few]
                    taps[tt, k : k + 1, j * few : (j + 1) * few] = row_of[:, (3 + k) * few : (4 + k) * few]
                usc[tt, :, j * ups : (j + 1) * ups] = row_of[:, wide : wide + ups]
        for zs in range(nz):
            for yy in range(2):
                row_of = table[2 * zs + yy, 0]
                cols = slice(yy * outs, (yy + 1) * outs)
                oc[zs, :, cols] = row_of[:, wide + ups : wide + ups + outs]
                dc[zs, :, cols] = row_of[:, wide + ups + outs :]
    c = taps.shape[2]

    @pl.loop(0, G)
    def _(gs):
        x = nrm[gs]
        row = lax.broadcasted_iota(jnp.int32, (win, c), 0)
        for tt in range(T):
            prod = jnp.dot(x, WA[tt], preferred_element_type=f32) * asc[tt]
            gated = prod[:, c : 2 * c] * prod[:, :c]
            before = jnp.where(row == 0, 0.0, pltpu.roll(gated, 1, 0))
            after = jnp.where(row == win - 1, 0.0, pltpu.roll(gated, win - 1, 0))
            conv = taps[tt, 0:1] * before + taps[tt, 1:2] * gated + taps[tt, 2:3] * after
            hid[gs, :, tt * c : (tt + 1) * c] = (prod[:, 2 * c :] * conv).astype(bf16)

    all_from_siblings(1)

    @pl.loop(0, nz)
    def _(zs):
        @pl.loop(0, G)
        def _(gs):
            h = hid[gs, pl.ds(off, rows), :]
            for yy in range(2):
                p1[gs, zs, :, yy * cw : (yy + 1) * cw] = jnp.dot(
                    h, WO[2 * zs + yy], preferred_element_type=f32
                ).astype(bf16)

    kick2(3)
    for m in others():
        copy(p1.at[m], q1.at[g], s1.at[m], r1.at[g], member(m)).start()
    cut = (2 * last) // 3
    steps(2, 1, cut)

    for m in others():
        arrived(q1.at[m], r1.at[m])

    def total(p, q, zs, at):
        acc = p[g, zs, at, :].astype(f32)
        for m in others():
            acc = acc + q[m, zs, at, :].astype(f32)
        return acc

    @pl.loop(0, rows // TILE)
    def _(i):
        at = pl.ds(pl.multiple_of(i * TILE, TILE), TILE)
        here = pl.ds(pl.multiple_of(t * rows + i * TILE, TILE), TILE)
        ssq = jnp.zeros((TILE, 1), f32)
        for zs in range(nz):
            m = tok[here, zs * pw : (zs + 1) * pw].astype(f32) + total(p1, q1, zs, at) * oc[zs]
            mid32[zs, at, :] = m
            ssq = ssq + jnp.sum(m * m, axis=-1, keepdims=True)
        inv = lax.rsqrt(ssq / D + norm_eps)
        for zs in range(nz):
            cols = slice(zs * pw, (zs + 1) * pw)
            mid[g, at, cols] = (mid32[zs, at, :] * inv * g2[:, cols]).astype(bf16)

    steps(2, cut, cut + 1)
    for m in others():
        copy(mid.at[g], mid.at[g], sa.at[m], ra.at[g], member(m)).start()
    steps(2, cut + 1, last)
    cut2 = (last + 1) // 2
    steps(3, 1, cut2)

    all_from_siblings(2)
    for m in others():
        arrived(mid.at[m], ra.at[m])
    u = usc.shape[2]

    @pl.loop(0, G)
    def _(gs):
        x = mid[gs]
        for tt in range(T):
            upper = jnp.dot(x, WU[tt], preferred_element_type=f32) * usc[tt]
            act[gs, :, tt * u : (tt + 1) * u] = jnp.square(jnp.maximum(upper, 0.0)).astype(bf16)

    def down(j):
        zs, _ = place(j)

        @pl.when(jnp.logical_and(zs >= 0, zs < nz))
        def _():
            for yy in range(2):
                from_siblings(3, 2 * zs + yy)

            @pl.loop(0, G)
            def _(gs):
                x = act[gs]
                for yy in range(2):
                    p2[gs, zs, :, yy * cw : (yy + 1) * cw] = jnp.dot(
                        x, WD[2 * zs + yy], preferred_element_type=f32
                    ).astype(bf16)

            for m in others():
                copy(p2.at[m, zs], q2.at[g, zs], s2.at[m, zs], r2.at[g, zs], member(m)).start()

    @pl.loop(0, last)
    def _(j):
        @pl.when(j >= cut2)
        def _():
            step(3, j)

        down(j)

    @pl.loop(0, nz)
    def _(zs):
        for m in others():
            arrived(q2.at[m, zs], r2.at[m, zs])

    @pl.loop(0, rows // TILE)
    def _(i):
        at = pl.ds(pl.multiple_of(i * TILE, TILE), TILE)
        here = pl.ds(pl.multiple_of(t * rows + i * TILE, TILE), TILE)
        for zs in range(nz):
            out[here, zs * pw : (zs + 1) * pw] = (
                mid32[zs, at, :] + total(p2, q2, zs, at) * dc[zs]
            ).astype(bf16)

    def half(tt):
        return out.at[pl.ds(pl.multiple_of(tt * rows, rows), rows)]

    for tt in siblings():
        copy(half(t), half(t), so.at[tt], ro.at[t], (r, f, tt)).start()

    for s in stages:
        own = slot(s, f, t)
        arrived(own, sy.at[s])

        def gone(ff, k, s=s, own=own):
            arrived(own, sz.at[s, ff, k])

        for ff in (f, fy):
            pl.when(has_lo)(functools.partial(gone, ff, 0))
            pl.when(has_hi)(functools.partial(gone, ff, 1))

        @pl.loop(1, last)
        def _(j):
            zs, nxt = place(j)
            ok = jnp.logical_and(zs >= 0, zs < nz)

            @pl.when(jnp.logical_and(ok, jnp.logical_and(nxt >= 0, nxt < nz)))
            def _():
                for yy in range(2):
                    gone(2 * zs + yy, 0)

        @pl.loop(0, 2 * nz)
        def _(ff):
            for _ in siblings():
                arrived(own, sd.at[s, ff])

    for m in others():
        arrived(nrm.at[m], sn.at[m])
        arrived(p1.at[m], s1.at[m])
        arrived(mid.at[m], sa.at[m])

        @pl.loop(0, nz)
        def _(zs):
            arrived(p2.at[m, zs], s2.at[m, zs])

    for tt in siblings():
        arrived(half(tt), ro.at[tt])
        arrived(half(tt), so.at[tt])

def line_kernel(
    nz, G, T, win, rows, inside,
    tok, g1, g2, vectors, weights,
    out,
    WA, WO, WU, WD, nrm, hid, p, q, mid32, mid, act,
    staged, leaving, gathered,
    rz, rd, re, sz, sd, sy, loc, rn, sn, r1, s1, ra, sa, r2, s2, ro, so,
):
    if inside:
        packed, table, asc, taps, usc, oc, dc = gathered
    else:
        asc, taps, usc, oc, dc = vectors
    D = tok.shape[1]
    pw = D // nz
    cw = pw // 2
    r, f, t = lax.axis_index("rep"), lax.axis_index("fs"), lax.axis_index("tp")
    z, y = f // 2, f % 2
    fy = z * 2 + 1 - y
    g = r * 2 + y
    ka, ko, ku, kd = (w.shape[0] for w in leaving)
    stages = range(5 if inside else 4)
    has_lo, has_hi = z > 0, z < nz - 1
    outer = jnp.logical_or(z == 0, z == nz - 1)
    inner = jnp.logical_not(outer)
    inward = jnp.where(2 * z < nz, 1, -1)
    across = z + 2 * inward
    if T == 2:
        start, off = t * (rows - HALO), t * HALO
    else:
        start = jnp.clip(t * rows - HALO, 0, tok.shape[0] - win)
        off = t * rows - start
    start, off = pl.multiple_of(start, HALO), pl.multiple_of(off, HALO)

    def member(m):
        return (m // 2, z * 2 + m % 2, t)

    def others():
        return [(g + d) % G for d in range(1, G)]

    gx, gy, gd = (1 - r) * 2 + y, r * 2 + 1 - y, (1 - r) * 2 + 1 - y

    def peers():
        return [gd, gx, gy]

    def siblings():
        return [(t + d) % T for d in range(1, T)]

    def copy(src, dst, ssem, rsem, dev):
        return pltpu.make_async_remote_copy(
            src_ref=src, dst_ref=dst, send_sem=ssem, recv_sem=rsem, device_id=dev, device_id_type=MESH
        )

    def arrived(ref, sem):
        pltpu.make_async_copy(ref, ref, sem).wait()

    def slot(s, ff, tt):
        if s == 0:
            return WA.at[tt, pl.ds(pl.multiple_of(ff * ka, ka), ka)]
        if s == 1:
            return WO.at[ff, pl.ds(pl.multiple_of(tt * ko, ko), ko)]
        if s == 2:
            return WU.at[tt, pl.ds(pl.multiple_of(ff * ku, ku), ku)]
        if s == 3:
            return WD.at[ff, pl.ds(pl.multiple_of(tt * kd, kd), kd)]
        return table.at[ff, tt]

    def to_siblings(s, ff, src):
        for tt in siblings():
            copy(src, slot(s, ff, t), sd.at[s], rd.at[s // 2, ff] if s % 2 else re.at[s // 2], (r, f, tt)).start()

    def both_ways(s, ff, src):
        @pl.when(has_lo)
        def _():
            copy(src, slot(s, ff, t), sz.at[s], rz.at[s, ff], (r, f - 2, t)).start()

        @pl.when(has_hi)
        def _():
            copy(src, slot(s, ff, t), sz.at[s], rz.at[s, ff], (r, f + 2, t)).start()

        @pl.when(outer)
        def _():
            copy(src, slot(s, ff, t), sz.at[s], rz.at[s, ff], (r, 2 * across + y, t)).start()

    def fetches():
        for i, w in enumerate(weights):
            src, dst = weights[i], staged[i]
            if w.shape[1] > dst.shape[1]:
                n = dst.shape[1]
                src = src.at[:, pl.ds(pl.multiple_of(r * n, n), n)]
            elif w.shape[0] > dst.shape[0]:
                n = dst.shape[0]
                src = src.at[pl.ds(pl.multiple_of(r * n, n), n)]
            yield pltpu.make_async_copy(src, dst, loc.at[i])

    def round_stage(s):
        parts = {0: (0, 1, 2), 1: (3,), 2: (4,), 3: (5,)}[s]
        high = leaving[s].shape[0]
        for i in parts:
            pltpu.make_async_copy(staged[i], staged[i], loc.at[i]).wait()
        for yy in range(2):

            @pl.when(y == yy)
            def _():
                @pl.loop(0, high // 32)
                def _(k):
                    at = pl.ds(pl.multiple_of(k * 32, 32), 32)
                    for n, i in enumerate(parts):
                        if s in (0, 2):
                            wide = staged[i].shape[1] // 2
                            mine = staged[i][at, yy * wide : (yy + 1) * wide]
                            theirs = staged[i][at, (1 - yy) * wide : (2 - yy) * wide]
                        else:
                            wide = staged[i].shape[1]
                            mine = staged[i][pl.ds(pl.multiple_of(yy * high + k * 32, 32), 32), :]
                            theirs = staged[i][pl.ds(pl.multiple_of((1 - yy) * high + k * 32, 32), 32), :]
                        cols = slice(n * wide, (n + 1) * wide)
                        leaving[s][at, cols] = theirs.astype(bf16)
                        if s == 0:
                            WA[t, pl.ds(pl.multiple_of(f * ka + k * 32, 32), 32), cols] = mine.astype(bf16)
                        elif s == 1:
                            WO[f, pl.ds(pl.multiple_of(t * ko + k * 32, 32), 32), :] = mine.astype(bf16)
                        elif s == 2:
                            WU[t, pl.ds(pl.multiple_of(f * ku + k * 32, 32), 32), :] = mine.astype(bf16)
                        else:
                            WD[f, pl.ds(pl.multiple_of(t * kd + k * 32, 32), 32), :] = mine.astype(bf16)

    def swap(s):
        own = slot(s, f, t)
        copy(leaving[s] if s < 4 else own, own, sy.at[s], rz.at[s, f], (r, fy, t)).start()
        to_siblings(s, f, own)

    def spread(s):
        both_ways(s, f, slot(s, f, t))

    def kick2(s):
        arrived(slot(s, fy, t), rz.at[s, fy])
        both_ways(s, fy, slot(s, fy, t))
        to_siblings(s, fy, slot(s, fy, t))

    def place(j):
        return (z + inward * j + nz) % nz

    def relayed(zs):
        return jnp.logical_and(inner, zs != z - inward)

    blocks = 2 * (nz - 1)

    def block(i):
        first, rest = i < 2, jnp.maximum(i - 2, 0)
        near_out, late_out = jnp.where(first, 1, 2 + rest % 2), jnp.where(first, i, rest // 2)
        near_in, late_in = jnp.where(i < 4, 1 + i % 2, nz - 1), jnp.where(i < 4, i // 2, i % 2)
        near, late = jnp.where(inner, near_in, near_out), jnp.where(inner, late_in, late_out)
        return place(near), (y + late) % 2

    def step(s, i):
        zs, yy = block(i)
        ff = 2 * zs + yy
        arrived(slot(s, ff, t), rz.at[s, ff])

        @pl.when(relayed(zs))
        def _():
            copy(
                slot(s, ff, t), slot(s, ff, t), sz.at[s], rz.at[s, ff], (r, 2 * (z - inward) + y, t)
            ).start()

        to_siblings(s, ff, slot(s, ff, t))

    def steps(s, lo, hi):
        @pl.loop(lo, hi)
        def _(j):
            step(s, j)

    def from_siblings(s, ff):
        for tt in siblings():
            arrived(slot(s, ff, tt), rd.at[s // 2, ff])

    def part_of(s, tt, n):
        if s == 0:
            return WA.at[tt, pl.ds(0, n * ka)]
        if s == 1:
            return WO.at[pl.ds(0, n), pl.ds(pl.multiple_of(tt * ko, ko), ko)]
        if s == 2:
            return WU.at[tt, pl.ds(0, n * ku)]
        if s == 3:
            return WD.at[pl.ds(0, n), pl.ds(pl.multiple_of(tt * kd, kd), kd)]
        return table.at[pl.ds(0, n), tt]

    def all_from_siblings(s):
        for tt in siblings():
            arrived(part_of(s, tt, 2 * nz), re.at[s // 2])

    for fetch in fetches():
        fetch.start()
    if inside:
        at_col = 0
        for v in vectors[:3]:
            packed[:, at_col : at_col + v.shape[1]] = v[...]
            at_col += v.shape[1]
        few = vectors[0].shape[1]
        for k in range(3):
            packed[:, at_col : at_col + few] = vectors[6][k : k + 1, pl.ds(pl.multiple_of(f * few, few), few)]
            at_col += few
        for v in vectors[3:6]:
            for k in range(v.shape[0]):
                packed[:, at_col : at_col + v.shape[1]] = v[k : k + 1, :]
                at_col += v.shape[1]
        table[f, t] = packed[...]

    barrier = pltpu.get_barrier_semaphore()
    for m in others():
        pl.semaphore_signal(barrier, inc=1, device_id=member(m), device_id_type=MESH)
    for tt in siblings():
        pl.semaphore_signal(barrier, inc=1, device_id=(r, f, tt), device_id_type=MESH)

    for zs in (z - 1, z + 1, across):
        near = jnp.logical_and(zs >= 0, zs < nz)

        @pl.when(jnp.logical_and(near, zs != z))
        def _():
            pl.semaphore_signal(barrier, inc=1, device_id=(r, 2 * zs + y, t), device_id_type=MESH)

    round_stage(0)
    round_stage(1)

    pl.semaphore_wait(barrier, G + T - 2 + jnp.where(outer, 2, 3))
    early = (0, 4, 1) if inside else (0, 1)
    for s in early:
        swap(s)
        spread(s)
    round_stage(2)
    round_stage(3)

    @pl.loop(0, win // TILE)
    def _(i):
        at = pl.ds(pl.multiple_of(i * TILE, TILE), TILE)
        x = tok[pl.ds(pl.multiple_of(start + i * TILE, TILE), TILE), :].astype(f32)
        x = x * lax.rsqrt(jnp.mean(x * x, axis=-1, keepdims=True) + norm_eps) * g1[...]
        nrm[g, at, :] = x.astype(bf16)

    for s in early:
        kick2(s)
    for m in (gx, gy):
        copy(nrm.at[g], nrm.at[g], sn, rn.at[g], member(m)).start()
    for s in (2, 3):
        swap(s)

    @pl.when(outer)
    def _():
        spread(2)

    steps(0, 0, 2)

    arrived(nrm.at[gy], rn.at[gy])
    copy(nrm.at[gy], nrm.at[gy], sn, rn.at[gy], member(gx)).start()

    steps(0, 2, 4)

    @pl.when(outer)
    def _():
        kick2(2)
        spread(3)

    steps(0, 4, blocks)

    @pl.when(outer)
    def _():
        kick2(3)

    if inside:
        steps(4, 0, blocks)

    @pl.when(inner)
    def _():
        steps(1, 0, blocks)
        spread(2)
        kick2(2)

    all_from_siblings(0)
    if inside:
        all_from_siblings(4)

    for m in (gx, gd):
        arrived(nrm.at[m], rn.at[m])
    if inside:
        few, ups, outs = vectors[0].shape[1], vectors[3].size, vectors[4].shape[1]
        wide = 3 * vectors[0].shape[1] * 2
        near = 2 * nz // G
        for tt in range(T):
            for j in range(near):
                row_of = table[g * near + j, tt]
                for k in range(3):
                    at_col = (k * near + j) * few
                    asc[tt, :, at_col : at_col + few] = row_of[:, k * few : (k + 1) * few]
                    taps[tt, k : k + 1, j * few : (j + 1) * few] = row_of[:, (3 + k) * few : (4 + k) * few]
                usc[tt, :, j * ups : (j + 1) * ups] = row_of[:, wide : wide + ups]
        for zs in range(nz):
            for yy in range(2):
                row_of = table[2 * zs + yy, 0]
                cols = slice(yy * outs, (yy + 1) * outs)
                oc[zs, :, cols] = row_of[:, wide + ups : wide + ups + outs]
                dc[zs, :, cols] = row_of[:, wide + ups + outs :]
    c = taps.shape[2]

    @pl.loop(0, G)
    def _(gs):
        x = nrm[gs]
        row = lax.broadcasted_iota(jnp.int32, (win, c), 0)
        for tt in range(T):
            prod = jnp.dot(x, WA[tt], preferred_element_type=f32) * asc[tt]
            gated = prod[:, c : 2 * c] * prod[:, :c]
            before = jnp.where(row == 0, 0.0, pltpu.roll(gated, 1, 0))
            after = jnp.where(row == win - 1, 0.0, pltpu.roll(gated, win - 1, 0))
            conv = taps[tt, 0:1] * before + taps[tt, 1:2] * gated + taps[tt, 2:3] * after
            hid[gs, :, tt * c : (tt + 1) * c] = (prod[:, 2 * c :] * conv).astype(bf16)

    def pair(ref, i, zs):
        return ref.at[i, pl.ds(2 * zs, 2)]

    def legs(zs):
        even = zs % 2 == 0
        return jnp.where(even, gx, gy), jnp.where(even, gy, gx)

    @pl.loop(0, nz)
    def _(j):
        zs = place(j)

        @pl.when(outer & (j > 0) & (j < nz - 1))
        def _():
            steps(1, jnp.where(j == 1, 0, 3), jnp.where(j == 1, 3, blocks))

        for yy in range(2):
            from_siblings(1, 2 * zs + yy)

        @pl.loop(0, G)
        def _(gs):
            h = hid[gs, pl.ds(off, rows), :]
            for yy in range(2):
                p[gs, 2 * zs + yy] = jnp.dot(h, WO[2 * zs + yy], preferred_element_type=f32).astype(bf16)

        first, _ = legs(zs)
        copy(pair(p, gd, zs), pair(q, 1, zs), s1, r1.at[1, zs], member(first)).start()
        copy(pair(p, first, zs), pair(q, 0, zs), s1, r1.at[0, zs], member(first)).start()

    @pl.loop(0, nz)
    def _(j):
        zs = place(j)
        _, second = legs(zs)
        arrived(pair(q, 1, zs), r1.at[1, zs])

        @pl.loop(0, rows // TILE)
        def _(k):
            at = pl.ds(pl.multiple_of(k * TILE, TILE), TILE)
            for yy in range(2):
                both = p[second, 2 * zs + yy, at, :].astype(f32) + q[1, 2 * zs + yy, at, :].astype(f32)
                p[second, 2 * zs + yy, at, :] = both.astype(bf16)

        copy(pair(p, second, zs), pair(q, 2, zs), s1, r1.at[2, zs], member(second)).start()

    cut = jnp.where(inner, blocks, 2)
    steps(2, 0, cut)

    @pl.when(inner)
    def _():
        spread(3)
        kick2(3)

    @pl.loop(0, nz)
    def _(zs):
        for i in (0, 2):
            arrived(pair(q, i, zs), r1.at[i, zs])

    @pl.loop(0, rows // TILE)
    def _(i):
        at = pl.ds(pl.multiple_of(i * TILE, TILE), TILE)
        here = pl.ds(pl.multiple_of(t * rows + i * TILE, TILE), TILE)
        ssq = jnp.zeros((TILE, 1), f32)
        for ff in range(2 * nz):
            half = slice(ff % 2 * cw, (ff % 2 + 1) * cw)
            acc = p[g, ff, at, :].astype(f32) + q[0, ff, at, :].astype(f32) + q[2, ff, at, :].astype(f32)
            m = tok[here, ff * cw : (ff + 1) * cw].astype(f32) + acc * oc[ff // 2, :, half]
            mid32[ff // 2, at, half] = m
            ssq = ssq + jnp.sum(m * m, axis=-1, keepdims=True)
        inv = lax.rsqrt(ssq / D + norm_eps)
        for zs in range(nz):
            cols = slice(zs * pw, (zs + 1) * pw)
            mid[g, at, cols] = (mid32[zs, at, :] * inv * g2[:, cols]).astype(bf16)

    for m in (gx, gy):
        copy(mid.at[g], mid.at[g], sa, ra.at[g], member(m)).start()

    cut1 = jnp.where(inner, blocks, 4)
    steps(2, cut, cut1)

    part = rows // 2
    for m, n, lo in ((gx, gy, part), (gy, gx, 0)):
        arrived(mid.at[m], ra.at[m])
        some = mid.at[m, pl.ds(lo, part)]
        copy(some, some, sa, ra.at[m] if lo else ra.at[G], member(n)).start()

    steps(2, cut1, blocks)

    cut2 = jnp.where(inner, blocks, 0)
    steps(3, 0, cut2)

    all_from_siblings(2)

    some = mid.at[gd, pl.ds(0, part)]
    arrived(some, ra.at[gd])
    arrived(some, ra.at[G])

    u = usc.shape[2]
    arrived(p.at[pl.ds(0, G - 1)], s1)

    @pl.loop(0, G)
    def _(gs):
        x = mid[gs]
        for tt in range(T):
            upper = jnp.dot(x, WU[tt], preferred_element_type=f32) * usc[tt]
            act[gs, :, tt * u : (tt + 1) * u] = jnp.square(jnp.maximum(upper, 0.0)).astype(bf16)

    def source(i):
        zs, yy = block(jnp.maximum(i - 2, 0))
        zs, yy = jnp.where(i < 2, z, zs), jnp.where(i < 2, (y + i) % 2, yy)
        return zs, yy, 2 * zs + yy

    def finish(i):
        zs, yy, ff = source(i)
        for m in range(G - 1):
            arrived(q.at[m, ff], r2.at[m, ff])
        wide = pl.ds(pl.multiple_of(yy * cw, cw), cw)
        cols = pl.ds(pl.multiple_of(ff * cw, cw), cw)

        @pl.loop(0, rows // TILE)
        def _(k):
            at = pl.ds(pl.multiple_of(k * TILE, TILE), TILE)
            acc = p[g, ff, at, :].astype(f32)
            for m in range(G - 1):
                acc = acc + q[m, ff, at, :].astype(f32)
            here = pl.ds(pl.multiple_of(t * rows + k * TILE, TILE), TILE)
            out[here, cols] = (mid32[zs, at, wide] + acc * dc[zs, :, wide]).astype(bf16)

        mine = out.at[pl.ds(pl.multiple_of(t * rows, rows), rows), cols]
        for tt in siblings():
            copy(mine, mine, so, ro, (r, f, tt)).start()

    @pl.loop(0, 2 * nz)
    def _(ff_at):
        _, _, ff = source(ff_at)

        @pl.when(outer & (ff_at > 1))
        def _():
            step(3, ff_at - 2)

        from_siblings(3, ff)

        @pl.loop(0, G)
        def _(gs):
            p[gs, ff] = jnp.dot(act[gs], WD[ff], preferred_element_type=f32).astype(bf16)

        for i, m in enumerate(peers()):
            copy(p.at[m, ff], q.at[i, ff], s2, r2.at[i, ff], member(m)).start()

        @pl.when(ff_at > 2)
        def _():
            finish(ff_at - 3)

    @pl.loop(2 * nz - 3, 2 * nz)
    def _(i):
        finish(i)

    for s in stages:
        arrived(slot(s, f, t), sy.at[s])
        arrived(part_of(s, t, nz), sz.at[s])

        @pl.when(inner)
        def _():
            arrived(part_of(s, t, nz), sz.at[s])

        for _ in siblings():
            arrived(part_of(s, t, 2 * nz), sd.at[s])

    arrived(nrm.at[pl.ds(0, G - 1)], sn)
    arrived(mid.at[pl.ds(0, G - 1)], sa)
    arrived(p.at[pl.ds(0, G - 1)], s2)
    half = out.at[pl.ds(0, rows)]
    for _ in siblings():
        arrived(half, ro)
        arrived(half, so)

def body(
    R, n_fs, T,
    tokens, mix_gain, value_weight, value_scale, inner_weight, inner_scale, outer_weight, outer_scale,
    conv_taps, out_weight, out_scale, mlp_gain, up_weight, up_scale, down_weight, down_scale,
):
    G, nz = 2 * R, n_fs // 2
    lined = T == 2 and nz == 4 and R == 2
    TOK, D = tokens.shape[1:]
    rows = TOK // T
    win = TOK if T == 1 else rows + HALO if T == 2 else rows + 2 * HALO
    r, f = lax.axis_index("rep"), lax.axis_index("fs")
    g = r * 2 + f % 2

    vs, us, os = value_scale.shape[0], up_scale.shape[0], out_scale.shape[0]
    inside = all(n % 128 == 0 for n in (vs, us, os))
    c, u = conv_taps.shape[1] // G, up_weight.shape[1] // G
    if inside:
        scales = (value_scale, inner_scale, outer_scale, up_scale, out_scale, down_scale)
        wide = 128 if lined else us
        vectors = tuple(v.reshape(-1, wide) if v is up_scale else v[None] for v in scales) + (conv_taps,)
    else:
        tap = lax.dynamic_slice_in_dim(conv_taps, f * vs, vs, axis=1)
        packed = jnp.concatenate(
            [value_scale, inner_scale, outer_scale, tap[0], tap[1], tap[2], up_scale, out_scale, down_scale]
        )
        every = lax.all_gather(packed, ("tp", "fs"), axis=0, tiled=False).reshape(T, n_fs, -1)

        def block(v):
            return lax.dynamic_index_in_dim(v.reshape(T, G, -1), g, axis=1, keepdims=True)

        small = [block(every[:, :, i * vs : (i + 1) * vs]) for i in range(6)]
        asc = jnp.concatenate(small[:3], axis=2)
        taps = jnp.concatenate(small[3:], axis=1)
        usc = block(every[:, :, 6 * vs : 6 * vs + us])
        oc = every[0, :, 6 * vs + us : 6 * vs + us + os].reshape(nz, 1, -1)
        dc = every[0, :, 6 * vs + us + os :].reshape(nz, 1, -1)
        vectors = (asc, taps, usc, oc, dc)
    weights = (value_weight, inner_weight, outer_weight, out_weight, up_weight, down_weight)
    ka, ko, kd = value_weight.shape[0], out_weight.shape[0] // G, down_weight.shape[0] // G
    cw = out_weight.shape[1]
    rounded = [(ka, 3 * c), (ko, cw), (ka, u), (kd, cw)]
    staged = [(ka, 2 * c)] * 3 + [(2 * ko, cw), (ka, 2 * u), (2 * kd, cw)]
    gathered = ()
    if inside:
        L = 6 * vs + us + 2 * os
        small = [(1, L), (n_fs, T, 1, L), (T, 1, 3 * c), (T, 3, c), (T, 1, u), (nz, 1, 2 * cw), (nz, 1, 2 * cw)]
        gathered = tuple(pltpu.VMEM(shape, f32) for shape in small)
    pw = D // nz
    dma = pltpu.SemaphoreType.DMA
    vmem = pl.BlockSpec(memory_space=pltpu.VMEM)
    hbm = pl.BlockSpec(memory_space=pl.ANY)
    held = [
        pltpu.VMEM((T, D, 3 * c), bf16),
        pltpu.VMEM((n_fs, T * ko, cw), bf16),
        pltpu.VMEM((T, D, u), bf16),
        pltpu.VMEM((n_fs, T * kd, cw), bf16),
        pltpu.VMEM((G, win, D), bf16),
        pltpu.VMEM((G, win, T * ko), bf16),
    ]
    reading = [
        tuple(pltpu.VMEM(shape, f32) for shape in staged),
        tuple(pltpu.VMEM(shape, bf16) for shape in rounded),
        gathered,
    ]
    if lined:
        run = line_kernel
        limit = 65000000
        scratch = [
            *held,
            pltpu.VMEM((G, n_fs, rows, cw), bf16),
            pltpu.VMEM((G - 1, n_fs, rows, cw), bf16),
            pltpu.VMEM((nz, rows, pw), f32),
            pltpu.VMEM((G, rows, D), bf16),
            pltpu.VMEM((G, rows, T * kd), bf16),
            *reading,
            dma((5, n_fs)),
            dma((2, n_fs)),
            dma((3,)),
            dma((5,)),
            dma((5,)),
            dma((5,)),
            dma((6,)),
            dma((G,)),
            dma,
            dma((G - 1, nz)),
            dma,
            dma((G + 1,)),
            dma,
            dma((G - 1, n_fs)),
            dma,
            dma,
            dma,
        ]
    else:
        run = kernel
        limit = 65000000
        scratch = [
            *held,
            pltpu.VMEM((G, nz, rows, pw), bf16),
            pltpu.VMEM((G, nz, rows, pw), bf16),
            pltpu.VMEM((nz, rows, pw), f32),
            pltpu.VMEM((G, rows, D), bf16),
            pltpu.VMEM((G, rows, T * kd), bf16),
            pltpu.VMEM((G, nz, rows, pw), bf16),
            pltpu.VMEM((G, nz, rows, pw), bf16),
            *reading,
            dma((5, n_fs)),
            dma((5, n_fs)),
            dma((5, n_fs, 2)),
            dma((5, n_fs)),
            dma((5,)),
            dma((6,)),
            dma((G,)),
            dma((G,)),
            dma((G,)),
            dma((G,)),
            dma((G,)),
            dma((G,)),
            dma((G, nz)),
            dma((G, nz)),
            dma((T,)),
            dma((T,)),
        ]
    result = pl.pallas_call(
        functools.partial(run, nz, G, T, win, rows, inside),
        out_shape=jax.ShapeDtypeStruct((TOK, D), bf16),
        in_specs=[vmem] * 3 + [(vmem,) * len(vectors), (hbm,) * 6],
        out_specs=vmem,
        scratch_shapes=scratch,
        compiler_params=pltpu.CompilerParams(collective_id=0, has_side_effects=True, vmem_limit_bytes=limit),
    )(tokens[0], mix_gain[None], mlp_gain[None], vectors, weights)
    return result[None]

def solution(mesh):
    placed = (
        P(("rep", "fs"), None, None),
        P(),
        P("fs", "tp"),
        P(("tp", "fs")),
        P("fs", "tp"),
        P(("tp", "fs")),
        P("fs", "tp"),
        P(("tp", "fs")),
        P(None, "tp"),
        P("tp", "fs"),
        P("fs"),
        P(),
        P("fs", "tp"),
        P(("tp", "fs")),
        P("tp", "fs"),
        P("fs"),
    )
    sizes = (mesh.shape["rep"], mesh.shape["fs"], mesh.shape["tp"])
    return jax.shard_map(
        functools.partial(body, *sizes),
        mesh=mesh,
        in_specs=placed,
        out_specs=P(("rep", "fs"), None, None),
        check_vma=False,
    )
```

```python
import functools

import jax
import jax.numpy as jnp
from jax import lax
from jax.experimental import pallas as pl
from jax.experimental.pallas import tpu as pltpu
from jax.sharding import PartitionSpec as P

MESH = pl.DeviceIdType.MESH
norm_eps = 1e-06
HALO = 16
TILE = 16
f32 = jnp.float32
bf16 = jnp.bfloat16

def kernel(
    nz, G, T, win, rows, inside,
    tok, g1, g2, vectors, weights,
    out,
    WA, WO, WU, WD, nrm, hid, p1, q1, mid32, mid, act, p2, q2,
    staged, leaving, gathered,
    rz, rd, sz, sd, sy, loc, rn, sn, r1, s1, ra, sa, r2, s2, ro, so,
):
    if inside:
        packed, table, asc, taps, usc, oc, dc = gathered
    else:
        asc, taps, usc, oc, dc = vectors
    D = tok.shape[1]
    pw = D // nz
    cw = pw // 2
    r, f, t = lax.axis_index("rep"), lax.axis_index("fs"), lax.axis_index("tp")
    z, y = f // 2, f % 2
    fy = z * 2 + 1 - y
    g = r * 2 + y
    ka, ko, ku, kd = (w.shape[0] for w in leaving)
    stages = range(5 if inside else 4)
    has_lo, has_hi = z > 0, z < nz - 1
    if T == 2:
        start, off = t * (rows - HALO), t * HALO
    else:
        start = jnp.clip(t * rows - HALO, 0, tok.shape[0] - win)
        off = t * rows - start
    start, off = pl.multiple_of(start, HALO), pl.multiple_of(off, HALO)

    def member(m):
        return (m // 2, z * 2 + m % 2, t)

    def others():
        return [(g + d) % G for d in range(1, G)]

    def siblings():
        return [(t + d) % T for d in range(1, T)]

    def copy(src, dst, ssem, rsem, dev):
        return pltpu.make_async_remote_copy(
            src_ref=src, dst_ref=dst, send_sem=ssem, recv_sem=rsem, device_id=dev, device_id_type=MESH
        )

    def arrived(ref, sem):
        pltpu.make_async_copy(ref, ref, sem).wait()

    def slot(s, ff, tt):
        if s == 0:
            return WA.at[tt, pl.ds(pl.multiple_of(ff * ka, ka), ka)]
        if s == 1:
            return WO.at[ff, pl.ds(pl.multiple_of(tt * ko, ko), ko)]
        if s == 2:
            return WU.at[tt, pl.ds(pl.multiple_of(ff * ku, ku), ku)]
        if s == 3:
            return WD.at[ff, pl.ds(pl.multiple_of(tt * kd, kd), kd)]
        return table.at[ff, tt]

    def to_siblings(s, ff, src):
        for tt in siblings():
            copy(src, slot(s, ff, t), sd.at[s, ff], rd.at[s, ff], (r, f, tt)).start()

    def both_ways(s, ff, src):
        @pl.when(has_lo)
        def _():
            copy(src, slot(s, ff, t), sz.at[s, ff, 0], rz.at[s, ff], (r, f - 2, t)).start()

        @pl.when(has_hi)
        def _():
            copy(src, slot(s, ff, t), sz.at[s, ff, 1], rz.at[s, ff], (r, f + 2, t)).start()

    def fetches():
        for i, w in enumerate(weights):
            src, dst = weights[i], staged[i]
            if w.shape[1] > dst.shape[1]:
                n = dst.shape[1]
                src = src.at[:, pl.ds(pl.multiple_of(r * n, n), n)]
            elif w.shape[0] > dst.shape[0]:
                n = dst.shape[0]
                src = src.at[pl.ds(pl.multiple_of(r * n, n), n)]
            yield pltpu.make_async_copy(src, dst, loc.at[i])

    def round_stage(s):
        parts = {0: (0, 1, 2), 1: (3,), 2: (4,), 3: (5,)}[s]
        high = leaving[s].shape[0]
        for i in parts:
            pltpu.make_async_copy(staged[i], staged[i], loc.at[i]).wait()
        for yy in range(2):

            @pl.when(y == yy)
            def _():
                @pl.loop(0, high // 32)
                def _(k):
                    at = pl.ds(pl.multiple_of(k * 32, 32), 32)
                    for n, i in enumerate(parts):
                        if s in (0, 2):
                            wide = staged[i].shape[1] // 2
                            mine = staged[i][at, yy * wide : (yy + 1) * wide]
                            theirs = staged[i][at, (1 - yy) * wide : (2 - yy) * wide]
                        else:
                            wide = staged[i].shape[1]
                            mine = staged[i][pl.ds(pl.multiple_of(yy * high + k * 32, 32), 32), :]
                            theirs = staged[i][pl.ds(pl.multiple_of((1 - yy) * high + k * 32, 32), 32), :]
                        cols = slice(n * wide, (n + 1) * wide)
                        leaving[s][at, cols] = theirs.astype(bf16)
                        if s == 0:
                            WA[t, pl.ds(pl.multiple_of(f * ka + k * 32, 32), 32), cols] = mine.astype(bf16)
                        elif s == 1:
                            WO[f, pl.ds(pl.multiple_of(t * ko + k * 32, 32), 32), :] = mine.astype(bf16)
                        elif s == 2:
                            WU[t, pl.ds(pl.multiple_of(f * ku + k * 32, 32), 32), :] = mine.astype(bf16)
                        else:
                            WD[f, pl.ds(pl.multiple_of(t * kd + k * 32, 32), 32), :] = mine.astype(bf16)

    def kick(s):
        own = slot(s, f, t)
        copy(leaving[s] if s < 4 else own, own, sy.at[s], rz.at[s, f], (r, fy, t)).start()
        both_ways(s, f, own)
        to_siblings(s, f, own)

    def kick2(s):
        arrived(slot(s, fy, t), rz.at[s, fy])
        both_ways(s, fy, slot(s, fy, t))
        to_siblings(s, fy, slot(s, fy, t))

    def place(j):
        k = (j + 1) // 2
        sg = 1 - 2 * (j % 2)
        return z + sg * k, z - sg

    def step(s, j):
        zs, nxt = place(j)

        @pl.when(jnp.logical_and(zs >= 0, zs < nz))
        def _():
            for yy in range(2):
                ff = 2 * zs + yy
                arrived(slot(s, ff, t), rz.at[s, ff])

                @pl.when(jnp.logical_and(nxt >= 0, nxt < nz))
                def _():
                    copy(
                        slot(s, ff, t), slot(s, ff, t), sz.at[s, ff, 0], rz.at[s, ff], (r, 2 * nxt + y, t)
                    ).start()

                to_siblings(s, ff, slot(s, ff, t))

    def steps(s, lo, hi):
        @pl.loop(lo, hi)
        def _(j):
            step(s, j)

    def from_siblings(s, ff):
        for tt in siblings():
            arrived(slot(s, ff, tt), rd.at[s, ff])

    def all_from_siblings(s):
        @pl.loop(0, 2 * nz)
        def _(ff):
            from_siblings(s, ff)

    last = 2 * nz - 1

    for fetch in fetches():
        fetch.start()
    if inside:
        at_col = 0
        for v in vectors[:3]:
            packed[:, at_col : at_col + v.shape[1]] = v[...]
            at_col += v.shape[1]
        few = vectors[0].shape[1]
        for k in range(3):
            packed[:, at_col : at_col + few] = vectors[6][k : k + 1, pl.ds(pl.multiple_of(f * few, few), few)]
            at_col += few
        for v in vectors[3:6]:
            packed[:, at_col : at_col + v.shape[1]] = v[...]
            at_col += v.shape[1]
        table[f, t] = packed[...]

    barrier = pltpu.get_barrier_semaphore()
    for m in others():
        pl.semaphore_signal(barrier, inc=1, device_id=member(m), device_id_type=MESH)
    for tt in siblings():
        pl.semaphore_signal(barrier, inc=1, device_id=(r, f, tt), device_id_type=MESH)

    @pl.when(has_lo)
    def _():
        pl.semaphore_signal(barrier, inc=1, device_id=(r, f - 2, t), device_id_type=MESH)

    @pl.when(has_hi)
    def _():
        pl.semaphore_signal(barrier, inc=1, device_id=(r, f + 2, t), device_id_type=MESH)

    pl.semaphore_wait(barrier, G + T - 2 + (z + nz - 1) // nz + (2 * nz - 2 - z) // nz)

    round_stage(0)
    round_stage(1)
    kick(0)
    if inside:
        kick(4)
    kick(1)
    round_stage(2)
    round_stage(3)

    @pl.loop(0, win // TILE)
    def _(i):
        at = pl.ds(pl.multiple_of(i * TILE, TILE), TILE)
        x = tok[pl.ds(pl.multiple_of(start + i * TILE, TILE), TILE), :].astype(f32)
        x = x * lax.rsqrt(jnp.mean(x * x, axis=-1, keepdims=True) + norm_eps) * g1[...]
        nrm[g, at, :] = x.astype(bf16)

    kick2(0)
    if inside:
        kick2(4)
    for m in others():
        copy(nrm.at[g], nrm.at[g], sn.at[m], rn.at[g], member(m)).start()
    kick(2)
    kick2(1)
    steps(0, 1, last)
    if inside:
        steps(4, 1, last)
    kick(3)
    kick2(2)
    steps(1, 1, last)

    all_from_siblings(0)
    for m in others():
        arrived(nrm.at[m], rn.at[m])
    if inside:
        all_from_siblings(4)
        few, ups, outs = vectors[0].shape[1], vectors[3].shape[1], vectors[4].shape[1]
        wide = 3 * vectors[0].shape[1] * 2
        near = 2 * nz // G
        for tt in range(T):
            for j in range(near):
                row_of = table[g * near + j, tt]
                for k in range(3):
                    at_col = (k * near + j) * few
                    asc[tt, :, at_col : at_col + few] = row_of[:, k * few : (k + 1) * few]
                    taps[tt, k : k + 1, j * few : (j + 1) * few] = row_of[:, (3 + k) * few : (4 + k) * few]
                usc[tt, :, j * ups : (j + 1) * ups] = row_of[:, wide : wide + ups]
        for zs in range(nz):
            for yy in range(2):
                row_of = table[2 * zs + yy, 0]
                cols = slice(yy * outs, (yy + 1) * outs)
                oc[zs, :, cols] = row_of[:, wide + ups : wide + ups + outs]
                dc[zs, :, cols] = row_of[:, wide + ups + outs :]
    c = taps.shape[2]

    @pl.loop(0, G)
    def _(gs):
        x = nrm[gs]
        row = lax.broadcasted_iota(jnp.int32, (win, c), 0)
        for tt in range(T):
            prod = jnp.dot(x, WA[tt], preferred_element_type=f32) * asc[tt]
            gated = prod[:, c : 2 * c] * prod[:, :c]
            before = jnp.where(row == 0, 0.0, pltpu.roll(gated, 1, 0))
            after = jnp.where(row == win - 1, 0.0, pltpu.roll(gated, win - 1, 0))
            conv = taps[tt, 0:1] * before + taps[tt, 1:2] * gated + taps[tt, 2:3] * after
            hid[gs, :, tt * c : (tt + 1) * c] = (prod[:, 2 * c :] * conv).astype(bf16)

    all_from_siblings(1)

    @pl.loop(0, nz)
    def _(zs):
        @pl.loop(0, G)
        def _(gs):
            h = hid[gs, pl.ds(off, rows), :]
            for yy in range(2):
                p1[gs, zs, :, yy * cw : (yy + 1) * cw] = jnp.dot(
                    h, WO[2 * zs + yy], preferred_element_type=f32
                ).astype(bf16)

    kick2(3)
    for m in others():
        copy(p1.at[m], q1.at[g], s1.at[m], r1.at[g], member(m)).start()
    cut = (2 * last) // 3
    steps(2, 1, cut)

    for m in others():
        arrived(q1.at[m], r1.at[m])

    def total(p, q, zs, at):
        acc = p[g, zs, at, :].astype(f32)
        for m in others():
            acc = acc + q[m, zs, at, :].astype(f32)
        return acc

    @pl.loop(0, rows // TILE)
    def _(i):
        at = pl.ds(pl.multiple_of(i * TILE, TILE), TILE)
        here = pl.ds(pl.multiple_of(t * rows + i * TILE, TILE), TILE)
        ssq = jnp.zeros((TILE, 1), f32)
        for zs in range(nz):
            m = tok[here, zs * pw : (zs + 1) * pw].astype(f32) + total(p1, q1, zs, at) * oc[zs]
            mid32[zs, at, :] = m
            ssq = ssq + jnp.sum(m * m, axis=-1, keepdims=True)
        inv = lax.rsqrt(ssq / D + norm_eps)
        for zs in range(nz):
            cols = slice(zs * pw, (zs + 1) * pw)
            mid[g, at, cols] = (mid32[zs, at, :] * inv * g2[:, cols]).astype(bf16)

    steps(2, cut, cut + 1)
    for m in others():
        copy(mid.at[g], mid.at[g], sa.at[m], ra.at[g], member(m)).start()
    steps(2, cut + 1, last)
    cut2 = (last + 1) // 2
    steps(3, 1, cut2)

    all_from_siblings(2)
    for m in others():
        arrived(mid.at[m], ra.at[m])
    u = usc.shape[2]

    @pl.loop(0, G)
    def _(gs):
        x = mid[gs]
        for tt in range(T):
            upper = jnp.dot(x, WU[tt], preferred_element_type=f32) * usc[tt]
            act[gs, :, tt * u : (tt + 1) * u] = jnp.square(jnp.maximum(upper, 0.0)).astype(bf16)

    def down(j):
        zs, _ = place(j)

        @pl.when(jnp.logical_and(zs >= 0, zs < nz))
        def _():
            for yy in range(2):
                from_siblings(3, 2 * zs + yy)

            @pl.loop(0, G)
            def _(gs):
                x = act[gs]
                for yy in range(2):
                    p2[gs, zs, :, yy * cw : (yy + 1) * cw] = jnp.dot(
                        x, WD[2 * zs + yy], preferred_element_type=f32
                    ).astype(bf16)

            for m in others():
                copy(p2.at[m, zs], q2.at[g, zs], s2.at[m, zs], r2.at[g, zs], member(m)).start()

    @pl.loop(0, last)
    def _(j):
        @pl.when(j >= cut2)
        def _():
            step(3, j)

        down(j)

    @pl.loop(0, nz)
    def _(zs):
        for m in others():
            arrived(q2.at[m, zs], r2.at[m, zs])

    @pl.loop(0, rows // TILE)
    def _(i):
        at = pl.ds(pl.multiple_of(i * TILE, TILE), TILE)
        here = pl.ds(pl.multiple_of(t * rows + i * TILE, TILE), TILE)
        for zs in range(nz):
            out[here, zs * pw : (zs + 1) * pw] = (
                mid32[zs, at, :] + total(p2, q2, zs, at) * dc[zs]
            ).astype(bf16)

    def half(tt):
        return out.at[pl.ds(pl.multiple_of(tt * rows, rows), rows)]

    for tt in siblings():
        copy(half(t), half(t), so.at[tt], ro.at[t], (r, f, tt)).start()

    for s in stages:
        own = slot(s, f, t)
        arrived(own, sy.at[s])

        def gone(ff, k, s=s, own=own):
            arrived(own, sz.at[s, ff, k])

        for ff in (f, fy):
            pl.when(has_lo)(functools.partial(gone, ff, 0))
            pl.when(has_hi)(functools.partial(gone, ff, 1))

        @pl.loop(1, last)
        def _(j):
            zs, nxt = place(j)
            ok = jnp.logical_and(zs >= 0, zs < nz)

            @pl.when(jnp.logical_and(ok, jnp.logical_and(nxt >= 0, nxt < nz)))
            def _():
                for yy in range(2):
                    gone(2 * zs + yy, 0)

        @pl.loop(0, 2 * nz)
        def _(ff):
            for _ in siblings():
                arrived(own, sd.at[s, ff])

    for m in others():
        arrived(nrm.at[m], sn.at[m])
        arrived(p1.at[m], s1.at[m])
        arrived(mid.at[m], sa.at[m])

        @pl.loop(0, nz)
        def _(zs):
            arrived(p2.at[m, zs], s2.at[m, zs])

    for tt in siblings():
        arrived(half(tt), ro.at[tt])
        arrived(half(tt), so.at[tt])

def line_kernel(
    nz, G, T, win, rows, inside,
    tok, g1, g2, vectors, weights,
    out,
    WA, WO, WU, WD, nrm, hid, p, q, mid32, mid, act,
    staged, leaving, gathered, detour,
    rz, rd, re, sz, sd, sy, loc, rn, rb, rh, rt, sn, sh, st, r1, s1, ra, sa, r2, s2, ro, so,
):
    packed, table, asc, taps, usc, oc, dc = gathered
    D = tok.shape[1]
    pw = D // nz
    cw = pw // 2
    r, f, t = lax.axis_index("rep"), lax.axis_index("fs"), lax.axis_index("tp")
    z, y = f // 2, f % 2
    fy = z * 2 + 1 - y
    g = r * 2 + y
    ka, ko, ku, kd = (w.shape[0] for w in leaving)
    outer = jnp.logical_or(z == 0, z == nz - 1)
    inner = jnp.logical_not(outer)
    inward = jnp.where(2 * z < nz, 1, -1)
    across = z + 2 * inward
    if T == 2:
        start, off = t * (rows - HALO), t * HALO
    else:
        start = jnp.clip(t * rows - HALO, 0, tok.shape[0] - win)
        off = t * rows - start
    start, off = pl.multiple_of(start, HALO), pl.multiple_of(off, HALO)

    def member(m):
        return (m // 2, z * 2 + m % 2, t)

    def others():
        return [(g + d) % G for d in range(1, G)]

    gx, gy, gd = (1 - r) * 2 + y, r * 2 + 1 - y, (1 - r) * 2 + 1 - y

    def peers():
        return [gd, gx, gy]

    def siblings():
        return [(t + d) % T for d in range(1, T)]

    def copy(src, dst, ssem, rsem, dev):
        return pltpu.make_async_remote_copy(
            src_ref=src, dst_ref=dst, send_sem=ssem, recv_sem=rsem, device_id=dev, device_id_type=MESH
        )

    def arrived(ref, sem):
        pltpu.make_async_copy(ref, ref, sem).wait()

    def slot(s, ff, tt):
        if s == 0:
            return WA.at[tt, pl.ds(pl.multiple_of(ff * ka, ka), ka)]
        if s == 1:
            return WO.at[ff, pl.ds(pl.multiple_of(tt * ko, ko), ko)]
        if s == 2:
            return WU.at[tt, pl.ds(pl.multiple_of(ff * ku, ku), ku)]
        if s == 3:
            return WD.at[ff, pl.ds(pl.multiple_of(tt * kd, kd), kd)]
        return table.at[ff, tt]

    def to_siblings(s, ff, src):
        for tt in siblings():
            copy(src, slot(s, ff, t), sd.at[s], rd.at[s // 2, ff] if s % 2 else re.at[s // 2], (r, f, tt)).start()

    def send(s, ff, zs):
        block = slot(s, ff, t)
        copy(block, block, sz.at[s], rz.at[s, ff], (r, 2 * zs + y, t)).start()

    def send_in(s, ff):
        send(s, ff, z + inward)

    def send_out(s, ff):
        send(s, ff, z - inward)

    def spread(s, ff):
        send_in(s, ff)

        @pl.when(inner)
        def _():
            send_out(s, ff)

        @pl.when(outer)
        def _():
            send(s, ff, across)

    def fetches():
        for i, w in enumerate(weights):
            src, dst = weights[i], staged[i]
            if w.shape[1] > dst.shape[1]:
                n = dst.shape[1]
                src = src.at[:, pl.ds(pl.multiple_of(r * n, n), n)]
            elif w.shape[0] > dst.shape[0]:
                n = dst.shape[0]
                src = src.at[pl.ds(pl.multiple_of(r * n, n), n)]
            yield pltpu.make_async_copy(src, dst, loc.at[i])

    def round_stage(s):
        parts = {0: (0, 1, 2), 1: (3,), 2: (4,), 3: (5,)}[s]
        high = leaving[s].shape[0]
        for i in parts:
            pltpu.make_async_copy(staged[i], staged[i], loc.at[i]).wait()
        for yy in range(2):

            @pl.when(y == yy)
            def _():
                @pl.loop(0, high // 32)
                def _(k):
                    at = pl.ds(pl.multiple_of(k * 32, 32), 32)
                    for n, i in enumerate(parts):
                        if s in (0, 2):
                            wide = staged[i].shape[1] // 2
                            mine = staged[i][at, yy * wide : (yy + 1) * wide]
                            theirs = staged[i][at, (1 - yy) * wide : (2 - yy) * wide]
                        else:
                            wide = staged[i].shape[1]
                            mine = staged[i][pl.ds(pl.multiple_of(yy * high + k * 32, 32), 32), :]
                            theirs = staged[i][pl.ds(pl.multiple_of((1 - yy) * high + k * 32, 32), 32), :]
                        cols = slice(n * wide, (n + 1) * wide)
                        leaving[s][at, cols] = theirs.astype(bf16)
                        if s == 0:
                            WA[t, pl.ds(pl.multiple_of(f * ka + k * 32, 32), 32), cols] = mine.astype(bf16)
                        elif s == 1:
                            WO[f, pl.ds(pl.multiple_of(t * ko + k * 32, 32), 32), :] = mine.astype(bf16)
                        elif s == 2:
                            WU[t, pl.ds(pl.multiple_of(f * ku + k * 32, 32), 32), :] = mine.astype(bf16)
                        else:
                            WD[f, pl.ds(pl.multiple_of(t * kd + k * 32, 32), 32), :] = mine.astype(bf16)

    def swap(s):
        own = slot(s, f, t)
        copy(leaving[s] if s < 4 else own, own, sy.at[s], rz.at[s, f], (r, fy, t)).start()

    def swapped(s):
        arrived(slot(s, fy, t), rz.at[s, fy])

    def both_to_siblings(s):
        for ff in (f, fy):
            to_siblings(s, ff, slot(s, ff, t))

    def place(j):
        return (z + inward * j + nz) % nz

    blocks = 2 * (nz - 1)

    def block(i):
        rest = jnp.maximum(i - 2, 0)
        near_in, late_in = jnp.where(i < 2, 1, 2 + rest % 2), jnp.where(i < 2, i, rest // 2)
        near, late = jnp.where(inner, near_in, 1 + i // 2), jnp.where(inner, late_in, i % 2)
        return place(near), (y + late) % 2

    def step(s, i):
        zs, yy = block(i)
        ff = 2 * zs + yy
        arrived(slot(s, ff, t), rz.at[s, ff])

        @pl.when(inner & (zs != z - inward))
        def _():
            send_out(s, ff)

        to_siblings(s, ff, slot(s, ff, t))

    def inner_step(s, near, late):
        ff = 2 * place(near) + (y + late) % 2
        arrived(slot(s, ff, t), rz.at[s, ff])
        if s and near < nz - 1:
            send_out(s, ff)
        elif s == 0 and near == nz - 1:
            send_in(0, ff)
        to_siblings(s, ff, slot(s, ff, t))

    def steps(s, lo, hi):
        @pl.loop(lo, hi)
        def _(j):
            step(s, j)

    def from_siblings(s, ff):
        for tt in siblings():
            arrived(slot(s, ff, tt), rd.at[s // 2, ff])

    def part_of(s, tt, n):
        if s == 0:
            return WA.at[tt, pl.ds(0, n * ka)]
        if s == 1:
            return WO.at[pl.ds(0, n), pl.ds(pl.multiple_of(tt * ko, ko), ko)]
        if s == 2:
            return WU.at[tt, pl.ds(0, n * ku)]
        if s == 3:
            return WD.at[pl.ds(0, n), pl.ds(pl.multiple_of(tt * kd, kd), kd)]
        return table.at[pl.ds(0, n), tt]

    def all_from_siblings(s):
        for tt in siblings():
            arrived(part_of(s, tt, 2 * nz), re.at[s // 2])

    for fetch in fetches():
        fetch.start()
    if inside:
        at_col = 0
        for v in vectors[:3]:
            packed[:, at_col : at_col + v.shape[1]] = v[...]
            at_col += v.shape[1]
        few = vectors[0].shape[1]
        for k in range(3):
            packed[:, at_col : at_col + few] = vectors[6][k : k + 1, pl.ds(pl.multiple_of(f * few, few), few)]
            at_col += few
        for v in vectors[3:6]:
            for k in range(v.shape[0]):
                packed[:, at_col : at_col + v.shape[1]] = v[k : k + 1, :]
                at_col += v.shape[1]
        table[f, t] = packed[...]

    barrier = pltpu.get_barrier_semaphore()
    for m in others():
        pl.semaphore_signal(barrier, inc=1, device_id=member(m), device_id_type=MESH)
    for tt in siblings():
        pl.semaphore_signal(barrier, inc=1, device_id=(r, f, tt), device_id_type=MESH)

    for zs in (z - 1, z + 1, across):
        near = jnp.logical_and(zs >= 0, zs < nz)

        @pl.when(jnp.logical_and(near, zs != z))
        def _():
            pl.semaphore_signal(barrier, inc=1, device_id=(r, 2 * zs + y, t), device_id_type=MESH)

    round_stage(0)
    round_stage(1)

    pl.semaphore_wait(barrier, G + T - 2 + jnp.where(outer, 2, 3))
    swap(0)
    send_in(0, f)
    swap(4)
    swap(1)

    @pl.when(inner)
    def _():
        for s in (4, 1):
            spread(s, f)

    round_stage(2)
    round_stage(3)

    @pl.when(inner)
    def _():
        for s in (2, 3):
            send_out(s, f)
        for i in range(2):
            copy(leaving[2 + i], detour[i], st.at[i], rt.at[i], (r, 2 * (z - inward) + y, t)).start()

    @pl.loop(0, win // TILE)
    def _(i):
        at = pl.ds(pl.multiple_of(i * TILE, TILE), TILE)
        x = tok[pl.ds(pl.multiple_of(start + i * TILE, TILE), TILE), :].astype(f32)
        x = x * lax.rsqrt(jnp.mean(x * x, axis=-1, keepdims=True) + norm_eps) * g1[...]
        nrm[g, at, :] = x.astype(bf16)

    low = win // 2 // TILE * TILE

    def rows_of(i, lower):
        return nrm.at[i, pl.ds(0, low)] if lower else nrm.at[i, pl.ds(low, win - low)]

    def offer(base, sem):
        for m in (gx, gy):
            copy(nrm.at[base + g], nrm.at[base + g], sn, sem.at[g], member(m)).start()

    def pass_on(base, sem, from_x):
        m, n = (gx, gy) if from_x else (gy, gx)
        arrived(nrm.at[base + m], sem.at[m])
        some = rows_of(base + m, not from_x)
        copy(some, some, sn, sem.at[m] if from_x else sem.at[G], member(n)).start()

    def passed(base, sem):
        arrived(rows_of(base + gd, False), sem.at[gd])
        arrived(rows_of(base + gd, True), sem.at[G])

    def project(base, gs):
        x = nrm[base + gs]
        row = lax.broadcasted_iota(jnp.int32, (win, c), 0)
        for tt in range(T):
            prod = jnp.dot(x, WA[tt], preferred_element_type=f32) * asc[tt]
            gated = prod[:, c : 2 * c] * prod[:, :c]
            before = jnp.where(row == 0, 0.0, pltpu.roll(gated, 1, 0))
            after = jnp.where(row == win - 1, 0.0, pltpu.roll(gated, win - 1, 0))
            conv = taps[tt, 0:1] * before + taps[tt, 1:2] * gated + taps[tt, 2:3] * after
            hid[base + gs, :, tt * c : (tt + 1) * c] = (prod[:, 2 * c :] * conv).astype(bf16)

    def nth(k):
        return jnp.where(k == 0, g, jnp.where(k == 1, gx, jnp.where(k == 2, gy, gd)))

    def unpack():
        few, ups, outs = vectors[0].shape[1], vectors[3].size, vectors[4].shape[1]
        wide = 3 * vectors[0].shape[1] * 2
        near = 2 * nz // G
        for tt in range(T):
            for j in range(near):
                row_of = table[g * near + j, tt]
                for k in range(3):
                    at_col = (k * near + j) * few
                    asc[tt, :, at_col : at_col + few] = row_of[:, k * few : (k + 1) * few]
                    taps[tt, k : k + 1, j * few : (j + 1) * few] = row_of[:, (3 + k) * few : (4 + k) * few]
                usc[tt, :, j * ups : (j + 1) * ups] = row_of[:, wide : wide + ups]
        for zs in range(nz):
            for yy in range(2):
                row_of = table[2 * zs + yy, 0]
                cols = slice(yy * outs, (yy + 1) * outs)
                oc[zs, :, cols] = row_of[:, wide + ups : wide + ups + outs]
                dc[zs, :, cols] = row_of[:, wide + ups + outs :]
    c = taps.shape[2]

    def project_far(lo, hi):
        @pl.loop(lo, hi)
        def _(k):
            gs = nth(k)

            @pl.when(k == G - 1)
            def _():
                passed(G, rb)

            project(G, gs)
            here = pl.ds(off, rows)
            copy(hid.at[G + gs, here], hid.at[gs, here], sh, rh.at[gs], (r, 2 * (z - inward) + y, t)).start()

    @pl.when(outer)
    def _():
        swap(2)
        swap(3)
        spread(4, f)
        swapped(0)
        send_in(0, fy)
        swapped(4)
        spread(4, fy)
        copy(nrm.at[g], nrm.at[G + g], sn, rb.at[g], (r, 2 * (z + inward) + y, t)).start()
        spread(1, f)
        swapped(1)
        spread(1, fy)
        for s in (4, 1):
            both_to_siblings(s)
        spread(2, f)
        for i in range(2):
            arrived(detour[i], rt.at[i])
            ff = 2 * (z + inward) + y
            copy(detour[i], slot(2 + i, ff, t), st.at[i], rz.at[2 + i, ff], (r, fy, t)).start()
        def give_back(i):
            ff = 2 * (z + inward) + 1 - y
            arrived(slot(2 + i, ff, t), rz.at[2 + i, ff])
            send_in(2 + i, ff)
            to_siblings(2 + i, ff, slot(2 + i, ff, t))

        give_back(0)
        swapped(2)
        spread(2, fy)
        both_to_siblings(2)
        give_back(1)
        swapped(3)
        for ff in (f, fy):
            spread(3, ff)
        both_to_siblings(3)
        steps(4, 0, blocks)
        steps(1, 0, blocks)
        all_from_siblings(4)
        unpack()

    @pl.when(inner)
    def _():
        offer(0, rn)
        swapped(0)
        send_in(0, fy)
        both_to_siblings(0)
        inner_step(0, 3, 0)
        inner_step(0, 1, 0)
        for s in (4, 1):
            swapped(s)
            spread(s, fy)
            both_to_siblings(s)
        pass_on(0, rn, True)
        inner_step(0, 2, 0)
        inner_step(0, 1, 1)
        pass_on(0, rn, False)
        inner_step(0, 3, 1)
        arrived(nrm.at[G + g], rb.at[g])
        offer(G, rb)
        inner_step(0, 2, 1)
        for s in (2, 3):
            send_in(s, f)
        all_from_siblings(0)
        steps(4, 0, blocks)
        all_from_siblings(4)
        unpack()
        steps(1, 0, blocks)
        passed(0, rn)
        @pl.loop(0, G)
        def _(gs):
            project(0, gs)
    @pl.when(inner)
    def _():
        project_far(0, 1)
        pass_on(G, rb, True)
        pass_on(G, rb, False)

    def pair(ref, i, zs):
        return ref.at[i, pl.ds(2 * zs, 2)]

    def legs(zs):
        even = zs % 2 == 0
        return jnp.where(even, gx, gy), jnp.where(even, gy, gx)

    def first_leg(zs):
        first, _ = legs(zs)
        copy(pair(p, gd, zs), pair(q, 1, zs), s1, r1.at[1, zs], member(first)).start()
        copy(pair(p, first, zs), pair(q, 0, zs), s1, r1.at[0, zs], member(first)).start()

    def own_leg(j, k):
        zs = 2 * j + k
        first, _ = legs(zs)
        copy(pair(p, first, zs), pair(q, 0, zs), s1, r1.at[0, zs], member(first)).start()

    def pass_leg(zs):
        first, _ = legs(zs)
        copy(pair(p, gd, zs), pair(q, 1, zs), s1, r1.at[1, zs], member(first)).start()

    pl.when(inner)(lambda: project_far(1, 3))

    @pl.loop(0, 2 * nz)
    def _(ff):
        from_siblings(1, ff)

    @pl.loop(0, G)
    def _(k):
        gs = nth(k)

        @pl.when(outer)
        def _():
            some = hid.at[gs, pl.ds(off, rows)]
            arrived(some, rh.at[gs])

        @pl.loop(0, 2 * nz)
        def _(ff):
            h = hid[gs, pl.ds(off, rows), :]
            p[gs, ff] = jnp.dot(h, WO[ff], preferred_element_type=f32).astype(bf16)

        @pl.when(outer & (k > 0) & (k < G - 1))
        def _():
            pl.loop(0, nz // 2)(lambda j: own_leg(j, k - 1))

        @pl.when(outer & (k == G - 1))
        def _():
            pl.loop(0, nz)(pass_leg)

    @pl.when(inner)
    def _():
        pl.loop(0, nz)(pass_leg)
        for k in range(2):
            pl.loop(0, nz // 2)(lambda j: own_leg(j, k))
        project_far(3, G)
        inner_step(2, 1, 0)
        inner_step(2, 2, 0)

    @pl.loop(0, nz)
    def _(j):
        zs = place(j)
        _, second = legs(zs)
        arrived(pair(q, 1, zs), r1.at[1, zs])

        @pl.loop(0, rows // TILE)
        def _(k):
            at = pl.ds(pl.multiple_of(k * TILE, TILE), TILE)
            for yy in range(2):
                both = p[second, 2 * zs + yy, at, :].astype(f32) + q[1, 2 * zs + yy, at, :].astype(f32)
                p[second, 2 * zs + yy, at, :] = both.astype(bf16)

        copy(pair(p, second, zs), pair(q, 2, zs), s1, r1.at[2, zs], member(second)).start()

    @pl.when(inner)
    def _():
        swapped(2)
        send_in(2, fy)
        both_to_siblings(2)

    pl.when(outer)(lambda: steps(2, 0, 1))

    @pl.loop(0, nz)
    def _(zs):
        for i in (0, 2):
            arrived(pair(q, i, zs), r1.at[i, zs])

    @pl.loop(0, rows // TILE)
    def _(i):
        at = pl.ds(pl.multiple_of(i * TILE, TILE), TILE)
        here = pl.ds(pl.multiple_of(t * rows + i * TILE, TILE), TILE)
        ssq = jnp.zeros((TILE, 1), f32)
        for ff in range(2 * nz):
            half = slice(ff % 2 * cw, (ff % 2 + 1) * cw)
            acc = p[g, ff, at, :].astype(f32) + q[0, ff, at, :].astype(f32) + q[2, ff, at, :].astype(f32)
            m = tok[here, ff * cw : (ff + 1) * cw].astype(f32) + acc * oc[ff // 2, :, half]
            mid32[ff // 2, at, half] = m
            ssq = ssq + jnp.sum(m * m, axis=-1, keepdims=True)
        inv = lax.rsqrt(ssq / D + norm_eps)
        for zs in range(nz):
            cols = slice(zs * pw, (zs + 1) * pw)
            mid[g, at, cols] = (mid32[zs, at, :] * inv * g2[:, cols]).astype(bf16)

    for m in (gx, gy):
        copy(mid.at[g], mid.at[g], sa, ra.at[g], member(m)).start()

    pl.when(outer)(lambda: steps(2, 2, 4))

    @pl.when(inner)
    def _():
        inner_step(2, 2, 1)
        swapped(3)
        send_in(3, fy)
        both_to_siblings(3)
        inner_step(2, 1, 1)

    part = rows // 2
    for m, n, lo in ((gx, gy, part), (gy, gx, 0)):
        arrived(mid.at[m], ra.at[m])
        some = mid.at[m, pl.ds(lo, part)]
        copy(some, some, sa, ra.at[m] if lo else ra.at[G], member(n)).start()

    pl.when(outer)(lambda: steps(2, 4, blocks))

    @pl.when(inner)
    def _():
        inner_step(3, 1, 0)
        inner_step(2, 3, 0)
        inner_step(2, 3, 1)

    all_from_siblings(2)
    u = usc.shape[2]
    arrived(p.at[pl.ds(0, G - 1)], s1)

    @pl.loop(0, G)
    def _(k):
        gs = nth(k)

        @pl.when(k == G - 1)
        def _():
            some = mid.at[gd, pl.ds(0, part)]
            arrived(some, ra.at[gd])
            arrived(some, ra.at[G])

        x = mid[gs]
        for tt in range(T):
            upper = jnp.dot(x, WU[tt], preferred_element_type=f32) * usc[tt]
            act[gs, :, tt * u : (tt + 1) * u] = jnp.square(jnp.maximum(upper, 0.0)).astype(bf16)

    pl.when(inner)(lambda: inner_step(3, 1, 1))

    def source(i):
        zs, yy = block(jnp.maximum(i - 2, 0))
        zs, yy = jnp.where(i < 2, z, zs), jnp.where(i < 2, (y + i) % 2, yy)
        return zs, yy, 2 * zs + yy

    def direct(i):
        zs, _, _ = source(i)
        return outer & (zs == place(nz - 1))

    def second_leg(i):
        _, _, ff = source(i)
        _, second = legs(ff)

        @pl.when(jnp.logical_not(direct(i)))
        def _():
            arrived(q.at[1, ff], r2.at[1, ff])

            @pl.loop(0, rows // TILE)
            def _(k):
                at = pl.ds(pl.multiple_of(k * TILE, TILE), TILE)
                both = p[second, ff, at, :].astype(f32) + q[1, ff, at, :].astype(f32)
                p[second, ff, at, :] = both.astype(bf16)

            copy(p.at[second, ff], q.at[2, ff], s2, r2.at[2, ff], member(second)).start()

    def finish(i):
        zs, yy, ff = source(i)
        wide = pl.ds(pl.multiple_of(yy * cw, cw), cw)
        cols = pl.ds(pl.multiple_of(ff * cw, cw), cw)

        def sum_up(slots):
            for m in slots:
                arrived(q.at[m, ff], r2.at[m, ff])

            @pl.loop(0, rows // TILE)
            def _(k):
                at = pl.ds(pl.multiple_of(k * TILE, TILE), TILE)
                acc = p[g, ff, at, :].astype(f32)
                for m in slots:
                    acc = acc + q[m, ff, at, :].astype(f32)
                here = pl.ds(pl.multiple_of(t * rows + k * TILE, TILE), TILE)
                out[here, cols] = (mid32[zs, at, wide] + acc * dc[zs, :, wide]).astype(bf16)

        far = direct(i)
        pl.when(far)(lambda: sum_up((0, 1, 2)))
        pl.when(jnp.logical_not(far))(lambda: sum_up((0, 2)))
        mine = out.at[pl.ds(pl.multiple_of(t * rows, rows), rows), cols]
        for tt in siblings():
            copy(mine, mine, so, ro, (r, f, tt)).start()

    @pl.loop(0, 2 * nz)
    def _(ff_at):
        _, _, ff = source(ff_at)

        @pl.when(outer & (ff_at > 1) & (ff_at != 3))
        def _():
            step(3, ff_at - 2)

        for i, (near, late) in enumerate(((2, 0), (3, 0), (2, 1), (3, 1))):
            pl.when(inner & (ff_at == 4 + i))(functools.partial(inner_step, 3, near, late))

        from_siblings(3, ff)

        @pl.loop(0, G)
        def _(gs):
            p[gs, ff] = jnp.dot(act[gs], WD[ff], preferred_element_type=f32).astype(bf16)

        first, second = legs(ff)
        far = direct(ff_at)
        copy(p.at[gd, ff], q.at[1, ff], s2, r2.at[1, ff], member(jnp.where(far, gd, first))).start()
        copy(p.at[first, ff], q.at[0, ff], s2, r2.at[0, ff], member(first)).start()

        @pl.when(far)
        def _():
            copy(p.at[second, ff], q.at[2, ff], s2, r2.at[2, ff], member(second)).start()

        @pl.when(ff_at > 1)
        def _():
            second_leg(ff_at - 2)

        @pl.when(ff_at > 3)
        def _():
            finish(ff_at - 4)

    @pl.loop(2 * nz - 2, 2 * nz)
    def _(i):
        second_leg(i)
        finish(i - 2)

    @pl.loop(2 * nz - 2, 2 * nz)
    def _(i):
        finish(i)

    for s in range(5):
        if s in (2, 3):
            pl.when(outer)(functools.partial(arrived, slot(s, f, t), sy.at[s]))
        else:
            arrived(slot(s, f, t), sy.at[s])
        few_sent, many_sent = {0: (2, 4), 2: (5, 7), 3: (5, 7)}.get(s, (4, 8))

        @pl.when(outer)
        def _():
            arrived(part_of(s, t, few_sent), sz.at[s])

        @pl.when(inner)
        def _():
            arrived(part_of(s, t, many_sent), sz.at[s])

        def gone(s=s):
            for _ in siblings():
                arrived(part_of(s, t, 2 * nz), sd.at[s])

        if s == 0:
            pl.when(inner)(gone)
        else:
            gone()

    @pl.when(outer)
    def _():
        arrived(nrm.at[0], sn)

    @pl.when(inner)
    def _():
        arrived(nrm.at[pl.ds(0, 2 * (G - 1))], sn)
        arrived(hid.at[pl.ds(0, G), pl.ds(0, rows)], sh)

    for i in range(2):
        arrived(detour[i], st.at[i])
    arrived(mid.at[pl.ds(0, G - 1)], sa)
    arrived(p.at[pl.ds(0, G - 1)], s2)
    half = out.at[pl.ds(0, rows)]
    for _ in siblings():
        arrived(half, ro)
        arrived(half, so)

def body(
    R, n_fs, T,
    tokens, mix_gain, value_weight, value_scale, inner_weight, inner_scale, outer_weight, outer_scale,
    conv_taps, out_weight, out_scale, mlp_gain, up_weight, up_scale, down_weight, down_scale,
):
    G, nz = 2 * R, n_fs // 2
    TOK, D = tokens.shape[1:]
    rows = TOK // T
    win = TOK if T == 1 else rows + HALO if T == 2 else rows + 2 * HALO
    r, f = lax.axis_index("rep"), lax.axis_index("fs")
    g = r * 2 + f % 2

    vs, us, os = value_scale.shape[0], up_scale.shape[0], out_scale.shape[0]
    inside = all(n % 128 == 0 for n in (vs, us, os))
    lined = inside and T == 2 and nz == 4 and R == 2
    c, u = conv_taps.shape[1] // G, up_weight.shape[1] // G
    if inside:
        scales = (value_scale, inner_scale, outer_scale, up_scale, out_scale, down_scale)
        wide = 128 if lined else us
        vectors = tuple(v.reshape(-1, wide) if v is up_scale else v[None] for v in scales) + (conv_taps,)
    else:
        tap = lax.dynamic_slice_in_dim(conv_taps, f * vs, vs, axis=1)
        packed = jnp.concatenate(
            [value_scale, inner_scale, outer_scale, tap[0], tap[1], tap[2], up_scale, out_scale, down_scale]
        )
        every = lax.all_gather(packed, ("tp", "fs"), axis=0, tiled=False).reshape(T, n_fs, -1)

        def block(v):
            return lax.dynamic_index_in_dim(v.reshape(T, G, -1), g, axis=1, keepdims=True)

        small = [block(every[:, :, i * vs : (i + 1) * vs]) for i in range(6)]
        asc = jnp.concatenate(small[:3], axis=2)
        taps = jnp.concatenate(small[3:], axis=1)
        usc = block(every[:, :, 6 * vs : 6 * vs + us])
        oc = every[0, :, 6 * vs + us : 6 * vs + us + os].reshape(nz, 1, -1)
        dc = every[0, :, 6 * vs + us + os :].reshape(nz, 1, -1)
        vectors = (asc, taps, usc, oc, dc)
    weights = (value_weight, inner_weight, outer_weight, out_weight, up_weight, down_weight)
    ka, ko, kd = value_weight.shape[0], out_weight.shape[0] // G, down_weight.shape[0] // G
    cw = out_weight.shape[1]
    rounded = [(ka, 3 * c), (ko, cw), (ka, u), (kd, cw)]
    staged = [(ka, 2 * c)] * 3 + [(2 * ko, cw), (ka, 2 * u), (2 * kd, cw)]
    gathered = ()
    if inside:
        L = 6 * vs + us + 2 * os
        small = [(1, L), (n_fs, T, 1, L), (T, 1, 3 * c), (T, 3, c), (T, 1, u), (nz, 1, 2 * cw), (nz, 1, 2 * cw)]
        gathered = tuple(pltpu.VMEM(shape, f32) for shape in small)
    pw = D // nz
    dma = pltpu.SemaphoreType.DMA
    vmem = pl.BlockSpec(memory_space=pltpu.VMEM)
    hbm = pl.BlockSpec(memory_space=pl.ANY)
    held = [
        pltpu.VMEM((T, D, 3 * c), bf16),
        pltpu.VMEM((n_fs, T * ko, cw), bf16),
        pltpu.VMEM((T, D, u), bf16),
        pltpu.VMEM((n_fs, T * kd, cw), bf16),
        pltpu.VMEM((2 * G if lined else G, win, D), bf16),
        pltpu.VMEM((2 * G if lined else G, win, T * ko), bf16),
    ]
    reading = [
        tuple(pltpu.VMEM(shape, f32) for shape in staged),
        tuple(pltpu.VMEM(shape, bf16) for shape in rounded),
        gathered,
    ]
    if lined:
        run = line_kernel
        limit = 65000000
        scratch = [
            *held,
            pltpu.VMEM((G, n_fs, rows, cw), bf16),
            pltpu.VMEM((G - 1, n_fs, rows, cw), bf16),
            pltpu.VMEM((nz, rows, pw), f32),
            pltpu.VMEM((G, rows, D), bf16),
            pltpu.VMEM((G, rows, T * kd), bf16),
            *reading,
            tuple(pltpu.VMEM(shape, bf16) for shape in rounded[2:]),
            dma((5, n_fs)),
            dma((2, n_fs)),
            dma((3,)),
            dma((5,)),
            dma((5,)),
            dma((5,)),
            dma((6,)),
            dma((G + 1,)),
            dma((G + 1,)),
            dma((G,)),
            dma((2,)),
            dma,
            dma,
            dma((2,)),
            dma((G - 1, nz)),
            dma,
            dma((G + 1,)),
            dma,
            dma((G - 1, n_fs)),
            dma,
            dma,
            dma,
        ]
    else:
        run = kernel
        limit = 65000000
        scratch = [
            *held,
            pltpu.VMEM((G, nz, rows, pw), bf16),
            pltpu.VMEM((G, nz, rows, pw), bf16),
            pltpu.VMEM((nz, rows, pw), f32),
            pltpu.VMEM((G, rows, D), bf16),
            pltpu.VMEM((G, rows, T * kd), bf16),
            pltpu.VMEM((G, nz, rows, pw), bf16),
            pltpu.VMEM((G, nz, rows, pw), bf16),
            *reading,
            dma((5, n_fs)),
            dma((5, n_fs)),
            dma((5, n_fs, 2)),
            dma((5, n_fs)),
            dma((5,)),
            dma((6,)),
            dma((G,)),
            dma((G,)),
            dma((G,)),
            dma((G,)),
            dma((G,)),
            dma((G,)),
            dma((G, nz)),
            dma((G, nz)),
            dma((T,)),
            dma((T,)),
        ]
    result = pl.pallas_call(
        functools.partial(run, nz, G, T, win, rows, inside),
        out_shape=jax.ShapeDtypeStruct((TOK, D), bf16),
        in_specs=[vmem] * 3 + [(vmem,) * len(vectors), (hbm,) * 6],
        out_specs=vmem,
        scratch_shapes=scratch,
        compiler_params=pltpu.CompilerParams(collective_id=0, has_side_effects=True, vmem_limit_bytes=limit),
    )(tokens[0], mix_gain[None], mlp_gain[None], vectors, weights)
    return result[None]

def solution(mesh):
    placed = (
        P(("rep", "fs"), None, None),
        P(),
        P("fs", "tp"),
        P(("tp", "fs")),
        P("fs", "tp"),
        P(("tp", "fs")),
        P("fs", "tp"),
        P(("tp", "fs")),
        P(None, "tp"),
        P("tp", "fs"),
        P("fs"),
        P(),
        P("fs", "tp"),
        P(("tp", "fs")),
        P("tp", "fs"),
        P("fs"),
    )
    sizes = (mesh.shape["rep"], mesh.shape["fs"], mesh.shape["tp"])
    return jax.shard_map(
        functools.partial(body, *sizes),
        mesh=mesh,
        in_specs=placed,
        out_specs=P(("rep", "fs"), None, None),
        check_vma=False,
    )
```

```python
import functools

import jax
import jax.numpy as jnp
from jax import lax
from jax.experimental import pallas as pl
from jax.experimental.pallas import tpu as pltpu
from jax.sharding import PartitionSpec as P

MESH = pl.DeviceIdType.MESH
norm_eps = 1e-06
HALO = 16
TILE = 16
f32 = jnp.float32
bf16 = jnp.bfloat16


def kernel(
    nz, G, T, win, rows, inside,
    tok, g1, g2, vectors, weights,
    out,
    WA, WO, WU, WD, nrm, hid, p1, q1, mid32, mid, act, p2, q2,
    staged, leaving, gathered,
    rz, rd, sz, sd, sy, loc, rn, sn, r1, s1, ra, sa, r2, s2, ro, so,
):
    if inside:
        packed, table, asc, taps, usc, oc, dc = gathered
    else:
        asc, taps, usc, oc, dc = vectors
    D = tok.shape[1]
    pw = D // nz
    cw = pw // 2
    r, f, t = lax.axis_index("rep"), lax.axis_index("fs"), lax.axis_index("tp")
    z, y = f // 2, f % 2
    fy = z * 2 + 1 - y
    g = r * 2 + y
    ka, ko, ku, kd = (w.shape[0] for w in leaving)
    stages = range(5 if inside else 4)
    has_lo, has_hi = z > 0, z < nz - 1
    if T == 2:
        start, off = t * (rows - HALO), t * HALO
    else:
        start = jnp.clip(t * rows - HALO, 0, tok.shape[0] - win)
        off = t * rows - start
    start, off = pl.multiple_of(start, HALO), pl.multiple_of(off, HALO)

    def member(m):
        return (m // 2, z * 2 + m % 2, t)

    def others():
        return [(g + d) % G for d in range(1, G)]

    def siblings():
        return [(t + d) % T for d in range(1, T)]

    def copy(src, dst, ssem, rsem, dev):
        return pltpu.make_async_remote_copy(
            src_ref=src, dst_ref=dst, send_sem=ssem, recv_sem=rsem, device_id=dev, device_id_type=MESH
        )

    def arrived(ref, sem):
        pltpu.make_async_copy(ref, ref, sem).wait()

    def slot(s, ff, tt):
        if s == 0:
            return WA.at[tt, pl.ds(pl.multiple_of(ff * ka, ka), ka)]
        if s == 1:
            return WO.at[ff, pl.ds(pl.multiple_of(tt * ko, ko), ko)]
        if s == 2:
            return WU.at[tt, pl.ds(pl.multiple_of(ff * ku, ku), ku)]
        if s == 3:
            return WD.at[ff, pl.ds(pl.multiple_of(tt * kd, kd), kd)]
        return table.at[ff, tt]

    def to_siblings(s, ff, src):
        for tt in siblings():
            copy(src, slot(s, ff, t), sd.at[s, ff], rd.at[s, ff], (r, f, tt)).start()

    def both_ways(s, ff, src):
        @pl.when(has_lo)
        def _():
            copy(src, slot(s, ff, t), sz.at[s, ff, 0], rz.at[s, ff], (r, f - 2, t)).start()

        @pl.when(has_hi)
        def _():
            copy(src, slot(s, ff, t), sz.at[s, ff, 1], rz.at[s, ff], (r, f + 2, t)).start()

    def fetches():
        for i, w in enumerate(weights):
            src, dst = weights[i], staged[i]
            if w.shape[1] > dst.shape[1]:
                n = dst.shape[1]
                src = src.at[:, pl.ds(pl.multiple_of(r * n, n), n)]
            elif w.shape[0] > dst.shape[0]:
                n = dst.shape[0]
                src = src.at[pl.ds(pl.multiple_of(r * n, n), n)]
            yield pltpu.make_async_copy(src, dst, loc.at[i])

    def round_stage(s):
        parts = {0: (0, 1, 2), 1: (3,), 2: (4,), 3: (5,)}[s]
        high = leaving[s].shape[0]
        for i in parts:
            pltpu.make_async_copy(staged[i], staged[i], loc.at[i]).wait()
        for yy in range(2):

            @pl.when(y == yy)
            def _():
                @pl.loop(0, high // 32)
                def _(k):
                    at = pl.ds(pl.multiple_of(k * 32, 32), 32)
                    for n, i in enumerate(parts):
                        if s in (0, 2):
                            wide = staged[i].shape[1] // 2
                            mine = staged[i][at, yy * wide : (yy + 1) * wide]
                            theirs = staged[i][at, (1 - yy) * wide : (2 - yy) * wide]
                        else:
                            wide = staged[i].shape[1]
                            mine = staged[i][pl.ds(pl.multiple_of(yy * high + k * 32, 32), 32), :]
                            theirs = staged[i][pl.ds(pl.multiple_of((1 - yy) * high + k * 32, 32), 32), :]
                        cols = slice(n * wide, (n + 1) * wide)
                        leaving[s][at, cols] = theirs.astype(bf16)
                        if s == 0:
                            WA[t, pl.ds(pl.multiple_of(f * ka + k * 32, 32), 32), cols] = mine.astype(bf16)
                        elif s == 1:
                            WO[f, pl.ds(pl.multiple_of(t * ko + k * 32, 32), 32), :] = mine.astype(bf16)
                        elif s == 2:
                            WU[t, pl.ds(pl.multiple_of(f * ku + k * 32, 32), 32), :] = mine.astype(bf16)
                        else:
                            WD[f, pl.ds(pl.multiple_of(t * kd + k * 32, 32), 32), :] = mine.astype(bf16)

    def kick(s):
        own = slot(s, f, t)
        copy(leaving[s] if s < 4 else own, own, sy.at[s], rz.at[s, f], (r, fy, t)).start()
        both_ways(s, f, own)
        to_siblings(s, f, own)

    def kick2(s):
        arrived(slot(s, fy, t), rz.at[s, fy])
        both_ways(s, fy, slot(s, fy, t))
        to_siblings(s, fy, slot(s, fy, t))

    def place(j):
        k = (j + 1) // 2
        sg = 1 - 2 * (j % 2)
        return z + sg * k, z - sg

    def step(s, j):
        zs, nxt = place(j)

        @pl.when(jnp.logical_and(zs >= 0, zs < nz))
        def _():
            for yy in range(2):
                ff = 2 * zs + yy
                arrived(slot(s, ff, t), rz.at[s, ff])

                @pl.when(jnp.logical_and(nxt >= 0, nxt < nz))
                def _():
                    copy(
                        slot(s, ff, t), slot(s, ff, t), sz.at[s, ff, 0], rz.at[s, ff], (r, 2 * nxt + y, t)
                    ).start()

                to_siblings(s, ff, slot(s, ff, t))

    def steps(s, lo, hi):
        @pl.loop(lo, hi)
        def _(j):
            step(s, j)

    def from_siblings(s, ff):
        for tt in siblings():
            arrived(slot(s, ff, tt), rd.at[s, ff])

    def all_from_siblings(s):
        @pl.loop(0, 2 * nz)
        def _(ff):
            from_siblings(s, ff)

    last = 2 * nz - 1

    for fetch in fetches():
        fetch.start()
    if inside:
        at_col = 0
        for v in vectors[:3]:
            packed[:, at_col : at_col + v.shape[1]] = v[...]
            at_col += v.shape[1]
        few = vectors[0].shape[1]
        for k in range(3):
            packed[:, at_col : at_col + few] = vectors[6][k : k + 1, pl.ds(pl.multiple_of(f * few, few), few)]
            at_col += few
        for v in vectors[3:6]:
            packed[:, at_col : at_col + v.shape[1]] = v[...]
            at_col += v.shape[1]
        table[f, t] = packed[...]

    barrier = pltpu.get_barrier_semaphore()
    for m in others():
        pl.semaphore_signal(barrier, inc=1, device_id=member(m), device_id_type=MESH)
    for tt in siblings():
        pl.semaphore_signal(barrier, inc=1, device_id=(r, f, tt), device_id_type=MESH)

    @pl.when(has_lo)
    def _():
        pl.semaphore_signal(barrier, inc=1, device_id=(r, f - 2, t), device_id_type=MESH)

    @pl.when(has_hi)
    def _():
        pl.semaphore_signal(barrier, inc=1, device_id=(r, f + 2, t), device_id_type=MESH)

    pl.semaphore_wait(barrier, G + T - 2 + (z + nz - 1) // nz + (2 * nz - 2 - z) // nz)

    round_stage(0)
    round_stage(1)
    kick(0)
    if inside:
        kick(4)
    kick(1)
    round_stage(2)
    round_stage(3)

    @pl.loop(0, win // TILE)
    def _(i):
        at = pl.ds(pl.multiple_of(i * TILE, TILE), TILE)
        x = tok[pl.ds(pl.multiple_of(start + i * TILE, TILE), TILE), :].astype(f32)
        x = x * lax.rsqrt(jnp.mean(x * x, axis=-1, keepdims=True) + norm_eps) * g1[...]
        nrm[g, at, :] = x.astype(bf16)

    kick2(0)
    if inside:
        kick2(4)
    for m in others():
        copy(nrm.at[g], nrm.at[g], sn.at[m], rn.at[g], member(m)).start()
    kick(2)
    kick2(1)
    steps(0, 1, last)
    if inside:
        steps(4, 1, last)
    kick(3)
    kick2(2)
    steps(1, 1, last)

    all_from_siblings(0)
    for m in others():
        arrived(nrm.at[m], rn.at[m])
    if inside:
        all_from_siblings(4)
        few, ups, outs = vectors[0].shape[1], vectors[3].shape[1], vectors[4].shape[1]
        wide = 3 * vectors[0].shape[1] * 2
        near = 2 * nz // G
        for tt in range(T):
            for j in range(near):
                row_of = table[g * near + j, tt]
                for k in range(3):
                    at_col = (k * near + j) * few
                    asc[tt, :, at_col : at_col + few] = row_of[:, k * few : (k + 1) * few]
                    taps[tt, k : k + 1, j * few : (j + 1) * few] = row_of[:, (3 + k) * few : (4 + k) * few]
                usc[tt, :, j * ups : (j + 1) * ups] = row_of[:, wide : wide + ups]
        for zs in range(nz):
            for yy in range(2):
                row_of = table[2 * zs + yy, 0]
                cols = slice(yy * outs, (yy + 1) * outs)
                oc[zs, :, cols] = row_of[:, wide + ups : wide + ups + outs]
                dc[zs, :, cols] = row_of[:, wide + ups + outs :]
    c = taps.shape[2]

    @pl.loop(0, G)
    def _(gs):
        x = nrm[gs]
        row = lax.broadcasted_iota(jnp.int32, (win, c), 0)
        for tt in range(T):
            prod = jnp.dot(x, WA[tt], preferred_element_type=f32) * asc[tt]
            gated = prod[:, c : 2 * c] * prod[:, :c]
            before = jnp.where(row == 0, 0.0, pltpu.roll(gated, 1, 0))
            after = jnp.where(row == win - 1, 0.0, pltpu.roll(gated, win - 1, 0))
            conv = taps[tt, 0:1] * before + taps[tt, 1:2] * gated + taps[tt, 2:3] * after
            hid[gs, :, tt * c : (tt + 1) * c] = (prod[:, 2 * c :] * conv).astype(bf16)

    all_from_siblings(1)

    @pl.loop(0, nz)
    def _(zs):
        @pl.loop(0, G)
        def _(gs):
            h = hid[gs, pl.ds(off, rows), :]
            for yy in range(2):
                p1[gs, zs, :, yy * cw : (yy + 1) * cw] = jnp.dot(
                    h, WO[2 * zs + yy], preferred_element_type=f32
                ).astype(bf16)

    kick2(3)
    for m in others():
        copy(p1.at[m], q1.at[g], s1.at[m], r1.at[g], member(m)).start()
    cut = (2 * last) // 3
    steps(2, 1, cut)

    for m in others():
        arrived(q1.at[m], r1.at[m])

    def total(p, q, zs, at):
        acc = p[g, zs, at, :].astype(f32)
        for m in others():
            acc = acc + q[m, zs, at, :].astype(f32)
        return acc

    @pl.loop(0, rows // TILE)
    def _(i):
        at = pl.ds(pl.multiple_of(i * TILE, TILE), TILE)
        here = pl.ds(pl.multiple_of(t * rows + i * TILE, TILE), TILE)
        ssq = jnp.zeros((TILE, 1), f32)
        for zs in range(nz):
            m = tok[here, zs * pw : (zs + 1) * pw].astype(f32) + total(p1, q1, zs, at) * oc[zs]
            mid32[zs, at, :] = m
            ssq = ssq + jnp.sum(m * m, axis=-1, keepdims=True)
        inv = lax.rsqrt(ssq / D + norm_eps)
        for zs in range(nz):
            cols = slice(zs * pw, (zs + 1) * pw)
            mid[g, at, cols] = (mid32[zs, at, :] * inv * g2[:, cols]).astype(bf16)

    steps(2, cut, cut + 1)
    for m in others():
        copy(mid.at[g], mid.at[g], sa.at[m], ra.at[g], member(m)).start()
    steps(2, cut + 1, last)
    cut2 = (last + 1) // 2
    steps(3, 1, cut2)

    all_from_siblings(2)
    for m in others():
        arrived(mid.at[m], ra.at[m])
    u = usc.shape[2]

    @pl.loop(0, G)
    def _(gs):
        x = mid[gs]
        for tt in range(T):
            upper = jnp.dot(x, WU[tt], preferred_element_type=f32) * usc[tt]
            act[gs, :, tt * u : (tt + 1) * u] = jnp.square(jnp.maximum(upper, 0.0)).astype(bf16)

    def down(j):
        zs, _ = place(j)

        @pl.when(jnp.logical_and(zs >= 0, zs < nz))
        def _():
            for yy in range(2):
                from_siblings(3, 2 * zs + yy)

            @pl.loop(0, G)
            def _(gs):
                x = act[gs]
                for yy in range(2):
                    p2[gs, zs, :, yy * cw : (yy + 1) * cw] = jnp.dot(
                        x, WD[2 * zs + yy], preferred_element_type=f32
                    ).astype(bf16)

            for m in others():
                copy(p2.at[m, zs], q2.at[g, zs], s2.at[m, zs], r2.at[g, zs], member(m)).start()

    @pl.loop(0, last)
    def _(j):
        @pl.when(j >= cut2)
        def _():
            step(3, j)

        down(j)

    @pl.loop(0, nz)
    def _(zs):
        for m in others():
            arrived(q2.at[m, zs], r2.at[m, zs])

    @pl.loop(0, rows // TILE)
    def _(i):
        at = pl.ds(pl.multiple_of(i * TILE, TILE), TILE)
        here = pl.ds(pl.multiple_of(t * rows + i * TILE, TILE), TILE)
        for zs in range(nz):
            out[here, zs * pw : (zs + 1) * pw] = (
                mid32[zs, at, :] + total(p2, q2, zs, at) * dc[zs]
            ).astype(bf16)

    def half(tt):
        return out.at[pl.ds(pl.multiple_of(tt * rows, rows), rows)]

    for tt in siblings():
        copy(half(t), half(t), so.at[tt], ro.at[t], (r, f, tt)).start()

    for s in stages:
        own = slot(s, f, t)
        arrived(own, sy.at[s])

        def gone(ff, k, s=s, own=own):
            arrived(own, sz.at[s, ff, k])

        for ff in (f, fy):
            pl.when(has_lo)(functools.partial(gone, ff, 0))
            pl.when(has_hi)(functools.partial(gone, ff, 1))

        @pl.loop(1, last)
        def _(j):
            zs, nxt = place(j)
            ok = jnp.logical_and(zs >= 0, zs < nz)

            @pl.when(jnp.logical_and(ok, jnp.logical_and(nxt >= 0, nxt < nz)))
            def _():
                for yy in range(2):
                    gone(2 * zs + yy, 0)

        @pl.loop(0, 2 * nz)
        def _(ff):
            for _ in siblings():
                arrived(own, sd.at[s, ff])

    for m in others():
        arrived(nrm.at[m], sn.at[m])
        arrived(p1.at[m], s1.at[m])
        arrived(mid.at[m], sa.at[m])

        @pl.loop(0, nz)
        def _(zs):
            arrived(p2.at[m, zs], s2.at[m, zs])

    for tt in siblings():
        arrived(half(tt), ro.at[tt])
        arrived(half(tt), so.at[tt])


def line_kernel(
    nz, G, T, win, rows, inside,
    tok, g1, g2, vectors, weights,
    out,
    WA, WO, WU, WD, nrm, hid, p, q, mid32, mid, act, fin,
    staged, leaving, gathered, detour,
    rz, rd, re, sz, sd, sy, loc, rn, rb, rh, rt, sn, sh, st, r1, s1, ra, sa, r2, s2, ro, so, fo,
):
    packed, table, asc, taps, usc, oc, dc = gathered
    D = tok.shape[1]
    pw = D // nz
    cw = pw // 2
    r, f, t = lax.axis_index("rep"), lax.axis_index("fs"), lax.axis_index("tp")
    z, y = f // 2, f % 2
    fy = z * 2 + 1 - y
    g = r * 2 + y
    ka, ko, ku, kd = (w.shape[0] for w in leaving)
    outer = jnp.logical_or(z == 0, z == nz - 1)
    inner = jnp.logical_not(outer)
    inward = jnp.where(2 * z < nz, 1, -1)
    across = z + 2 * inward
    if T == 2:
        start, off = t * (rows - HALO), t * HALO
    else:
        start = jnp.clip(t * rows - HALO, 0, tok.shape[0] - win)
        off = t * rows - start
    start, off = pl.multiple_of(start, HALO), pl.multiple_of(off, HALO)

    def member(m):
        return (m // 2, z * 2 + m % 2, t)

    def others():
        return [(g + d) % G for d in range(1, G)]

    gx, gy, gd = (1 - r) * 2 + y, r * 2 + 1 - y, (1 - r) * 2 + 1 - y

    def peers():
        return [gd, gx, gy]

    def siblings():
        return [(t + d) % T for d in range(1, T)]

    def copy(src, dst, ssem, rsem, dev):
        return pltpu.make_async_remote_copy(
            src_ref=src, dst_ref=dst, send_sem=ssem, recv_sem=rsem, device_id=dev, device_id_type=MESH
        )

    def arrived(ref, sem):
        pltpu.make_async_copy(ref, ref, sem).wait()

    def slot(s, ff, tt):
        if s == 0:
            return WA.at[tt, pl.ds(pl.multiple_of(ff * ka, ka), ka)]
        if s == 1:
            return WO.at[ff, pl.ds(pl.multiple_of(tt * ko, ko), ko)]
        if s == 2:
            return WU.at[tt, pl.ds(pl.multiple_of(ff * ku, ku), ku)]
        if s == 3:
            return WD.at[ff, pl.ds(pl.multiple_of(tt * kd, kd), kd)]
        return table.at[ff, tt]

    def to_siblings(s, ff, src):
        for tt in siblings():
            copy(src, slot(s, ff, t), sd.at[s], rd.at[s // 2, ff] if s % 2 else re.at[s // 2], (r, f, tt)).start()

    def send(s, ff, zs):
        block = slot(s, ff, t)
        copy(block, block, sz.at[s], rz.at[s, ff], (r, 2 * zs + y, t)).start()

    def send_in(s, ff):
        send(s, ff, z + inward)

    def send_out(s, ff):
        send(s, ff, z - inward)

    def spread(s, ff):
        send_in(s, ff)

        @pl.when(inner)
        def _():
            send_out(s, ff)

        @pl.when(outer)
        def _():
            send(s, ff, across)

    def fetches():
        for i, w in enumerate(weights):
            src, dst = weights[i], staged[i]
            if w.shape[1] > dst.shape[1]:
                n = dst.shape[1]
                src = src.at[:, pl.ds(pl.multiple_of(r * n, n), n)]
            elif w.shape[0] > dst.shape[0]:
                n = dst.shape[0]
                src = src.at[pl.ds(pl.multiple_of(r * n, n), n)]
            yield pltpu.make_async_copy(src, dst, loc.at[i])

    def round_stage(s):
        parts = {0: (0, 1, 2), 1: (3,), 2: (4,), 3: (5,)}[s]
        high = leaving[s].shape[0]
        for i in parts:
            pltpu.make_async_copy(staged[i], staged[i], loc.at[i]).wait()
        for yy in range(2):

            @pl.when(y == yy)
            def _():
                @pl.loop(0, high // 32)
                def _(k):
                    at = pl.ds(pl.multiple_of(k * 32, 32), 32)
                    for n, i in enumerate(parts):
                        if s in (0, 2):
                            wide = staged[i].shape[1] // 2
                            mine = staged[i][at, yy * wide : (yy + 1) * wide]
                            theirs = staged[i][at, (1 - yy) * wide : (2 - yy) * wide]
                        else:
                            wide = staged[i].shape[1]
                            mine = staged[i][pl.ds(pl.multiple_of(yy * high + k * 32, 32), 32), :]
                            theirs = staged[i][pl.ds(pl.multiple_of((1 - yy) * high + k * 32, 32), 32), :]
                        cols = slice(n * wide, (n + 1) * wide)
                        leaving[s][at, cols] = theirs.astype(bf16)
                        if s == 0:
                            WA[t, pl.ds(pl.multiple_of(f * ka + k * 32, 32), 32), cols] = mine.astype(bf16)
                        elif s == 1:
                            WO[f, pl.ds(pl.multiple_of(t * ko + k * 32, 32), 32), :] = mine.astype(bf16)
                        elif s == 2:
                            WU[t, pl.ds(pl.multiple_of(f * ku + k * 32, 32), 32), :] = mine.astype(bf16)
                        else:
                            WD[f, pl.ds(pl.multiple_of(t * kd + k * 32, 32), 32), :] = mine.astype(bf16)

    def swap(s):
        own = slot(s, f, t)
        copy(leaving[s] if s < 4 else own, own, sy.at[s], rz.at[s, f], (r, fy, t)).start()

    def swapped(s):
        arrived(slot(s, fy, t), rz.at[s, fy])

    def both_to_siblings(s):
        for ff in (f, fy):
            to_siblings(s, ff, slot(s, ff, t))

    def place(j):
        return (z + inward * j + nz) % nz

    blocks = 2 * (nz - 1)

    def block(i):
        return place(1 + i // 2), (y + i) % 2

    def step(s, i):
        zs, yy = block(i)
        ff = 2 * zs + yy
        arrived(slot(s, ff, t), rz.at[s, ff])

        @pl.when(inner & (zs != z - inward))
        def _():
            send_out(s, ff)

        to_siblings(s, ff, slot(s, ff, t))

    def inner_step(s, near, late):
        ff = 2 * place(near) + (y + late) % 2
        arrived(slot(s, ff, t), rz.at[s, ff])
        if s and near < nz - 1:
            send_out(s, ff)
        elif s == 0 and near == nz - 1:
            send_in(0, ff)
        to_siblings(s, ff, slot(s, ff, t))

    def steps(s, lo, hi):
        @pl.loop(lo, hi)
        def _(j):
            step(s, j)

    def from_siblings(s, ff):
        for tt in siblings():
            arrived(slot(s, ff, tt), rd.at[s // 2, ff])

    def part_of(s, tt, n):
        if s == 0:
            return WA.at[tt, pl.ds(0, n * ka)]
        if s == 1:
            return WO.at[pl.ds(0, n), pl.ds(pl.multiple_of(tt * ko, ko), ko)]
        if s == 2:
            return WU.at[tt, pl.ds(0, n * ku)]
        if s == 3:
            return WD.at[pl.ds(0, n), pl.ds(pl.multiple_of(tt * kd, kd), kd)]
        return table.at[pl.ds(0, n), tt]

    def all_from_siblings(s):
        for tt in siblings():
            arrived(part_of(s, tt, 2 * nz), re.at[s // 2])

    for fetch in fetches():
        fetch.start()
    if inside:
        at_col = 0
        for v in vectors[:3]:
            packed[:, at_col : at_col + v.shape[1]] = v[...]
            at_col += v.shape[1]
        few = vectors[0].shape[1]
        for k in range(3):
            packed[:, at_col : at_col + few] = vectors[6][k : k + 1, pl.ds(pl.multiple_of(f * few, few), few)]
            at_col += few
        for v in vectors[3:6]:
            for k in range(v.shape[0]):
                packed[:, at_col : at_col + v.shape[1]] = v[k : k + 1, :]
                at_col += v.shape[1]
        table[f, t] = packed[...]

    barrier = pltpu.get_barrier_semaphore()
    for m in others():
        pl.semaphore_signal(barrier, inc=1, device_id=member(m), device_id_type=MESH)
    for tt in siblings():
        pl.semaphore_signal(barrier, inc=1, device_id=(r, f, tt), device_id_type=MESH)

    for zs in (z - 1, z + 1, across):
        near = jnp.logical_and(zs >= 0, zs < nz)

        @pl.when(jnp.logical_and(near, zs != z))
        def _():
            pl.semaphore_signal(barrier, inc=1, device_id=(r, 2 * zs + y, t), device_id_type=MESH)

    round_stage(0)
    round_stage(1)
    pl.semaphore_wait(barrier, G + T - 2 + jnp.where(outer, 2, 3))
    swap(0)
    send_in(0, f)
    swap(4)
    swap(1)

    @pl.when(inner)
    def _():
        for s in (4, 1):
            spread(s, f)

    round_stage(2)
    round_stage(3)

    @pl.when(inner)
    def _():
        for s in (2, 3):
            send_out(s, f)
        for i in range(2):
            copy(leaving[2 + i], detour[i], st.at[i], rt.at[i], (r, 2 * (z - inward) + y, t)).start()

    @pl.loop(0, win // TILE)
    def _(i):
        at = pl.ds(pl.multiple_of(i * TILE, TILE), TILE)
        x = tok[pl.ds(pl.multiple_of(start + i * TILE, TILE), TILE), :].astype(f32)
        x = x * lax.rsqrt(jnp.mean(x * x, axis=-1, keepdims=True) + norm_eps) * g1[...]
        nrm[g, at, :] = x.astype(bf16)

    low = win // 2 // TILE * TILE

    def rows_of(i, lower):
        return nrm.at[i, pl.ds(0, low)] if lower else nrm.at[i, pl.ds(low, win - low)]

    def offer(base, sem):
        for m in (gx, gy):
            copy(nrm.at[base + g], nrm.at[base + g], sn, sem.at[g], member(m)).start()

    def pass_on(base, sem, from_x):
        m, n = (gx, gy) if from_x else (gy, gx)
        arrived(nrm.at[base + m], sem.at[m])
        some = rows_of(base + m, not from_x)
        copy(some, some, sn, sem.at[m] if from_x else sem.at[G], member(n)).start()

    def passed(base, sem):
        arrived(rows_of(base + gd, False), sem.at[gd])
        arrived(rows_of(base + gd, True), sem.at[G])

    def project(base, gs):
        x = nrm[base + gs]
        row = lax.broadcasted_iota(jnp.int32, (win, c), 0)
        for tt in range(T):
            prod = jnp.dot(x, WA[tt], preferred_element_type=f32) * asc[tt]
            gated = prod[:, c : 2 * c] * prod[:, :c]
            before = jnp.where(row == 0, 0.0, pltpu.roll(gated, 1, 0))
            after = jnp.where(row == win - 1, 0.0, pltpu.roll(gated, win - 1, 0))
            conv = taps[tt, 0:1] * before + taps[tt, 1:2] * gated + taps[tt, 2:3] * after
            hid[base + gs, :, tt * c : (tt + 1) * c] = (prod[:, 2 * c :] * conv).astype(bf16)

    def nth(k):
        return jnp.where(k == 0, g, jnp.where(k == 1, gx, jnp.where(k == 2, gy, gd)))

    def unpack():
        few, ups, outs = vectors[0].shape[1], vectors[3].size, vectors[4].shape[1]
        wide = 3 * vectors[0].shape[1] * 2
        near = 2 * nz // G
        for tt in range(T):
            for j in range(near):
                row_of = table[g * near + j, tt]
                for k in range(3):
                    at_col = (k * near + j) * few
                    asc[tt, :, at_col : at_col + few] = row_of[:, k * few : (k + 1) * few]
                    taps[tt, k : k + 1, j * few : (j + 1) * few] = row_of[:, (3 + k) * few : (4 + k) * few]
                usc[tt, :, j * ups : (j + 1) * ups] = row_of[:, wide : wide + ups]
        for zs in range(nz):
            for yy in range(2):
                row_of = table[2 * zs + yy, 0]
                cols = slice(yy * outs, (yy + 1) * outs)
                oc[zs, :, cols] = row_of[:, wide + ups : wide + ups + outs]
                dc[zs, :, cols] = row_of[:, wide + ups + outs :]
    c = taps.shape[2]

    def hand_over(gs):
        here = pl.ds(off, rows)
        copy(hid.at[G + gs, here], hid.at[gs, here], sh, rh.at[gs], (r, 2 * (z - inward) + y, t)).start()

    def project_far(lo, hi):
        @pl.loop(lo, hi)
        def _(k):
            gs = nth(k)

            @pl.when(k == G - 1)
            def _():
                passed(G, rb)

            project(G, gs)
            hand_over(gs)

    @pl.when(outer)
    def _():
        swap(2)
        swap(3)
        spread(4, f)
        swapped(0)
        send_in(0, fy)
        swapped(4)
        spread(4, fy)
        copy(nrm.at[g], nrm.at[G + g], sn, rb.at[g], (r, 2 * (z + inward) + y, t)).start()
        spread(1, f)
        swapped(1)
        spread(1, fy)
        for s in (4, 1):
            both_to_siblings(s)
        spread(2, f)
        for i in range(2):
            arrived(detour[i], rt.at[i])
            ff = 2 * (z + inward) + y
            copy(detour[i], slot(2 + i, ff, t), st.at[i], rz.at[2 + i, ff], (r, fy, t)).start()
        def give_back(i):
            ff = 2 * (z + inward) + 1 - y
            arrived(slot(2 + i, ff, t), rz.at[2 + i, ff])
            send_in(2 + i, ff)
            to_siblings(2 + i, ff, slot(2 + i, ff, t))

        give_back(0)
        swapped(2)
        spread(2, fy)
        both_to_siblings(2)
        give_back(1)
        swapped(3)
        for ff in (f, fy):
            send(3, ff, across)
            send_in(3, ff)
        both_to_siblings(3)
        steps(4, 0, blocks)
        steps(1, 0, blocks)
        all_from_siblings(4)
        unpack()

    @pl.when(inner)
    def _():
        offer(0, rn)
        swapped(0)
        send_in(0, fy)
        both_to_siblings(0)
        inner_step(0, 3, 0)
        inner_step(0, 1, 0)
        for s in (4, 1):
            swapped(s)
            spread(s, fy)
            both_to_siblings(s)
        pass_on(0, rn, True)
        inner_step(0, 2, 0)
        inner_step(0, 1, 1)
        pass_on(0, rn, False)
        inner_step(0, 3, 1)
        arrived(nrm.at[G + g], rb.at[g])
        offer(G, rb)
        inner_step(0, 2, 1)
        for s in (2, 3):
            send_in(s, f)
        all_from_siblings(0)
        steps(4, 0, blocks)
        all_from_siblings(4)
        unpack()
        steps(1, 0, blocks)
        passed(0, rn)
        @pl.loop(0, G)
        def _(gs):
            project(0, gs)
    @pl.when(inner)
    def _():
        project(G, g)
        pass_on(G, rb, True)
        pass_on(G, rb, False)

    def pair(ref, i, zs):
        return ref.at[i, pl.ds(2 * zs, 2)]

    def legs(zs):
        even = zs % 2 == 0
        return jnp.where(even, gx, gy), jnp.where(even, gy, gx)

    def first_leg(zs):
        first, _ = legs(zs)
        copy(pair(p, gd, zs), pair(q, 1, zs), s1, r1.at[1, zs], member(first)).start()
        copy(pair(p, first, zs), pair(q, 0, zs), s1, r1.at[0, zs], member(first)).start()

    def own_leg(j, k):
        zs = 2 * j + k
        first, _ = legs(zs)
        copy(pair(p, first, zs), pair(q, 0, zs), s1, r1.at[0, zs], member(first)).start()

    def pass_leg(zs):
        first, _ = legs(zs)
        copy(pair(p, gd, zs), pair(q, 1, zs), s1, r1.at[1, zs], member(first)).start()

    pl.when(inner)(lambda: project_far(1, 3))

    @pl.loop(0, 2 * nz)
    def _(ff):
        from_siblings(1, ff)

    @pl.loop(0, G)
    def _(k):
        gs = nth((k + 1) % G)

        @pl.when(outer)
        def _():
            some = hid.at[gs, pl.ds(off, rows)]
            arrived(some, rh.at[gs])

        @pl.loop(0, 2 * nz)
        def _(ff):
            h = hid[gs, pl.ds(off, rows), :]
            p[gs, ff] = jnp.dot(h, WO[ff], preferred_element_type=f32).astype(bf16)

        @pl.when(outer & (k < 2))
        def _():
            pl.loop(0, nz // 2)(lambda j: own_leg(j, k))

        @pl.when(outer & (k == 2))
        def _():
            pl.loop(0, nz)(pass_leg)

    @pl.when(inner)
    def _():
        pl.loop(0, nz)(pass_leg)
        for k in range(2):
            pl.loop(0, nz // 2)(lambda j: own_leg(j, k))
        project_far(3, G)
        hand_over(g)
        inner_step(2, 1, 0)
        inner_step(2, 2, 0)

    @pl.loop(0, nz)
    def _(j):
        zs = place(j)
        _, second = legs(zs)
        arrived(pair(q, 1, zs), r1.at[1, zs])

        @pl.loop(0, rows // TILE)
        def _(k):
            at = pl.ds(pl.multiple_of(k * TILE, TILE), TILE)
            for yy in range(2):
                both = p[second, 2 * zs + yy, at, :].astype(f32) + q[1, 2 * zs + yy, at, :].astype(f32)
                p[second, 2 * zs + yy, at, :] = both.astype(bf16)

        copy(pair(p, second, zs), pair(q, 2, zs), s1, r1.at[2, zs], member(second)).start()

    @pl.when(inner)
    def _():
        swapped(2)
        send_in(2, fy)
        both_to_siblings(2)

    pl.when(outer)(lambda: steps(2, 0, 1))
    @pl.loop(0, nz)
    def _(zs):
        for i in (0, 2):
            arrived(pair(q, i, zs), r1.at[i, zs])

    @pl.loop(0, rows // TILE)
    def _(i):
        at = pl.ds(pl.multiple_of(i * TILE, TILE), TILE)
        here = pl.ds(pl.multiple_of(t * rows + i * TILE, TILE), TILE)
        ssq = jnp.zeros((TILE, 1), f32)
        for ff in range(2 * nz):
            half = slice(ff % 2 * cw, (ff % 2 + 1) * cw)
            acc = p[g, ff, at, :].astype(f32) + q[0, ff, at, :].astype(f32) + q[2, ff, at, :].astype(f32)
            m = tok[here, ff * cw : (ff + 1) * cw].astype(f32) + acc * oc[ff // 2, :, half]
            mid32[ff // 2, at, half] = m
            ssq = ssq + jnp.sum(m * m, axis=-1, keepdims=True)
        inv = lax.rsqrt(ssq / D + norm_eps)
        for zs in range(nz):
            cols = slice(zs * pw, (zs + 1) * pw)
            mid[g, at, cols] = (mid32[zs, at, :] * inv * g2[:, cols]).astype(bf16)

    for m in (gx, gy):
        copy(mid.at[g], mid.at[g], sa, ra.at[g], member(m)).start()
    pl.when(outer)(lambda: steps(2, 2, 4))

    @pl.when(inner)
    def _():
        inner_step(2, 2, 1)
        swapped(3)
        send_in(3, fy)
        both_to_siblings(3)
        inner_step(2, 1, 1)

    part = rows // 2
    for m, n, lo in ((gx, gy, part), (gy, gx, 0)):
        arrived(mid.at[m], ra.at[m])
        some = mid.at[m, pl.ds(lo, part)]
        copy(some, some, sa, ra.at[m] if lo else ra.at[G], member(n)).start()
    pl.when(outer)(lambda: steps(2, 4, blocks))

    @pl.when(inner)
    def _():
        inner_step(3, 1, 0)
        inner_step(3, 1, 1)
        inner_step(2, 3, 0)
        inner_step(2, 3, 1)

    all_from_siblings(2)
    u = usc.shape[2]
    arrived(p.at[pl.ds(0, G - 1)], s1)

    @pl.loop(0, G)
    def _(k):
        gs = nth(k)

        @pl.when(k == G - 1)
        def _():
            some = mid.at[gd, pl.ds(0, part)]
            arrived(some, ra.at[gd])
            arrived(some, ra.at[G])

        x = mid[gs]
        for tt in range(T):
            upper = jnp.dot(x, WU[tt], preferred_element_type=f32) * usc[tt]
            act[gs, :, tt * u : (tt + 1) * u] = jnp.square(jnp.maximum(upper, 0.0)).astype(bf16)

    @pl.when(inner)
    def _():
        inner_step(3, 2, 0)

    def source(i):
        zs, yy = block(jnp.maximum(i - 2, 0))
        zs, yy = jnp.where(i < 2, z, zs), jnp.where(i < 2, (y + i) % 2, yy)
        return zs, yy, 2 * zs + yy

    def direct(i):
        return outer & (i > 3)

    def second_leg(i):
        _, _, ff = source(i)
        _, second = legs(ff)

        @pl.when(jnp.logical_not(direct(i)))
        def _():
            arrived(q.at[1, ff], r2.at[1, ff])

            @pl.loop(0, rows // TILE)
            def _(k):
                at = pl.ds(pl.multiple_of(k * TILE, TILE), TILE)
                both = p[second, ff, at, :].astype(f32) + q[1, ff, at, :].astype(f32)
                p[second, ff, at, :] = both.astype(bf16)

            copy(p.at[second, ff], q.at[2, ff], s2, r2.at[2, ff], member(second)).start()

    def finish(i):
        zs, yy, ff = source(i)
        wide = pl.ds(pl.multiple_of(yy * cw, cw), cw)
        cols = pl.ds(pl.multiple_of(ff * cw, cw), cw)

        def sum_up(slots):
            for m in slots:
                arrived(q.at[m, ff], r2.at[m, ff])

            @pl.loop(0, rows // TILE)
            def _(k):
                at = pl.ds(pl.multiple_of(k * TILE, TILE), TILE)
                acc = p[g, ff, at, :].astype(f32)
                for m in slots:
                    acc = acc + q[m, ff, at, :].astype(f32)
                fin[ff, at, :] = (mid32[zs, at, wide] + acc * dc[zs, :, wide]).astype(bf16)

        far = direct(i)
        pl.when(far)(lambda: sum_up((0, 1, 2)))
        pl.when(jnp.logical_not(far))(lambda: sum_up((0, 2)))
        mine = out.at[pl.ds(pl.multiple_of(t * rows, rows), rows), cols]
        for tt in siblings():
            copy(fin.at[ff], mine, so, ro, (r, f, tt)).start()
        pltpu.make_async_copy(fin.at[ff], mine, fo).start()

    @pl.loop(0, 2 * nz)
    def _(ff_at):
        _, _, ff = source(ff_at)

        @pl.when(outer & (ff_at > 1) & (ff_at != 3))
        def _():
            step(3, ff_at - 2)

        for at, near, late in ((3, 2, 1), (6, 3, 0), (7, 3, 1)):
            pl.when(inner & (ff_at == at))(functools.partial(inner_step, 3, near, late))

        from_siblings(3, ff)

        @pl.loop(0, G)
        def _(gs):
            p[gs, ff] = jnp.dot(act[gs], WD[ff], preferred_element_type=f32).astype(bf16)

        first, second = legs(ff)
        far = direct(ff_at)
        copy(p.at[gd, ff], q.at[1, ff], s2, r2.at[1, ff], member(jnp.where(far, gd, first))).start()
        copy(p.at[first, ff], q.at[0, ff], s2, r2.at[0, ff], member(first)).start()

        @pl.when(far)
        def _():
            copy(p.at[second, ff], q.at[2, ff], s2, r2.at[2, ff], member(second)).start()

        @pl.when(ff_at > 1)
        def _():
            second_leg(ff_at - 2)

        @pl.when(ff_at > 5)
        def _():
            finish(ff_at - 6)

    second_leg(2 * nz - 2)
    pl.loop(2, 4)(finish)
    second_leg(2 * nz - 1)
    pl.loop(4, 2 * nz)(finish)

    for s in range(5):
        if s in (2, 3):
            pl.when(outer)(functools.partial(arrived, slot(s, f, t), sy.at[s]))
        else:
            arrived(slot(s, f, t), sy.at[s])
        few_sent, many_sent = {0: (2, 4), 2: (5, 7), 3: (5, 7)}.get(s, (4, 8))

        @pl.when(outer)
        def _():
            arrived(part_of(s, t, few_sent), sz.at[s])

        @pl.when(inner)
        def _():
            arrived(part_of(s, t, many_sent), sz.at[s])

        def gone(s=s):
            for _ in siblings():
                arrived(part_of(s, t, 2 * nz), sd.at[s])

        if s == 0:
            pl.when(inner)(gone)
        else:
            gone()

    @pl.when(outer)
    def _():
        arrived(nrm.at[0], sn)

    @pl.when(inner)
    def _():
        arrived(nrm.at[pl.ds(0, 2 * (G - 1))], sn)
        arrived(hid.at[pl.ds(0, G), pl.ds(0, rows)], sh)

    for i in range(2):
        arrived(detour[i], st.at[i])
    arrived(mid.at[pl.ds(0, G - 1)], sa)
    arrived(p.at[pl.ds(0, G - 1)], s2)
    half = out.at[pl.ds(0, rows)]
    for _ in siblings():
        arrived(half, ro)
        arrived(fin, so)
    pltpu.make_async_copy(fin, fin, fo).wait()


def body(
    R, n_fs, T,
    tokens, mix_gain, value_weight, value_scale, inner_weight, inner_scale, outer_weight, outer_scale,
    conv_taps, out_weight, out_scale, mlp_gain, up_weight, up_scale, down_weight, down_scale,
):
    G, nz = 2 * R, n_fs // 2
    TOK, D = tokens.shape[1:]
    rows = TOK // T
    win = TOK if T == 1 else rows + HALO if T == 2 else rows + 2 * HALO
    r, f = lax.axis_index("rep"), lax.axis_index("fs")
    g = r * 2 + f % 2

    vs, us, os = value_scale.shape[0], up_scale.shape[0], out_scale.shape[0]
    inside = all(n % 128 == 0 for n in (vs, us, os))
    lined = inside and T == 2 and nz == 4 and R == 2
    c, u = conv_taps.shape[1] // G, up_weight.shape[1] // G
    if inside:
        scales = (value_scale, inner_scale, outer_scale, up_scale, out_scale, down_scale)
        wide = 128 if lined else us
        vectors = tuple(v.reshape(-1, wide) if v is up_scale else v[None] for v in scales) + (conv_taps,)
    else:
        tap = lax.dynamic_slice_in_dim(conv_taps, f * vs, vs, axis=1)
        packed = jnp.concatenate(
            [value_scale, inner_scale, outer_scale, tap[0], tap[1], tap[2], up_scale, out_scale, down_scale]
        )
        every = lax.all_gather(packed, ("tp", "fs"), axis=0, tiled=False).reshape(T, n_fs, -1)

        def block(v):
            return lax.dynamic_index_in_dim(v.reshape(T, G, -1), g, axis=1, keepdims=True)

        small = [block(every[:, :, i * vs : (i + 1) * vs]) for i in range(6)]
        asc = jnp.concatenate(small[:3], axis=2)
        taps = jnp.concatenate(small[3:], axis=1)
        usc = block(every[:, :, 6 * vs : 6 * vs + us])
        oc = every[0, :, 6 * vs + us : 6 * vs + us + os].reshape(nz, 1, -1)
        dc = every[0, :, 6 * vs + us + os :].reshape(nz, 1, -1)
        vectors = (asc, taps, usc, oc, dc)
    weights = (value_weight, inner_weight, outer_weight, out_weight, up_weight, down_weight)
    ka, ko, kd = value_weight.shape[0], out_weight.shape[0] // G, down_weight.shape[0] // G
    cw = out_weight.shape[1]
    rounded = [(ka, 3 * c), (ko, cw), (ka, u), (kd, cw)]
    staged = [(ka, 2 * c)] * 3 + [(2 * ko, cw), (ka, 2 * u), (2 * kd, cw)]
    gathered = ()
    if inside:
        L = 6 * vs + us + 2 * os
        small = [(1, L), (n_fs, T, 1, L), (T, 1, 3 * c), (T, 3, c), (T, 1, u), (nz, 1, 2 * cw), (nz, 1, 2 * cw)]
        gathered = tuple(pltpu.VMEM(shape, f32) for shape in small)
    pw = D // nz
    dma = pltpu.SemaphoreType.DMA
    vmem = pl.BlockSpec(memory_space=pltpu.VMEM)
    hbm = pl.BlockSpec(memory_space=pl.ANY)
    held = [
        pltpu.VMEM((T, D, 3 * c), bf16),
        pltpu.VMEM((n_fs, T * ko, cw), bf16),
        pltpu.VMEM((T, D, u), bf16),
        pltpu.VMEM((n_fs, T * kd, cw), bf16),
        pltpu.VMEM((2 * G if lined else G, win, D), bf16),
        pltpu.VMEM((2 * G if lined else G, win, T * ko), bf16),
    ]
    reading = [
        tuple(pltpu.VMEM(shape, f32) for shape in staged),
        tuple(pltpu.VMEM(shape, bf16) for shape in rounded),
        gathered,
    ]
    if lined:
        run = line_kernel
        limit = 65000000
        scratch = [
            *held,
            pltpu.VMEM((G, n_fs, rows, cw), bf16),
            pltpu.VMEM((G - 1, n_fs, rows, cw), bf16),
            pltpu.VMEM((nz, rows, pw), f32),
            pltpu.VMEM((G, rows, D), bf16),
            pltpu.VMEM((G, rows, T * kd), bf16),
            pltpu.VMEM((n_fs, rows, cw), bf16),
            *reading,
            tuple(pltpu.VMEM(shape, bf16) for shape in rounded[2:]),
            dma((5, n_fs)),
            dma((2, n_fs)),
            dma((3,)),
            dma((5,)),
            dma((5,)),
            dma((5,)),
            dma((6,)),
            dma((G + 1,)),
            dma((G + 1,)),
            dma((G,)),
            dma((2,)),
            dma,
            dma,
            dma((2,)),
            dma((G - 1, nz)),
            dma,
            dma((G + 1,)),
            dma,
            dma((G - 1, n_fs)),
            dma,
            dma,
            dma,
            dma,
        ]
    else:
        run = kernel
        limit = 65000000
        scratch = [
            *held,
            pltpu.VMEM((G, nz, rows, pw), bf16),
            pltpu.VMEM((G, nz, rows, pw), bf16),
            pltpu.VMEM((nz, rows, pw), f32),
            pltpu.VMEM((G, rows, D), bf16),
            pltpu.VMEM((G, rows, T * kd), bf16),
            pltpu.VMEM((G, nz, rows, pw), bf16),
            pltpu.VMEM((G, nz, rows, pw), bf16),
            *reading,
            dma((5, n_fs)),
            dma((5, n_fs)),
            dma((5, n_fs, 2)),
            dma((5, n_fs)),
            dma((5,)),
            dma((6,)),
            dma((G,)),
            dma((G,)),
            dma((G,)),
            dma((G,)),
            dma((G,)),
            dma((G,)),
            dma((G, nz)),
            dma((G, nz)),
            dma((T,)),
            dma((T,)),
        ]
    result = pl.pallas_call(
        functools.partial(run, nz, G, T, win, rows, inside),
        out_shape=jax.ShapeDtypeStruct((TOK, D), bf16),
        in_specs=[vmem] * 3 + [(vmem,) * len(vectors), (hbm,) * 6],
        out_specs=hbm if lined else vmem,
        scratch_shapes=scratch,
        compiler_params=pltpu.CompilerParams(collective_id=0, has_side_effects=True, vmem_limit_bytes=limit),
    )(tokens[0], mix_gain[None], mlp_gain[None], vectors, weights)
    return result[None]


def solution(mesh):
    placed = (
        P(("rep", "fs"), None, None),
        P(),
        P("fs", "tp"),
        P(("tp", "fs")),
        P("fs", "tp"),
        P(("tp", "fs")),
        P("fs", "tp"),
        P(("tp", "fs")),
        P(None, "tp"),
        P("tp", "fs"),
        P("fs"),
        P(),
        P("fs", "tp"),
        P(("tp", "fs")),
        P("tp", "fs"),
        P("fs"),
    )
    sizes = (mesh.shape["rep"], mesh.shape["fs"], mesh.shape["tp"])
    return jax.shard_map(
        functools.partial(body, *sizes),
        mesh=mesh,
        in_specs=placed,
        out_specs=P(("rep", "fs"), None, None),
        check_vma=False,
    )
```

```python
import functools

import jax
import jax.numpy as jnp
from jax import lax
from jax.experimental import pallas as pl
from jax.experimental.pallas import tpu as pltpu
from jax.sharding import PartitionSpec as P

MESH = pl.DeviceIdType.MESH
norm_eps = 1e-06
HALO = 16
TILE = 16
f32 = jnp.float32
bf16 = jnp.bfloat16


def kernel(
    nz, G, T, win, rows, inside,
    tok, g1, g2, vectors, weights,
    out,
    WA, WO, WU, WD, nrm, hid, p1, q1, mid32, mid, act, p2, q2,
    staged, leaving, gathered,
    rz, rd, sz, sd, sy, loc, rn, sn, r1, s1, ra, sa, r2, s2, ro, so,
):
    if inside:
        packed, table, asc, taps, usc, oc, dc = gathered
    else:
        asc, taps, usc, oc, dc = vectors
    D = tok.shape[1]
    pw = D // nz
    cw = pw // 2
    r, f, t = lax.axis_index("rep"), lax.axis_index("fs"), lax.axis_index("tp")
    z, y = f // 2, f % 2
    fy = z * 2 + 1 - y
    g = r * 2 + y
    ka, ko, ku, kd = (w.shape[0] for w in leaving)
    stages = range(5 if inside else 4)
    has_lo, has_hi = z > 0, z < nz - 1
    if T == 2:
        start, off = t * (rows - HALO), t * HALO
    else:
        start = jnp.clip(t * rows - HALO, 0, tok.shape[0] - win)
        off = t * rows - start
    start, off = pl.multiple_of(start, HALO), pl.multiple_of(off, HALO)

    def member(m):
        return (m // 2, z * 2 + m % 2, t)

    def others():
        return [(g + d) % G for d in range(1, G)]

    def siblings():
        return [(t + d) % T for d in range(1, T)]

    def copy(src, dst, ssem, rsem, dev):
        return pltpu.make_async_remote_copy(
            src_ref=src, dst_ref=dst, send_sem=ssem, recv_sem=rsem, device_id=dev, device_id_type=MESH
        )

    def arrived(ref, sem):
        pltpu.make_async_copy(ref, ref, sem).wait()

    def slot(s, ff, tt):
        if s == 0:
            return WA.at[tt, pl.ds(pl.multiple_of(ff * ka, ka), ka)]
        if s == 1:
            return WO.at[ff, pl.ds(pl.multiple_of(tt * ko, ko), ko)]
        if s == 2:
            return WU.at[tt, pl.ds(pl.multiple_of(ff * ku, ku), ku)]
        if s == 3:
            return WD.at[ff, pl.ds(pl.multiple_of(tt * kd, kd), kd)]
        return table.at[ff, tt]

    def to_siblings(s, ff, src):
        for tt in siblings():
            copy(src, slot(s, ff, t), sd.at[s, ff], rd.at[s, ff], (r, f, tt)).start()

    def both_ways(s, ff, src):
        @pl.when(has_lo)
        def _():
            copy(src, slot(s, ff, t), sz.at[s, ff, 0], rz.at[s, ff], (r, f - 2, t)).start()

        @pl.when(has_hi)
        def _():
            copy(src, slot(s, ff, t), sz.at[s, ff, 1], rz.at[s, ff], (r, f + 2, t)).start()

    def fetches():
        for i, w in enumerate(weights):
            src, dst = weights[i], staged[i]
            if w.shape[1] > dst.shape[1]:
                n = dst.shape[1]
                src = src.at[:, pl.ds(pl.multiple_of(r * n, n), n)]
            elif w.shape[0] > dst.shape[0]:
                n = dst.shape[0]
                src = src.at[pl.ds(pl.multiple_of(r * n, n), n)]
            yield pltpu.make_async_copy(src, dst, loc.at[i])

    def round_stage(s):
        parts = {0: (0, 1, 2), 1: (3,), 2: (4,), 3: (5,)}[s]
        high = leaving[s].shape[0]
        for i in parts:
            pltpu.make_async_copy(staged[i], staged[i], loc.at[i]).wait()
        for yy in range(2):

            @pl.when(y == yy)
            def _():
                @pl.loop(0, high // 32)
                def _(k):
                    at = pl.ds(pl.multiple_of(k * 32, 32), 32)
                    for n, i in enumerate(parts):
                        if s in (0, 2):
                            wide = staged[i].shape[1] // 2
                            mine = staged[i][at, yy * wide : (yy + 1) * wide]
                            theirs = staged[i][at, (1 - yy) * wide : (2 - yy) * wide]
                        else:
                            wide = staged[i].shape[1]
                            mine = staged[i][pl.ds(pl.multiple_of(yy * high + k * 32, 32), 32), :]
                            theirs = staged[i][pl.ds(pl.multiple_of((1 - yy) * high + k * 32, 32), 32), :]
                        cols = slice(n * wide, (n + 1) * wide)
                        leaving[s][at, cols] = theirs.astype(bf16)
                        if s == 0:
                            WA[t, pl.ds(pl.multiple_of(f * ka + k * 32, 32), 32), cols] = mine.astype(bf16)
                        elif s == 1:
                            WO[f, pl.ds(pl.multiple_of(t * ko + k * 32, 32), 32), :] = mine.astype(bf16)
                        elif s == 2:
                            WU[t, pl.ds(pl.multiple_of(f * ku + k * 32, 32), 32), :] = mine.astype(bf16)
                        else:
                            WD[f, pl.ds(pl.multiple_of(t * kd + k * 32, 32), 32), :] = mine.astype(bf16)

    def kick(s):
        own = slot(s, f, t)
        copy(leaving[s] if s < 4 else own, own, sy.at[s], rz.at[s, f], (r, fy, t)).start()
        both_ways(s, f, own)
        to_siblings(s, f, own)

    def kick2(s):
        arrived(slot(s, fy, t), rz.at[s, fy])
        both_ways(s, fy, slot(s, fy, t))
        to_siblings(s, fy, slot(s, fy, t))

    def place(j):
        k = (j + 1) // 2
        sg = 1 - 2 * (j % 2)
        return z + sg * k, z - sg

    def step(s, j):
        zs, nxt = place(j)

        @pl.when(jnp.logical_and(zs >= 0, zs < nz))
        def _():
            for yy in range(2):
                ff = 2 * zs + yy
                arrived(slot(s, ff, t), rz.at[s, ff])

                @pl.when(jnp.logical_and(nxt >= 0, nxt < nz))
                def _():
                    copy(
                        slot(s, ff, t), slot(s, ff, t), sz.at[s, ff, 0], rz.at[s, ff], (r, 2 * nxt + y, t)
                    ).start()

                to_siblings(s, ff, slot(s, ff, t))

    def steps(s, lo, hi):
        @pl.loop(lo, hi)
        def _(j):
            step(s, j)

    def from_siblings(s, ff):
        for tt in siblings():
            arrived(slot(s, ff, tt), rd.at[s, ff])

    def all_from_siblings(s):
        @pl.loop(0, 2 * nz)
        def _(ff):
            from_siblings(s, ff)

    last = 2 * nz - 1

    for fetch in fetches():
        fetch.start()
    if inside:
        at_col = 0
        for v in vectors[:3]:
            packed[:, at_col : at_col + v.shape[1]] = v[...]
            at_col += v.shape[1]
        few = vectors[0].shape[1]
        for k in range(3):
            packed[:, at_col : at_col + few] = vectors[6][k : k + 1, pl.ds(pl.multiple_of(f * few, few), few)]
            at_col += few
        for v in vectors[3:6]:
            packed[:, at_col : at_col + v.shape[1]] = v[...]
            at_col += v.shape[1]
        table[f, t] = packed[...]

    barrier = pltpu.get_barrier_semaphore()
    for m in others():
        pl.semaphore_signal(barrier, inc=1, device_id=member(m), device_id_type=MESH)
    for tt in siblings():
        pl.semaphore_signal(barrier, inc=1, device_id=(r, f, tt), device_id_type=MESH)

    @pl.when(has_lo)
    def _():
        pl.semaphore_signal(barrier, inc=1, device_id=(r, f - 2, t), device_id_type=MESH)

    @pl.when(has_hi)
    def _():
        pl.semaphore_signal(barrier, inc=1, device_id=(r, f + 2, t), device_id_type=MESH)

    pl.semaphore_wait(barrier, G + T - 2 + (z + nz - 1) // nz + (2 * nz - 2 - z) // nz)

    round_stage(0)
    round_stage(1)
    kick(0)
    if inside:
        kick(4)
    kick(1)
    round_stage(2)
    round_stage(3)

    @pl.loop(0, win // TILE)
    def _(i):
        at = pl.ds(pl.multiple_of(i * TILE, TILE), TILE)
        x = tok[pl.ds(pl.multiple_of(start + i * TILE, TILE), TILE), :].astype(f32)
        x = x * lax.rsqrt(jnp.mean(x * x, axis=-1, keepdims=True) + norm_eps) * g1[...]
        nrm[g, at, :] = x.astype(bf16)

    kick2(0)
    if inside:
        kick2(4)
    for m in others():
        copy(nrm.at[g], nrm.at[g], sn.at[m], rn.at[g], member(m)).start()
    kick(2)
    kick2(1)
    steps(0, 1, last)
    if inside:
        steps(4, 1, last)
    kick(3)
    kick2(2)
    steps(1, 1, last)

    all_from_siblings(0)
    for m in others():
        arrived(nrm.at[m], rn.at[m])
    if inside:
        all_from_siblings(4)
        few, ups, outs = vectors[0].shape[1], vectors[3].shape[1], vectors[4].shape[1]
        wide = 3 * vectors[0].shape[1] * 2
        near = 2 * nz // G
        for tt in range(T):
            for j in range(near):
                row_of = table[g * near + j, tt]
                for k in range(3):
                    at_col = (k * near + j) * few
                    asc[tt, :, at_col : at_col + few] = row_of[:, k * few : (k + 1) * few]
                    taps[tt, k : k + 1, j * few : (j + 1) * few] = row_of[:, (3 + k) * few : (4 + k) * few]
                usc[tt, :, j * ups : (j + 1) * ups] = row_of[:, wide : wide + ups]
        for zs in range(nz):
            for yy in range(2):
                row_of = table[2 * zs + yy, 0]
                cols = slice(yy * outs, (yy + 1) * outs)
                oc[zs, :, cols] = row_of[:, wide + ups : wide + ups + outs]
                dc[zs, :, cols] = row_of[:, wide + ups + outs :]
    c = taps.shape[2]

    @pl.loop(0, G)
    def _(gs):
        x = nrm[gs]
        row = lax.broadcasted_iota(jnp.int32, (win, c), 0)
        for tt in range(T):
            prod = jnp.dot(x, WA[tt], preferred_element_type=f32) * asc[tt]
            gated = prod[:, c : 2 * c] * prod[:, :c]
            before = jnp.where(row == 0, 0.0, pltpu.roll(gated, 1, 0))
            after = jnp.where(row == win - 1, 0.0, pltpu.roll(gated, win - 1, 0))
            conv = taps[tt, 0:1] * before + taps[tt, 1:2] * gated + taps[tt, 2:3] * after
            hid[gs, :, tt * c : (tt + 1) * c] = (prod[:, 2 * c :] * conv).astype(bf16)

    all_from_siblings(1)

    @pl.loop(0, nz)
    def _(zs):
        @pl.loop(0, G)
        def _(gs):
            h = hid[gs, pl.ds(off, rows), :]
            for yy in range(2):
                p1[gs, zs, :, yy * cw : (yy + 1) * cw] = jnp.dot(
                    h, WO[2 * zs + yy], preferred_element_type=f32
                ).astype(bf16)

    kick2(3)
    for m in others():
        copy(p1.at[m], q1.at[g], s1.at[m], r1.at[g], member(m)).start()
    cut = (2 * last) // 3
    steps(2, 1, cut)

    for m in others():
        arrived(q1.at[m], r1.at[m])

    def total(p, q, zs, at):
        acc = p[g, zs, at, :].astype(f32)
        for m in others():
            acc = acc + q[m, zs, at, :].astype(f32)
        return acc

    @pl.loop(0, rows // TILE)
    def _(i):
        at = pl.ds(pl.multiple_of(i * TILE, TILE), TILE)
        here = pl.ds(pl.multiple_of(t * rows + i * TILE, TILE), TILE)
        ssq = jnp.zeros((TILE, 1), f32)
        for zs in range(nz):
            m = tok[here, zs * pw : (zs + 1) * pw].astype(f32) + total(p1, q1, zs, at) * oc[zs]
            mid32[zs, at, :] = m
            ssq = ssq + jnp.sum(m * m, axis=-1, keepdims=True)
        inv = lax.rsqrt(ssq / D + norm_eps)
        for zs in range(nz):
            cols = slice(zs * pw, (zs + 1) * pw)
            mid[g, at, cols] = (mid32[zs, at, :] * inv * g2[:, cols]).astype(bf16)

    steps(2, cut, cut + 1)
    for m in others():
        copy(mid.at[g], mid.at[g], sa.at[m], ra.at[g], member(m)).start()
    steps(2, cut + 1, last)
    cut2 = (last + 1) // 2
    steps(3, 1, cut2)

    all_from_siblings(2)
    for m in others():
        arrived(mid.at[m], ra.at[m])
    u = usc.shape[2]

    @pl.loop(0, G)
    def _(gs):
        x = mid[gs]
        for tt in range(T):
            upper = jnp.dot(x, WU[tt], preferred_element_type=f32) * usc[tt]
            act[gs, :, tt * u : (tt + 1) * u] = jnp.square(jnp.maximum(upper, 0.0)).astype(bf16)

    def down(j):
        zs, _ = place(j)

        @pl.when(jnp.logical_and(zs >= 0, zs < nz))
        def _():
            for yy in range(2):
                from_siblings(3, 2 * zs + yy)

            @pl.loop(0, G)
            def _(gs):
                x = act[gs]
                for yy in range(2):
                    p2[gs, zs, :, yy * cw : (yy + 1) * cw] = jnp.dot(
                        x, WD[2 * zs + yy], preferred_element_type=f32
                    ).astype(bf16)

            for m in others():
                copy(p2.at[m, zs], q2.at[g, zs], s2.at[m, zs], r2.at[g, zs], member(m)).start()

    @pl.loop(0, last)
    def _(j):
        @pl.when(j >= cut2)
        def _():
            step(3, j)

        down(j)

    @pl.loop(0, nz)
    def _(zs):
        for m in others():
            arrived(q2.at[m, zs], r2.at[m, zs])

    @pl.loop(0, rows // TILE)
    def _(i):
        at = pl.ds(pl.multiple_of(i * TILE, TILE), TILE)
        here = pl.ds(pl.multiple_of(t * rows + i * TILE, TILE), TILE)
        for zs in range(nz):
            out[here, zs * pw : (zs + 1) * pw] = (
                mid32[zs, at, :] + total(p2, q2, zs, at) * dc[zs]
            ).astype(bf16)

    def half(tt):
        return out.at[pl.ds(pl.multiple_of(tt * rows, rows), rows)]

    for tt in siblings():
        copy(half(t), half(t), so.at[tt], ro.at[t], (r, f, tt)).start()

    for s in stages:
        own = slot(s, f, t)
        arrived(own, sy.at[s])

        def gone(ff, k, s=s, own=own):
            arrived(own, sz.at[s, ff, k])

        for ff in (f, fy):
            pl.when(has_lo)(functools.partial(gone, ff, 0))
            pl.when(has_hi)(functools.partial(gone, ff, 1))

        @pl.loop(1, last)
        def _(j):
            zs, nxt = place(j)
            ok = jnp.logical_and(zs >= 0, zs < nz)

            @pl.when(jnp.logical_and(ok, jnp.logical_and(nxt >= 0, nxt < nz)))
            def _():
                for yy in range(2):
                    gone(2 * zs + yy, 0)

        @pl.loop(0, 2 * nz)
        def _(ff):
            for _ in siblings():
                arrived(own, sd.at[s, ff])

    for m in others():
        arrived(nrm.at[m], sn.at[m])
        arrived(p1.at[m], s1.at[m])
        arrived(mid.at[m], sa.at[m])

        @pl.loop(0, nz)
        def _(zs):
            arrived(p2.at[m, zs], s2.at[m, zs])

    for tt in siblings():
        arrived(half(tt), ro.at[tt])
        arrived(half(tt), so.at[tt])


def line_kernel(
    nz, G, T, win, rows, inside,
    tok, g1, g2, vectors, weights,
    out,
    WA, WO, WU, WD, nrm, hid, p, q, mid32, mid, act, fin,
    staged, leaving, gathered, detour,
    rz, rd, re, sz, sd, sy, loc, rn, rb, rh, rt, sn, sh, st, r1, s1, ra, sa, r2, s2, ro, so, fo,
):
    packed, table, asc, taps, usc, oc, dc = gathered
    D = tok.shape[1]
    pw = D // nz
    cw = pw // 2
    r, f, t = lax.axis_index("rep"), lax.axis_index("fs"), lax.axis_index("tp")
    z, y = f // 2, f % 2
    fy = z * 2 + 1 - y
    g = r * 2 + y
    ka, ko, ku, kd = (w.shape[0] for w in leaving)
    outer = jnp.logical_or(z == 0, z == nz - 1)
    inner = jnp.logical_not(outer)
    inward = jnp.where(2 * z < nz, 1, -1)
    across = z + 2 * inward
    if T == 2:
        start, off = t * (rows - HALO), t * HALO
    else:
        start = jnp.clip(t * rows - HALO, 0, tok.shape[0] - win)
        off = t * rows - start
    start, off = pl.multiple_of(start, HALO), pl.multiple_of(off, HALO)

    def member(m):
        return (m // 2, z * 2 + m % 2, t)

    def others():
        return [(g + d) % G for d in range(1, G)]

    gx, gy, gd = (1 - r) * 2 + y, r * 2 + 1 - y, (1 - r) * 2 + 1 - y

    def peers():
        return [gd, gx, gy]

    def siblings():
        return [(t + d) % T for d in range(1, T)]

    def copy(src, dst, ssem, rsem, dev):
        return pltpu.make_async_remote_copy(
            src_ref=src, dst_ref=dst, send_sem=ssem, recv_sem=rsem, device_id=dev, device_id_type=MESH
        )

    def arrived(ref, sem):
        pltpu.make_async_copy(ref, ref, sem).wait()

    def slot(s, ff, tt):
        if s == 0:
            return WA.at[tt, pl.ds(pl.multiple_of(ff * ka, ka), ka)]
        if s == 1:
            return WO.at[ff, pl.ds(pl.multiple_of(tt * ko, ko), ko)]
        if s == 2:
            return WU.at[tt, pl.ds(pl.multiple_of(ff * ku, ku), ku)]
        if s == 3:
            return WD.at[ff, pl.ds(pl.multiple_of(tt * kd, kd), kd)]
        return table.at[ff, tt]

    def to_siblings(s, ff, src):
        for tt in siblings():
            copy(src, slot(s, ff, t), sd.at[s], rd.at[s // 2, ff] if s % 2 else re.at[s // 2], (r, f, tt)).start()

    def send(s, ff, zs):
        block = slot(s, ff, t)
        copy(block, block, sz.at[s], rz.at[s, ff], (r, 2 * zs + y, t)).start()

    def send_in(s, ff):
        send(s, ff, z + inward)

    def send_out(s, ff):
        send(s, ff, z - inward)

    def spread(s, ff):
        send_in(s, ff)

        @pl.when(inner)
        def _():
            send_out(s, ff)

        @pl.when(outer)
        def _():
            send(s, ff, across)

    def fetches():
        for i, w in enumerate(weights):
            src, dst = weights[i], staged[i]
            if w.shape[1] > dst.shape[1]:
                n = dst.shape[1]
                src = src.at[:, pl.ds(pl.multiple_of(r * n, n), n)]
            elif w.shape[0] > dst.shape[0]:
                n = dst.shape[0]
                src = src.at[pl.ds(pl.multiple_of(r * n, n), n)]
            yield pltpu.make_async_copy(src, dst, loc.at[i])

    def round_stage(s):
        parts = {0: (0, 1, 2), 1: (3,), 2: (4,), 3: (5,)}[s]
        high = leaving[s].shape[0]
        for i in parts:
            pltpu.make_async_copy(staged[i], staged[i], loc.at[i]).wait()
        for yy in range(2):

            @pl.when(y == yy)
            def _():
                @pl.loop(0, high // 32)
                def _(k):
                    at = pl.ds(pl.multiple_of(k * 32, 32), 32)
                    for n, i in enumerate(parts):
                        if s in (0, 2):
                            wide = staged[i].shape[1] // 2
                            mine = staged[i][at, yy * wide : (yy + 1) * wide]
                            theirs = staged[i][at, (1 - yy) * wide : (2 - yy) * wide]
                        else:
                            wide = staged[i].shape[1]
                            mine = staged[i][pl.ds(pl.multiple_of(yy * high + k * 32, 32), 32), :]
                            theirs = staged[i][pl.ds(pl.multiple_of((1 - yy) * high + k * 32, 32), 32), :]
                        cols = slice(n * wide, (n + 1) * wide)
                        leaving[s][at, cols] = theirs.astype(bf16)
                        if s == 0:
                            WA[t, pl.ds(pl.multiple_of(f * ka + k * 32, 32), 32), cols] = mine.astype(bf16)
                        elif s == 1:
                            WO[f, pl.ds(pl.multiple_of(t * ko + k * 32, 32), 32), :] = mine.astype(bf16)
                        elif s == 2:
                            WU[t, pl.ds(pl.multiple_of(f * ku + k * 32, 32), 32), :] = mine.astype(bf16)
                        else:
                            WD[f, pl.ds(pl.multiple_of(t * kd + k * 32, 32), 32), :] = mine.astype(bf16)

    def swap(s):
        own = slot(s, f, t)
        copy(leaving[s] if s < 4 else own, own, sy.at[s], rz.at[s, f], (r, fy, t)).start()

    def swapped(s):
        arrived(slot(s, fy, t), rz.at[s, fy])

    def both_to_siblings(s):
        for ff in (f, fy):
            to_siblings(s, ff, slot(s, ff, t))

    def place(j):
        return (z + inward * j + nz) % nz

    blocks = 2 * (nz - 1)

    def block(i):
        return place(1 + i // 2), (y + i) % 2

    def step(s, i):
        zs, yy = block(i)
        ff = 2 * zs + yy
        arrived(slot(s, ff, t), rz.at[s, ff])

        @pl.when(inner & (zs != z - inward))
        def _():
            send_out(s, ff)

        to_siblings(s, ff, slot(s, ff, t))

    def inner_step(s, near, late):
        ff = 2 * place(near) + (y + late) % 2
        arrived(slot(s, ff, t), rz.at[s, ff])
        if s and near < nz - 1:
            send_out(s, ff)
        elif s == 0 and near == nz - 1:
            send_in(0, ff)
        to_siblings(s, ff, slot(s, ff, t))

    def steps(s, lo, hi):
        @pl.loop(lo, hi)
        def _(j):
            step(s, j)

    def from_siblings(s, ff):
        for tt in siblings():
            arrived(slot(s, ff, tt), rd.at[s // 2, ff])

    def part_of(s, tt, n):
        if s == 0:
            return WA.at[tt, pl.ds(0, n * ka)]
        if s == 1:
            return WO.at[pl.ds(0, n), pl.ds(pl.multiple_of(tt * ko, ko), ko)]
        if s == 2:
            return WU.at[tt, pl.ds(0, n * ku)]
        if s == 3:
            return WD.at[pl.ds(0, n), pl.ds(pl.multiple_of(tt * kd, kd), kd)]
        return table.at[pl.ds(0, n), tt]

    def all_from_siblings(s):
        for tt in siblings():
            arrived(part_of(s, tt, 2 * nz), re.at[s // 2])

    for fetch in fetches():
        fetch.start()
    if inside:
        at_col = 0
        for v in vectors[:3]:
            packed[:, at_col : at_col + v.shape[1]] = v[...]
            at_col += v.shape[1]
        few = vectors[0].shape[1]
        for k in range(3):
            packed[:, at_col : at_col + few] = vectors[6][k : k + 1, pl.ds(pl.multiple_of(f * few, few), few)]
            at_col += few
        for v in vectors[3:6]:
            for k in range(v.shape[0]):
                packed[:, at_col : at_col + v.shape[1]] = v[k : k + 1, :]
                at_col += v.shape[1]
        table[f, t] = packed[...]

    barrier = pltpu.get_barrier_semaphore()
    for m in others():
        pl.semaphore_signal(barrier, inc=1, device_id=member(m), device_id_type=MESH)
    for tt in siblings():
        pl.semaphore_signal(barrier, inc=1, device_id=(r, f, tt), device_id_type=MESH)

    for zs in (z - 1, z + 1, across):
        near = jnp.logical_and(zs >= 0, zs < nz)

        @pl.when(jnp.logical_and(near, zs != z))
        def _():
            pl.semaphore_signal(barrier, inc=1, device_id=(r, 2 * zs + y, t), device_id_type=MESH)

    round_stage(0)
    round_stage(1)
    pl.semaphore_wait(barrier, G + T - 2 + jnp.where(outer, 2, 3))
    swap(0)
    send_in(0, f)
    swap(4)
    swap(1)

    @pl.when(inner)
    def _():
        for s in (4, 1):
            spread(s, f)

    round_stage(2)
    round_stage(3)

    @pl.when(inner)
    def _():
        for s in (2, 3):
            send_out(s, f)
        for i in range(2):
            copy(leaving[2 + i], detour[i], st.at[i], rt.at[i], (r, 2 * (z - inward) + y, t)).start()

    @pl.loop(0, win // TILE)
    def _(i):
        at = pl.ds(pl.multiple_of(i * TILE, TILE), TILE)
        x = tok[pl.ds(pl.multiple_of(start + i * TILE, TILE), TILE), :].astype(f32)
        x = x * lax.rsqrt(jnp.mean(x * x, axis=-1, keepdims=True) + norm_eps) * g1[...]
        nrm[g, at, :] = x.astype(bf16)

    low = win // 2 // TILE * TILE

    def rows_of(i, lower):
        return nrm.at[i, pl.ds(0, low)] if lower else nrm.at[i, pl.ds(low, win - low)]

    def offer(base, sem):
        for m in (gx, gy):
            copy(nrm.at[base + g], nrm.at[base + g], sn, sem.at[g], member(m)).start()

    def pass_on(base, sem, from_x):
        m, n = (gx, gy) if from_x else (gy, gx)
        arrived(nrm.at[base + m], sem.at[m])
        some = rows_of(base + m, not from_x)
        copy(some, some, sn, sem.at[m] if from_x else sem.at[G], member(n)).start()

    def passed(base, sem):
        arrived(rows_of(base + gd, False), sem.at[gd])
        arrived(rows_of(base + gd, True), sem.at[G])

    def project(base, gs):
        x = nrm[base + gs]
        row = lax.broadcasted_iota(jnp.int32, (win, c), 0)
        for tt in range(T):
            prod = jnp.dot(x, WA[tt], preferred_element_type=f32) * asc[tt]
            gated = prod[:, c : 2 * c] * prod[:, :c]
            before = jnp.where(row == 0, 0.0, pltpu.roll(gated, 1, 0))
            after = jnp.where(row == win - 1, 0.0, pltpu.roll(gated, win - 1, 0))
            conv = taps[tt, 0:1] * before + taps[tt, 1:2] * gated + taps[tt, 2:3] * after
            hid[base + gs, :, tt * c : (tt + 1) * c] = (prod[:, 2 * c :] * conv).astype(bf16)

    def nth(k):
        return jnp.where(k == 0, g, jnp.where(k == 1, gx, jnp.where(k == 2, gy, gd)))

    def unpack():
        few, ups, outs = vectors[0].shape[1], vectors[3].size, vectors[4].shape[1]
        wide = 3 * vectors[0].shape[1] * 2
        near = 2 * nz // G
        for tt in range(T):
            for j in range(near):
                row_of = table[g * near + j, tt]
                for k in range(3):
                    at_col = (k * near + j) * few
                    asc[tt, :, at_col : at_col + few] = row_of[:, k * few : (k + 1) * few]
                    taps[tt, k : k + 1, j * few : (j + 1) * few] = row_of[:, (3 + k) * few : (4 + k) * few]
                usc[tt, :, j * ups : (j + 1) * ups] = row_of[:, wide : wide + ups]
        for zs in range(nz):
            for yy in range(2):
                row_of = table[2 * zs + yy, 0]
                cols = slice(yy * outs, (yy + 1) * outs)
                oc[zs, :, cols] = row_of[:, wide + ups : wide + ups + outs]
                dc[zs, :, cols] = row_of[:, wide + ups + outs :]
    c = taps.shape[2]

    def hand_over(gs):
        here = pl.ds(off, rows)
        copy(hid.at[G + gs, here], hid.at[gs, here], sh, rh.at[gs], (r, 2 * (z - inward) + y, t)).start()

    def project_far(lo, hi):
        @pl.loop(lo, hi)
        def _(k):
            gs = nth(k)

            @pl.when(k == G - 1)
            def _():
                passed(G, rb)

            project(G, gs)
            hand_over(gs)

    @pl.when(outer)
    def _():
        swap(2)
        swap(3)
        spread(4, f)
        swapped(0)
        send_in(0, fy)
        swapped(4)
        spread(4, fy)
        copy(nrm.at[g], nrm.at[G + g], sn, rb.at[g], (r, 2 * (z + inward) + y, t)).start()
        spread(1, f)
        swapped(1)
        spread(1, fy)
        for s in (4, 1):
            both_to_siblings(s)
        spread(2, f)
        for i in range(2):
            arrived(detour[i], rt.at[i])
            ff = 2 * (z + inward) + y
            copy(detour[i], slot(2 + i, ff, t), st.at[i], rz.at[2 + i, ff], (r, fy, t)).start()
        def give_back(i):
            ff = 2 * (z + inward) + 1 - y
            arrived(slot(2 + i, ff, t), rz.at[2 + i, ff])
            send_in(2 + i, ff)
            to_siblings(2 + i, ff, slot(2 + i, ff, t))

        give_back(0)
        swapped(2)
        spread(2, fy)
        both_to_siblings(2)
        give_back(1)
        swapped(3)
        for ff in (f, fy):
            send(3, ff, across)
            send_in(3, ff)
        both_to_siblings(3)
        steps(4, 0, blocks)
        steps(1, 0, blocks)
        all_from_siblings(4)
        unpack()

    @pl.when(inner)
    def _():
        offer(0, rn)
        swapped(0)
        send_in(0, fy)
        both_to_siblings(0)
        inner_step(0, 3, 0)
        inner_step(0, 1, 0)
        for s in (4, 1):
            swapped(s)
            spread(s, fy)
            both_to_siblings(s)
        pass_on(0, rn, True)
        inner_step(0, 2, 0)
        inner_step(0, 1, 1)
        pass_on(0, rn, False)
        inner_step(0, 3, 1)
        arrived(nrm.at[G + g], rb.at[g])
        offer(G, rb)
        inner_step(0, 2, 1)
        for s in (2, 3):
            send_in(s, f)
        all_from_siblings(0)
        steps(4, 0, blocks)
        all_from_siblings(4)
        unpack()
        steps(1, 0, blocks)
        passed(0, rn)
        @pl.loop(0, G)
        def _(gs):
            project(0, gs)
    @pl.when(inner)
    def _():
        project(G, g)
        pass_on(G, rb, True)
        pass_on(G, rb, False)

    def pair(ref, i, zs):
        return ref.at[i, pl.ds(2 * zs, 2)]

    def legs(zs):
        even = zs % 2 == 0
        return jnp.where(even, gx, gy), jnp.where(even, gy, gx)

    def first_leg(zs):
        first, _ = legs(zs)
        copy(pair(p, gd, zs), pair(q, 1, zs), s1, r1.at[1, zs], member(first)).start()
        copy(pair(p, first, zs), pair(q, 0, zs), s1, r1.at[0, zs], member(first)).start()

    def own_leg(j, k):
        zs = 2 * j + k
        first, _ = legs(zs)
        copy(pair(p, first, zs), pair(q, 0, zs), s1, r1.at[0, zs], member(first)).start()

    def pass_leg(zs):
        first, _ = legs(zs)
        copy(pair(p, gd, zs), pair(q, 1, zs), s1, r1.at[1, zs], member(first)).start()

    pl.when(inner)(lambda: project_far(1, 3))

    @pl.loop(0, 2 * nz)
    def _(ff):
        from_siblings(1, ff)

    @pl.loop(0, G)
    def _(k):
        gs = nth((k + 1) % G)

        @pl.when(outer)
        def _():
            some = hid.at[gs, pl.ds(off, rows)]
            arrived(some, rh.at[gs])

        @pl.loop(0, 2 * nz)
        def _(ff):
            h = hid[gs, pl.ds(off, rows), :]
            p[gs, ff] = jnp.dot(h, WO[ff], preferred_element_type=f32).astype(bf16)

        @pl.when(outer & (k < 2))
        def _():
            pl.loop(0, nz // 2)(lambda j: own_leg(j, k))

        @pl.when(outer & (k == 2))
        def _():
            pl.loop(0, nz)(pass_leg)

    @pl.when(inner)
    def _():
        pl.loop(0, nz)(pass_leg)
        for k in range(2):
            pl.loop(0, nz // 2)(lambda j: own_leg(j, k))
        project_far(3, G)
        hand_over(g)
        inner_step(2, 1, 0)
        inner_step(2, 2, 0)

    @pl.loop(0, nz)
    def _(j):
        zs = place(j)
        _, second = legs(zs)
        arrived(pair(q, 1, zs), r1.at[1, zs])

        @pl.loop(0, rows // TILE)
        def _(k):
            at = pl.ds(pl.multiple_of(k * TILE, TILE), TILE)
            for yy in range(2):
                both = p[second, 2 * zs + yy, at, :].astype(f32) + q[1, 2 * zs + yy, at, :].astype(f32)
                p[second, 2 * zs + yy, at, :] = both.astype(bf16)

        copy(pair(p, second, zs), pair(q, 2, zs), s1, r1.at[2, zs], member(second)).start()

    @pl.when(inner)
    def _():
        swapped(2)
        send_in(2, fy)
        both_to_siblings(2)
        inner_step(2, 2, 1)

    pl.when(outer)(lambda: steps(2, 0, 1))
    @pl.loop(0, nz)
    def _(zs):
        for i in (0, 2):
            arrived(pair(q, i, zs), r1.at[i, zs])

    @pl.loop(0, rows // TILE)
    def _(i):
        at = pl.ds(pl.multiple_of(i * TILE, TILE), TILE)
        here = pl.ds(pl.multiple_of(t * rows + i * TILE, TILE), TILE)
        ssq = jnp.zeros((TILE, 1), f32)
        for ff in range(2 * nz):
            half = slice(ff % 2 * cw, (ff % 2 + 1) * cw)
            acc = p[g, ff, at, :].astype(f32) + q[0, ff, at, :].astype(f32) + q[2, ff, at, :].astype(f32)
            m = tok[here, ff * cw : (ff + 1) * cw].astype(f32) + acc * oc[ff // 2, :, half]
            mid32[ff // 2, at, half] = m
            ssq = ssq + jnp.sum(m * m, axis=-1, keepdims=True)
        inv = lax.rsqrt(ssq / D + norm_eps)
        for zs in range(nz):
            cols = slice(zs * pw, (zs + 1) * pw)
            mid[g, at, cols] = (mid32[zs, at, :] * inv * g2[:, cols]).astype(bf16)

    part = rows // 2

    def half_of(m, h):
        return mid.at[m, pl.ds(h * part, part)]

    for h in range(2):
        for m, way in ((gx, 1 - h), (gy, h)):
            copy(half_of(g, way), half_of(g, way), sa, ra.at[g, way], member(m)).start()
    @pl.when(outer)
    def _():
        steps(2, 2, 3)
        steps(2, 4, 5)


    @pl.when(inner)
    def _():
        inner_step(2, 1, 1)
        inner_step(3, 1, 0)
        swapped(3)
        send_in(3, fy)
        both_to_siblings(3)

    for m, n, h in ((gx, gy, 1), (gy, gx, 0)):
        arrived(half_of(m, h), ra.at[m, h])
        copy(half_of(m, h), half_of(m, h), sa, ra.at[m, h], member(n)).start()
    @pl.when(outer)
    def _():
        steps(2, 5, 6)
        steps(2, 3, 4)


    @pl.when(inner)
    def _():
        inner_step(2, 3, 0)
        inner_step(2, 3, 1)
        inner_step(3, 1, 1)

    all_from_siblings(2)
    u = usc.shape[2]
    arrived(p.at[pl.ds(0, G - 1)], s1)

    @pl.loop(0, G)
    def _(k):
        gs = nth(k)

        @pl.when((k == 1) | (k == G - 1))
        def _():
            arrived(half_of(gs, 0), ra.at[gs, 0])

        @pl.when(k > 1)
        def _():
            arrived(half_of(gs, 1), ra.at[gs, 1])

        x = mid[gs]
        for tt in range(T):
            upper = jnp.dot(x, WU[tt], preferred_element_type=f32) * usc[tt]
            act[gs, :, tt * u : (tt + 1) * u] = jnp.square(jnp.maximum(upper, 0.0)).astype(bf16)

    @pl.when(inner)
    def _():
        inner_step(3, 2, 0)

    def source(i):
        zs, yy = block(jnp.maximum(i - 2, 0))
        zs, yy = jnp.where(i < 2, z, zs), jnp.where(i < 2, (y + i) % 2, yy)
        return zs, yy, 2 * zs + yy

    def direct(i):
        return outer & (i > 5)

    def second_leg(i):
        _, _, ff = source(i)
        _, second = legs(ff)

        @pl.when(jnp.logical_not(direct(i)))
        def _():
            arrived(q.at[1, ff], r2.at[1, ff])

            @pl.loop(0, rows // TILE)
            def _(k):
                at = pl.ds(pl.multiple_of(k * TILE, TILE), TILE)
                both = p[second, ff, at, :].astype(f32) + q[1, ff, at, :].astype(f32)
                p[second, ff, at, :] = both.astype(bf16)

            copy(p.at[second, ff], q.at[2, ff], s2, r2.at[2, ff], member(second)).start()

    def finish(i):
        zs, yy, ff = source(i)
        wide = pl.ds(pl.multiple_of(yy * cw, cw), cw)
        cols = pl.ds(pl.multiple_of(ff * cw, cw), cw)

        def sum_up(slots):
            for m in slots:
                arrived(q.at[m, ff], r2.at[m, ff])

            @pl.loop(0, rows // TILE)
            def _(k):
                at = pl.ds(pl.multiple_of(k * TILE, TILE), TILE)
                acc = p[g, ff, at, :].astype(f32)
                for m in slots:
                    acc = acc + q[m, ff, at, :].astype(f32)
                fin[ff, at, :] = (mid32[zs, at, wide] + acc * dc[zs, :, wide]).astype(bf16)

        far = direct(i)
        pl.when(far)(lambda: sum_up((0, 1, 2)))
        pl.when(jnp.logical_not(far))(lambda: sum_up((0, 2)))
        mine = out.at[pl.ds(pl.multiple_of(t * rows, rows), rows), cols]
        for tt in siblings():
            copy(fin.at[ff], mine, so, ro, (r, f, tt)).start()
        pltpu.make_async_copy(fin.at[ff], mine, fo).start()

    @pl.loop(0, 2 * nz)
    def _(ff_at):
        _, _, ff = source(ff_at)

        @pl.when(ff_at > 1)
        def _():
            second_leg(ff_at - 2)

        @pl.when(outer & (ff_at > 1) & (ff_at != 3))
        def _():
            step(3, ff_at - 2)

        for at, near, late in ((3, 2, 1), (6, 3, 0), (7, 3, 1)):
            pl.when(inner & (ff_at == at))(functools.partial(inner_step, 3, near, late))

        from_siblings(3, ff)

        first, second = legs(ff)
        far = direct(ff_at)

        @pl.loop(0, G)
        def _(k):
            gs = jnp.where(k == 0, gd, jnp.where(k == 1, first, jnp.where(k == 2, second, g)))
            p[gs, ff] = jnp.dot(act[gs], WD[ff], preferred_element_type=f32).astype(bf16)

            @pl.when(k == 0)
            def _():
                to = member(jnp.where(far, gd, first))
                copy(p.at[gd, ff], q.at[1, ff], s2, r2.at[1, ff], to).start()

            @pl.when(k == 1)
            def _():
                copy(p.at[first, ff], q.at[0, ff], s2, r2.at[0, ff], member(first)).start()

            @pl.when(far & (k == 2))
            def _():
                copy(p.at[second, ff], q.at[2, ff], s2, r2.at[2, ff], member(second)).start()

        @pl.when(ff_at > 5)
        def _():
            finish(ff_at - 6)

    second_leg(2 * nz - 2)
    pl.loop(2, 4)(finish)
    second_leg(2 * nz - 1)
    pl.loop(4, 2 * nz)(finish)

    for s in range(5):
        if s in (2, 3):
            pl.when(outer)(functools.partial(arrived, slot(s, f, t), sy.at[s]))
        else:
            arrived(slot(s, f, t), sy.at[s])
        few_sent, many_sent = {0: (2, 4), 2: (5, 7), 3: (5, 7)}.get(s, (4, 8))

        @pl.when(outer)
        def _():
            arrived(part_of(s, t, few_sent), sz.at[s])

        @pl.when(inner)
        def _():
            arrived(part_of(s, t, many_sent), sz.at[s])

        def gone(s=s):
            for _ in siblings():
                arrived(part_of(s, t, 2 * nz), sd.at[s])

        if s == 0:
            pl.when(inner)(gone)
        else:
            gone()

    @pl.when(outer)
    def _():
        arrived(nrm.at[0], sn)

    @pl.when(inner)
    def _():
        arrived(nrm.at[pl.ds(0, 2 * (G - 1))], sn)
        arrived(hid.at[pl.ds(0, G), pl.ds(0, rows)], sh)

    for i in range(2):
        arrived(detour[i], st.at[i])
    arrived(mid.at[pl.ds(0, G - 1)], sa)
    arrived(p.at[pl.ds(0, G - 1)], s2)
    half = out.at[pl.ds(0, rows)]
    for _ in siblings():
        arrived(half, ro)
        arrived(fin, so)
    pltpu.make_async_copy(fin, fin, fo).wait()


def body(
    R, n_fs, T,
    tokens, mix_gain, value_weight, value_scale, inner_weight, inner_scale, outer_weight, outer_scale,
    conv_taps, out_weight, out_scale, mlp_gain, up_weight, up_scale, down_weight, down_scale,
):
    G, nz = 2 * R, n_fs // 2
    TOK, D = tokens.shape[1:]
    rows = TOK // T
    win = TOK if T == 1 else rows + HALO if T == 2 else rows + 2 * HALO
    r, f = lax.axis_index("rep"), lax.axis_index("fs")
    g = r * 2 + f % 2

    vs, us, os = value_scale.shape[0], up_scale.shape[0], out_scale.shape[0]
    inside = all(n % 128 == 0 for n in (vs, us, os))
    lined = inside and T == 2 and nz == 4 and R == 2
    c, u = conv_taps.shape[1] // G, up_weight.shape[1] // G
    if inside:
        scales = (value_scale, inner_scale, outer_scale, up_scale, out_scale, down_scale)
        wide = 128 if lined else us
        vectors = tuple(v.reshape(-1, wide) if v is up_scale else v[None] for v in scales) + (conv_taps,)
    else:
        tap = lax.dynamic_slice_in_dim(conv_taps, f * vs, vs, axis=1)
        packed = jnp.concatenate(
            [value_scale, inner_scale, outer_scale, tap[0], tap[1], tap[2], up_scale, out_scale, down_scale]
        )
        every = lax.all_gather(packed, ("tp", "fs"), axis=0, tiled=False).reshape(T, n_fs, -1)

        def block(v):
            return lax.dynamic_index_in_dim(v.reshape(T, G, -1), g, axis=1, keepdims=True)

        small = [block(every[:, :, i * vs : (i + 1) * vs]) for i in range(6)]
        asc = jnp.concatenate(small[:3], axis=2)
        taps = jnp.concatenate(small[3:], axis=1)
        usc = block(every[:, :, 6 * vs : 6 * vs + us])
        oc = every[0, :, 6 * vs + us : 6 * vs + us + os].reshape(nz, 1, -1)
        dc = every[0, :, 6 * vs + us + os :].reshape(nz, 1, -1)
        vectors = (asc, taps, usc, oc, dc)
    weights = (value_weight, inner_weight, outer_weight, out_weight, up_weight, down_weight)
    ka, ko, kd = value_weight.shape[0], out_weight.shape[0] // G, down_weight.shape[0] // G
    cw = out_weight.shape[1]
    rounded = [(ka, 3 * c), (ko, cw), (ka, u), (kd, cw)]
    staged = [(ka, 2 * c)] * 3 + [(2 * ko, cw), (ka, 2 * u), (2 * kd, cw)]
    gathered = ()
    if inside:
        L = 6 * vs + us + 2 * os
        small = [(1, L), (n_fs, T, 1, L), (T, 1, 3 * c), (T, 3, c), (T, 1, u), (nz, 1, 2 * cw), (nz, 1, 2 * cw)]
        gathered = tuple(pltpu.VMEM(shape, f32) for shape in small)
    pw = D // nz
    dma = pltpu.SemaphoreType.DMA
    vmem = pl.BlockSpec(memory_space=pltpu.VMEM)
    hbm = pl.BlockSpec(memory_space=pl.ANY)
    held = [
        pltpu.VMEM((T, D, 3 * c), bf16),
        pltpu.VMEM((n_fs, T * ko, cw), bf16),
        pltpu.VMEM((T, D, u), bf16),
        pltpu.VMEM((n_fs, T * kd, cw), bf16),
        pltpu.VMEM((2 * G if lined else G, win, D), bf16),
        pltpu.VMEM((2 * G if lined else G, win, T * ko), bf16),
    ]
    reading = [
        tuple(pltpu.VMEM(shape, f32) for shape in staged),
        tuple(pltpu.VMEM(shape, bf16) for shape in rounded),
        gathered,
    ]
    if lined:
        run = line_kernel
        limit = 65000000
        scratch = [
            *held,
            pltpu.VMEM((G, n_fs, rows, cw), bf16),
            pltpu.VMEM((G - 1, n_fs, rows, cw), bf16),
            pltpu.VMEM((nz, rows, pw), f32),
            pltpu.VMEM((G, rows, D), bf16),
            pltpu.VMEM((G, rows, T * kd), bf16),
            pltpu.VMEM((n_fs, rows, cw), bf16),
            *reading,
            tuple(pltpu.VMEM(shape, bf16) for shape in rounded[2:]),
            dma((5, n_fs)),
            dma((2, n_fs)),
            dma((3,)),
            dma((5,)),
            dma((5,)),
            dma((5,)),
            dma((6,)),
            dma((G + 1,)),
            dma((G + 1,)),
            dma((G,)),
            dma((2,)),
            dma,
            dma,
            dma((2,)),
            dma((G - 1, nz)),
            dma,
            dma((G, 2)),
            dma,
            dma((G - 1, n_fs)),
            dma,
            dma,
            dma,
            dma,
        ]
    else:
        run = kernel
        limit = 65000000
        scratch = [
            *held,
            pltpu.VMEM((G, nz, rows, pw), bf16),
            pltpu.VMEM((G, nz, rows, pw), bf16),
            pltpu.VMEM((nz, rows, pw), f32),
            pltpu.VMEM((G, rows, D), bf16),
            pltpu.VMEM((G, rows, T * kd), bf16),
            pltpu.VMEM((G, nz, rows, pw), bf16),
            pltpu.VMEM((G, nz, rows, pw), bf16),
            *reading,
            dma((5, n_fs)),
            dma((5, n_fs)),
            dma((5, n_fs, 2)),
            dma((5, n_fs)),
            dma((5,)),
            dma((6,)),
            dma((G,)),
            dma((G,)),
            dma((G,)),
            dma((G,)),
            dma((G,)),
            dma((G,)),
            dma((G, nz)),
            dma((G, nz)),
            dma((T,)),
            dma((T,)),
        ]
    result = pl.pallas_call(
        functools.partial(run, nz, G, T, win, rows, inside),
        out_shape=jax.ShapeDtypeStruct((TOK, D), bf16),
        in_specs=[vmem] * 3 + [(vmem,) * len(vectors), (hbm,) * 6],
        out_specs=hbm if lined else vmem,
        scratch_shapes=scratch,
        compiler_params=pltpu.CompilerParams(collective_id=0, has_side_effects=True, vmem_limit_bytes=limit),
    )(tokens[0], mix_gain[None], mlp_gain[None], vectors, weights)
    return result[None]


def solution(mesh):
    placed = (
        P(("rep", "fs"), None, None),
        P(),
        P("fs", "tp"),
        P(("tp", "fs")),
        P("fs", "tp"),
        P(("tp", "fs")),
        P("fs", "tp"),
        P(("tp", "fs")),
        P(None, "tp"),
        P("tp", "fs"),
        P("fs"),
        P(),
        P("fs", "tp"),
        P(("tp", "fs")),
        P("tp", "fs"),
        P("fs"),
    )
    sizes = (mesh.shape["rep"], mesh.shape["fs"], mesh.shape["tp"])
    return jax.shard_map(
        functools.partial(body, *sizes),
        mesh=mesh,
        in_specs=placed,
        out_specs=P(("rep", "fs"), None, None),
        check_vma=False,
    )
```

```python
import functools

import jax
import jax.numpy as jnp
from jax import lax
from jax.experimental import pallas as pl
from jax.experimental.pallas import tpu as pltpu
from jax.sharding import PartitionSpec as P

MESH = pl.DeviceIdType.MESH
norm_eps = 1e-06
HALO = 16
TILE = 16
f32 = jnp.float32
bf16 = jnp.bfloat16


def kernel(
    nz, G, T, win, rows, inside,
    tok, g1, g2, vectors, weights,
    out,
    WA, WO, WU, WD, nrm, hid, p1, q1, mid32, mid, act, p2, q2,
    staged, leaving, gathered,
    rz, rd, sz, sd, sy, loc, rn, sn, r1, s1, ra, sa, r2, s2, ro, so,
):
    if inside:
        packed, table, asc, taps, usc, oc, dc = gathered
    else:
        asc, taps, usc, oc, dc = vectors
    D = tok.shape[1]
    pw = D // nz
    cw = pw // 2
    r, f, t = lax.axis_index("rep"), lax.axis_index("fs"), lax.axis_index("tp")
    z, y = f // 2, f % 2
    fy = z * 2 + 1 - y
    g = r * 2 + y
    ka, ko, ku, kd = (w.shape[0] for w in leaving)
    stages = range(5 if inside else 4)
    has_lo, has_hi = z > 0, z < nz - 1
    if T == 2:
        start, off = t * (rows - HALO), t * HALO
    else:
        start = jnp.clip(t * rows - HALO, 0, tok.shape[0] - win)
        off = t * rows - start
    start, off = pl.multiple_of(start, HALO), pl.multiple_of(off, HALO)

    def member(m):
        return (m // 2, z * 2 + m % 2, t)

    def others():
        return [(g + d) % G for d in range(1, G)]

    def siblings():
        return [(t + d) % T for d in range(1, T)]

    def copy(src, dst, ssem, rsem, dev):
        return pltpu.make_async_remote_copy(
            src_ref=src, dst_ref=dst, send_sem=ssem, recv_sem=rsem, device_id=dev, device_id_type=MESH
        )

    def arrived(ref, sem):
        pltpu.make_async_copy(ref, ref, sem).wait()

    def slot(s, ff, tt):
        if s == 0:
            return WA.at[tt, pl.ds(pl.multiple_of(ff * ka, ka), ka)]
        if s == 1:
            return WO.at[ff, pl.ds(pl.multiple_of(tt * ko, ko), ko)]
        if s == 2:
            return WU.at[tt, pl.ds(pl.multiple_of(ff * ku, ku), ku)]
        if s == 3:
            return WD.at[ff, pl.ds(pl.multiple_of(tt * kd, kd), kd)]
        return table.at[ff, tt]

    def to_siblings(s, ff, src):
        for tt in siblings():
            copy(src, slot(s, ff, t), sd.at[s, ff], rd.at[s, ff], (r, f, tt)).start()

    def both_ways(s, ff, src):
        @pl.when(has_lo)
        def _():
            copy(src, slot(s, ff, t), sz.at[s, ff, 0], rz.at[s, ff], (r, f - 2, t)).start()

        @pl.when(has_hi)
        def _():
            copy(src, slot(s, ff, t), sz.at[s, ff, 1], rz.at[s, ff], (r, f + 2, t)).start()

    def fetches():
        for i, w in enumerate(weights):
            src, dst = weights[i], staged[i]
            if w.shape[1] > dst.shape[1]:
                n = dst.shape[1]
                src = src.at[:, pl.ds(pl.multiple_of(r * n, n), n)]
            elif w.shape[0] > dst.shape[0]:
                n = dst.shape[0]
                src = src.at[pl.ds(pl.multiple_of(r * n, n), n)]
            yield pltpu.make_async_copy(src, dst, loc.at[i])

    def round_stage(s):
        parts = {0: (0, 1, 2), 1: (3,), 2: (4,), 3: (5,)}[s]
        high = leaving[s].shape[0]
        for i in parts:
            pltpu.make_async_copy(staged[i], staged[i], loc.at[i]).wait()
        for yy in range(2):

            @pl.when(y == yy)
            def _():
                @pl.loop(0, high // 32)
                def _(k):
                    at = pl.ds(pl.multiple_of(k * 32, 32), 32)
                    for n, i in enumerate(parts):
                        if s in (0, 2):
                            wide = staged[i].shape[1] // 2
                            mine = staged[i][at, yy * wide : (yy + 1) * wide]
                            theirs = staged[i][at, (1 - yy) * wide : (2 - yy) * wide]
                        else:
                            wide = staged[i].shape[1]
                            mine = staged[i][pl.ds(pl.multiple_of(yy * high + k * 32, 32), 32), :]
                            theirs = staged[i][pl.ds(pl.multiple_of((1 - yy) * high + k * 32, 32), 32), :]
                        cols = slice(n * wide, (n + 1) * wide)
                        leaving[s][at, cols] = theirs.astype(bf16)
                        if s == 0:
                            WA[t, pl.ds(pl.multiple_of(f * ka + k * 32, 32), 32), cols] = mine.astype(bf16)
                        elif s == 1:
                            WO[f, pl.ds(pl.multiple_of(t * ko + k * 32, 32), 32), :] = mine.astype(bf16)
                        elif s == 2:
                            WU[t, pl.ds(pl.multiple_of(f * ku + k * 32, 32), 32), :] = mine.astype(bf16)
                        else:
                            WD[f, pl.ds(pl.multiple_of(t * kd + k * 32, 32), 32), :] = mine.astype(bf16)

    def kick(s):
        own = slot(s, f, t)
        copy(leaving[s] if s < 4 else own, own, sy.at[s], rz.at[s, f], (r, fy, t)).start()
        both_ways(s, f, own)
        to_siblings(s, f, own)

    def kick2(s):
        arrived(slot(s, fy, t), rz.at[s, fy])
        both_ways(s, fy, slot(s, fy, t))
        to_siblings(s, fy, slot(s, fy, t))

    def place(j):
        k = (j + 1) // 2
        sg = 1 - 2 * (j % 2)
        return z + sg * k, z - sg

    def step(s, j):
        zs, nxt = place(j)

        @pl.when(jnp.logical_and(zs >= 0, zs < nz))
        def _():
            for yy in range(2):
                ff = 2 * zs + yy
                arrived(slot(s, ff, t), rz.at[s, ff])

                @pl.when(jnp.logical_and(nxt >= 0, nxt < nz))
                def _():
                    copy(
                        slot(s, ff, t), slot(s, ff, t), sz.at[s, ff, 0], rz.at[s, ff], (r, 2 * nxt + y, t)
                    ).start()

                to_siblings(s, ff, slot(s, ff, t))

    def steps(s, lo, hi):
        @pl.loop(lo, hi)
        def _(j):
            step(s, j)

    def from_siblings(s, ff):
        for tt in siblings():
            arrived(slot(s, ff, tt), rd.at[s, ff])

    def all_from_siblings(s):
        @pl.loop(0, 2 * nz)
        def _(ff):
            from_siblings(s, ff)

    last = 2 * nz - 1

    for fetch in fetches():
        fetch.start()
    if inside:
        at_col = 0
        for v in vectors[:3]:
            packed[:, at_col : at_col + v.shape[1]] = v[...]
            at_col += v.shape[1]
        few = vectors[0].shape[1]
        for k in range(3):
            packed[:, at_col : at_col + few] = vectors[6][k : k + 1, pl.ds(pl.multiple_of(f * few, few), few)]
            at_col += few
        for v in vectors[3:6]:
            packed[:, at_col : at_col + v.shape[1]] = v[...]
            at_col += v.shape[1]
        table[f, t] = packed[...]

    barrier = pltpu.get_barrier_semaphore()
    for m in others():
        pl.semaphore_signal(barrier, inc=1, device_id=member(m), device_id_type=MESH)
    for tt in siblings():
        pl.semaphore_signal(barrier, inc=1, device_id=(r, f, tt), device_id_type=MESH)

    @pl.when(has_lo)
    def _():
        pl.semaphore_signal(barrier, inc=1, device_id=(r, f - 2, t), device_id_type=MESH)

    @pl.when(has_hi)
    def _():
        pl.semaphore_signal(barrier, inc=1, device_id=(r, f + 2, t), device_id_type=MESH)

    pl.semaphore_wait(barrier, G + T - 2 + (z + nz - 1) // nz + (2 * nz - 2 - z) // nz)

    round_stage(0)
    round_stage(1)
    kick(0)
    if inside:
        kick(4)
    kick(1)
    round_stage(2)
    round_stage(3)

    @pl.loop(0, win // TILE)
    def _(i):
        at = pl.ds(pl.multiple_of(i * TILE, TILE), TILE)
        x = tok[pl.ds(pl.multiple_of(start + i * TILE, TILE), TILE), :].astype(f32)
        x = x * lax.rsqrt(jnp.mean(x * x, axis=-1, keepdims=True) + norm_eps) * g1[...]
        nrm[g, at, :] = x.astype(bf16)

    kick2(0)
    if inside:
        kick2(4)
    for m in others():
        copy(nrm.at[g], nrm.at[g], sn.at[m], rn.at[g], member(m)).start()
    kick(2)
    kick2(1)
    steps(0, 1, last)
    if inside:
        steps(4, 1, last)
    kick(3)
    kick2(2)
    steps(1, 1, last)

    all_from_siblings(0)
    for m in others():
        arrived(nrm.at[m], rn.at[m])
    if inside:
        all_from_siblings(4)
        few, ups, outs = vectors[0].shape[1], vectors[3].shape[1], vectors[4].shape[1]
        wide = 3 * vectors[0].shape[1] * 2
        near = 2 * nz // G
        for tt in range(T):
            for j in range(near):
                row_of = table[g * near + j, tt]
                for k in range(3):
                    at_col = (k * near + j) * few
                    asc[tt, :, at_col : at_col + few] = row_of[:, k * few : (k + 1) * few]
                    taps[tt, k : k + 1, j * few : (j + 1) * few] = row_of[:, (3 + k) * few : (4 + k) * few]
                usc[tt, :, j * ups : (j + 1) * ups] = row_of[:, wide : wide + ups]
        for zs in range(nz):
            for yy in range(2):
                row_of = table[2 * zs + yy, 0]
                cols = slice(yy * outs, (yy + 1) * outs)
                oc[zs, :, cols] = row_of[:, wide + ups : wide + ups + outs]
                dc[zs, :, cols] = row_of[:, wide + ups + outs :]
    c = taps.shape[2]

    @pl.loop(0, G)
    def _(gs):
        x = nrm[gs]
        row = lax.broadcasted_iota(jnp.int32, (win, c), 0)
        for tt in range(T):
            prod = jnp.dot(x, WA[tt], preferred_element_type=f32) * asc[tt]
            gated = prod[:, c : 2 * c] * prod[:, :c]
            before = jnp.where(row == 0, 0.0, pltpu.roll(gated, 1, 0))
            after = jnp.where(row == win - 1, 0.0, pltpu.roll(gated, win - 1, 0))
            conv = taps[tt, 0:1] * before + taps[tt, 1:2] * gated + taps[tt, 2:3] * after
            hid[gs, :, tt * c : (tt + 1) * c] = (prod[:, 2 * c :] * conv).astype(bf16)

    all_from_siblings(1)

    @pl.loop(0, nz)
    def _(zs):
        @pl.loop(0, G)
        def _(gs):
            h = hid[gs, pl.ds(off, rows), :]
            for yy in range(2):
                p1[gs, zs, :, yy * cw : (yy + 1) * cw] = jnp.dot(
                    h, WO[2 * zs + yy], preferred_element_type=f32
                ).astype(bf16)

    kick2(3)
    for m in others():
        copy(p1.at[m], q1.at[g], s1.at[m], r1.at[g], member(m)).start()
    cut = (2 * last) // 3
    steps(2, 1, cut)

    for m in others():
        arrived(q1.at[m], r1.at[m])

    def total(p, q, zs, at):
        acc = p[g, zs, at, :].astype(f32)
        for m in others():
            acc = acc + q[m, zs, at, :].astype(f32)
        return acc

    @pl.loop(0, rows // TILE)
    def _(i):
        at = pl.ds(pl.multiple_of(i * TILE, TILE), TILE)
        here = pl.ds(pl.multiple_of(t * rows + i * TILE, TILE), TILE)
        ssq = jnp.zeros((TILE, 1), f32)
        for zs in range(nz):
            m = tok[here, zs * pw : (zs + 1) * pw].astype(f32) + total(p1, q1, zs, at) * oc[zs]
            mid32[zs, at, :] = m
            ssq = ssq + jnp.sum(m * m, axis=-1, keepdims=True)
        inv = lax.rsqrt(ssq / D + norm_eps)
        for zs in range(nz):
            cols = slice(zs * pw, (zs + 1) * pw)
            mid[g, at, cols] = (mid32[zs, at, :] * inv * g2[:, cols]).astype(bf16)

    steps(2, cut, cut + 1)
    for m in others():
        copy(mid.at[g], mid.at[g], sa.at[m], ra.at[g], member(m)).start()
    steps(2, cut + 1, last)
    cut2 = (last + 1) // 2
    steps(3, 1, cut2)

    all_from_siblings(2)
    for m in others():
        arrived(mid.at[m], ra.at[m])
    u = usc.shape[2]

    @pl.loop(0, G)
    def _(gs):
        x = mid[gs]
        for tt in range(T):
            upper = jnp.dot(x, WU[tt], preferred_element_type=f32) * usc[tt]
            act[gs, :, tt * u : (tt + 1) * u] = jnp.square(jnp.maximum(upper, 0.0)).astype(bf16)

    def down(j):
        zs, _ = place(j)

        @pl.when(jnp.logical_and(zs >= 0, zs < nz))
        def _():
            for yy in range(2):
                from_siblings(3, 2 * zs + yy)

            @pl.loop(0, G)
            def _(gs):
                x = act[gs]
                for yy in range(2):
                    p2[gs, zs, :, yy * cw : (yy + 1) * cw] = jnp.dot(
                        x, WD[2 * zs + yy], preferred_element_type=f32
                    ).astype(bf16)

            for m in others():
                copy(p2.at[m, zs], q2.at[g, zs], s2.at[m, zs], r2.at[g, zs], member(m)).start()

    @pl.loop(0, last)
    def _(j):
        @pl.when(j >= cut2)
        def _():
            step(3, j)

        down(j)

    @pl.loop(0, nz)
    def _(zs):
        for m in others():
            arrived(q2.at[m, zs], r2.at[m, zs])

    @pl.loop(0, rows // TILE)
    def _(i):
        at = pl.ds(pl.multiple_of(i * TILE, TILE), TILE)
        here = pl.ds(pl.multiple_of(t * rows + i * TILE, TILE), TILE)
        for zs in range(nz):
            out[here, zs * pw : (zs + 1) * pw] = (
                mid32[zs, at, :] + total(p2, q2, zs, at) * dc[zs]
            ).astype(bf16)

    def half(tt):
        return out.at[pl.ds(pl.multiple_of(tt * rows, rows), rows)]

    for tt in siblings():
        copy(half(t), half(t), so.at[tt], ro.at[t], (r, f, tt)).start()

    for s in stages:
        own = slot(s, f, t)
        arrived(own, sy.at[s])

        def gone(ff, k, s=s, own=own):
            arrived(own, sz.at[s, ff, k])

        for ff in (f, fy):
            pl.when(has_lo)(functools.partial(gone, ff, 0))
            pl.when(has_hi)(functools.partial(gone, ff, 1))

        @pl.loop(1, last)
        def _(j):
            zs, nxt = place(j)
            ok = jnp.logical_and(zs >= 0, zs < nz)

            @pl.when(jnp.logical_and(ok, jnp.logical_and(nxt >= 0, nxt < nz)))
            def _():
                for yy in range(2):
                    gone(2 * zs + yy, 0)

        @pl.loop(0, 2 * nz)
        def _(ff):
            for _ in siblings():
                arrived(own, sd.at[s, ff])

    for m in others():
        arrived(nrm.at[m], sn.at[m])
        arrived(p1.at[m], s1.at[m])
        arrived(mid.at[m], sa.at[m])

        @pl.loop(0, nz)
        def _(zs):
            arrived(p2.at[m, zs], s2.at[m, zs])

    for tt in siblings():
        arrived(half(tt), ro.at[tt])
        arrived(half(tt), so.at[tt])


def line_kernel(
    nz, G, T, win, rows, inside,
    tok, g1, g2, vectors, weights,
    out,
    WA, WO, WU, WD, nrm, hid, p, q, mid32, mid, act, fin,
    staged, leaving, gathered, detour,
    rz, rd, re, sz, sd, sy, loc, rn, rb, rh, rt, sn, sh, st, r1, s1, ra, sa, r2, s2, ro, so, fo,
):
    packed, table, asc, taps, usc, oc, dc = gathered
    D = tok.shape[1]
    pw = D // nz
    cw = pw // 2
    r, f, t = lax.axis_index("rep"), lax.axis_index("fs"), lax.axis_index("tp")
    z, y = f // 2, f % 2
    fy = z * 2 + 1 - y
    g = r * 2 + y
    ka, ko, ku, kd = (w.shape[0] for w in leaving)
    outer = jnp.logical_or(z == 0, z == nz - 1)
    inner = jnp.logical_not(outer)
    inward = jnp.where(2 * z < nz, 1, -1)
    across = z + 2 * inward
    if T == 2:
        start, off = t * (rows - HALO), t * HALO
    else:
        start = jnp.clip(t * rows - HALO, 0, tok.shape[0] - win)
        off = t * rows - start
    start, off = pl.multiple_of(start, HALO), pl.multiple_of(off, HALO)

    def member(m):
        return (m // 2, z * 2 + m % 2, t)

    def others():
        return [(g + d) % G for d in range(1, G)]

    gx, gy, gd = (1 - r) * 2 + y, r * 2 + 1 - y, (1 - r) * 2 + 1 - y

    def peers():
        return [gd, gx, gy]

    def siblings():
        return [(t + d) % T for d in range(1, T)]

    def copy(src, dst, ssem, rsem, dev):
        return pltpu.make_async_remote_copy(
            src_ref=src, dst_ref=dst, send_sem=ssem, recv_sem=rsem, device_id=dev, device_id_type=MESH
        )

    def arrived(ref, sem):
        pltpu.make_async_copy(ref, ref, sem).wait()

    def slot(s, ff, tt):
        if s == 0:
            return WA.at[tt, pl.ds(pl.multiple_of(ff * ka, ka), ka)]
        if s == 1:
            return WO.at[ff, pl.ds(pl.multiple_of(tt * ko, ko), ko)]
        if s == 2:
            return WU.at[tt, pl.ds(pl.multiple_of(ff * ku, ku), ku)]
        if s == 3:
            return WD.at[ff, pl.ds(pl.multiple_of(tt * kd, kd), kd)]
        return table.at[ff, tt]

    def to_siblings(s, ff, src):
        for tt in siblings():
            copy(src, slot(s, ff, t), sd.at[s], rd.at[s // 2, ff] if s % 2 else re.at[s // 2], (r, f, tt)).start()

    def send(s, ff, zs):
        block = slot(s, ff, t)
        copy(block, block, sz.at[s], rz.at[s, ff], (r, 2 * zs + y, t)).start()

    def send_in(s, ff):
        send(s, ff, z + inward)

    def send_out(s, ff):
        send(s, ff, z - inward)

    def spread(s, ff):
        send_in(s, ff)

        @pl.when(inner)
        def _():
            send_out(s, ff)

        @pl.when(outer)
        def _():
            send(s, ff, across)

    def fetches():
        for i, w in enumerate(weights):
            src, dst = weights[i], staged[i]
            if w.shape[1] > dst.shape[1]:
                n = dst.shape[1]
                src = src.at[:, pl.ds(pl.multiple_of(r * n, n), n)]
            elif w.shape[0] > dst.shape[0]:
                n = dst.shape[0]
                src = src.at[pl.ds(pl.multiple_of(r * n, n), n)]
            yield pltpu.make_async_copy(src, dst, loc.at[i])

    def round_stage(s):
        parts = {0: (0, 1, 2), 1: (3,), 2: (4,), 3: (5,)}[s]
        high = leaving[s].shape[0]
        for i in parts:
            pltpu.make_async_copy(staged[i], staged[i], loc.at[i]).wait()
        for yy in range(2):

            @pl.when(y == yy)
            def _():
                @pl.loop(0, high // 32)
                def _(k):
                    at = pl.ds(pl.multiple_of(k * 32, 32), 32)
                    for n, i in enumerate(parts):
                        if s in (0, 2):
                            wide = staged[i].shape[1] // 2
                            mine = staged[i][at, yy * wide : (yy + 1) * wide]
                            theirs = staged[i][at, (1 - yy) * wide : (2 - yy) * wide]
                        else:
                            wide = staged[i].shape[1]
                            mine = staged[i][pl.ds(pl.multiple_of(yy * high + k * 32, 32), 32), :]
                            theirs = staged[i][pl.ds(pl.multiple_of((1 - yy) * high + k * 32, 32), 32), :]
                        cols = slice(n * wide, (n + 1) * wide)
                        leaving[s][at, cols] = theirs.astype(bf16)
                        if s == 0:
                            WA[t, pl.ds(pl.multiple_of(f * ka + k * 32, 32), 32), cols] = mine.astype(bf16)
                        elif s == 1:
                            WO[f, pl.ds(pl.multiple_of(t * ko + k * 32, 32), 32), :] = mine.astype(bf16)
                        elif s == 2:
                            WU[t, pl.ds(pl.multiple_of(f * ku + k * 32, 32), 32), :] = mine.astype(bf16)
                        else:
                            WD[f, pl.ds(pl.multiple_of(t * kd + k * 32, 32), 32), :] = mine.astype(bf16)

    def swap(s):
        own = slot(s, f, t)
        copy(leaving[s] if s < 4 else own, own, sy.at[s], rz.at[s, f], (r, fy, t)).start()

    def swapped(s):
        arrived(slot(s, fy, t), rz.at[s, fy])

    def both_to_siblings(s):
        for ff in (f, fy):
            to_siblings(s, ff, slot(s, ff, t))

    def place(j):
        return (z + inward * j + nz) % nz

    blocks = 2 * (nz - 1)

    def block(i):
        return place(1 + i // 2), (y + i) % 2

    def step(s, i):
        zs, yy = block(i)
        ff = 2 * zs + yy
        arrived(slot(s, ff, t), rz.at[s, ff])

        @pl.when(inner & (zs != z - inward))
        def _():
            send_out(s, ff)

        to_siblings(s, ff, slot(s, ff, t))

    def inner_step(s, near, late):
        ff = 2 * place(near) + (y + late) % 2
        arrived(slot(s, ff, t), rz.at[s, ff])
        if s and near < nz - 1:
            send_out(s, ff)
        elif s == 0 and near == nz - 1:
            send_in(0, ff)
        to_siblings(s, ff, slot(s, ff, t))

    def steps(s, lo, hi):
        @pl.loop(lo, hi)
        def _(j):
            step(s, j)

    def from_siblings(s, ff):
        for tt in siblings():
            arrived(slot(s, ff, tt), rd.at[s // 2, ff])

    def part_of(s, tt, n):
        if s == 0:
            return WA.at[tt, pl.ds(0, n * ka)]
        if s == 1:
            return WO.at[pl.ds(0, n), pl.ds(pl.multiple_of(tt * ko, ko), ko)]
        if s == 2:
            return WU.at[tt, pl.ds(0, n * ku)]
        if s == 3:
            return WD.at[pl.ds(0, n), pl.ds(pl.multiple_of(tt * kd, kd), kd)]
        return table.at[pl.ds(0, n), tt]

    def all_from_siblings(s):
        for tt in siblings():
            arrived(part_of(s, tt, 2 * nz), re.at[s // 2])

    for fetch in fetches():
        fetch.start()
    if inside:
        at_col = 0
        for v in vectors[:3]:
            packed[:, at_col : at_col + v.shape[1]] = v[...]
            at_col += v.shape[1]
        few = vectors[0].shape[1]
        for k in range(3):
            packed[:, at_col : at_col + few] = vectors[6][k : k + 1, pl.ds(pl.multiple_of(f * few, few), few)]
            at_col += few
        for v in vectors[3:6]:
            for k in range(v.shape[0]):
                packed[:, at_col : at_col + v.shape[1]] = v[k : k + 1, :]
                at_col += v.shape[1]
        table[f, t] = packed[...]

    barrier = pltpu.get_barrier_semaphore()
    for m in others():
        pl.semaphore_signal(barrier, inc=1, device_id=member(m), device_id_type=MESH)
    for tt in siblings():
        pl.semaphore_signal(barrier, inc=1, device_id=(r, f, tt), device_id_type=MESH)

    for zs in (z - 1, z + 1, across):
        near = jnp.logical_and(zs >= 0, zs < nz)

        @pl.when(jnp.logical_and(near, zs != z))
        def _():
            pl.semaphore_signal(barrier, inc=1, device_id=(r, 2 * zs + y, t), device_id_type=MESH)

    round_stage(0)
    round_stage(1)
    pl.semaphore_wait(barrier, G + T - 2 + jnp.where(outer, 2, 3))
    swap(0)
    send_in(0, f)
    swap(4)
    swap(1)

    @pl.when(inner)
    def _():
        for s in (4, 1):
            spread(s, f)

    round_stage(2)
    round_stage(3)

    @pl.when(inner)
    def _():
        for s in (2, 3):
            send_out(s, f)
        for i in range(2):
            copy(leaving[2 + i], detour[i], st.at[i], rt.at[i], (r, 2 * (z - inward) + y, t)).start()

    @pl.loop(0, win // TILE)
    def _(i):
        at = pl.ds(pl.multiple_of(i * TILE, TILE), TILE)
        x = tok[pl.ds(pl.multiple_of(start + i * TILE, TILE), TILE), :].astype(f32)
        x = x * lax.rsqrt(jnp.mean(x * x, axis=-1, keepdims=True) + norm_eps) * g1[...]
        nrm[g, at, :] = x.astype(bf16)

    low = win // 2 // TILE * TILE

    def rows_of(i, lower):
        return nrm.at[i, pl.ds(0, low)] if lower else nrm.at[i, pl.ds(low, win - low)]

    def offer(base, sem):
        for m in (gx, gy):
            copy(nrm.at[base + g], nrm.at[base + g], sn, sem.at[g], member(m)).start()

    def pass_on(base, sem, from_x):
        m, n = (gx, gy) if from_x else (gy, gx)
        arrived(nrm.at[base + m], sem.at[m])
        some = rows_of(base + m, not from_x)
        copy(some, some, sn, sem.at[m] if from_x else sem.at[G], member(n)).start()

    def passed(base, sem):
        arrived(rows_of(base + gd, False), sem.at[gd])
        arrived(rows_of(base + gd, True), sem.at[G])

    def project(base, gs):
        x = nrm[base + gs]
        row = lax.broadcasted_iota(jnp.int32, (win, c), 0)
        for tt in range(T):
            prod = jnp.dot(x, WA[tt], preferred_element_type=f32) * asc[tt]
            gated = prod[:, c : 2 * c] * prod[:, :c]
            before = jnp.where(row == 0, 0.0, pltpu.roll(gated, 1, 0))
            after = jnp.where(row == win - 1, 0.0, pltpu.roll(gated, win - 1, 0))
            conv = taps[tt, 0:1] * before + taps[tt, 1:2] * gated + taps[tt, 2:3] * after
            hid[base + gs, :, tt * c : (tt + 1) * c] = (prod[:, 2 * c :] * conv).astype(bf16)

    def nth(k):
        return jnp.where(k == 0, g, jnp.where(k == 1, gx, jnp.where(k == 2, gy, gd)))

    def unpack():
        few, ups, outs = vectors[0].shape[1], vectors[3].size, vectors[4].shape[1]
        wide = 3 * vectors[0].shape[1] * 2
        near = 2 * nz // G
        for tt in range(T):
            for j in range(near):
                row_of = table[g * near + j, tt]
                for k in range(3):
                    at_col = (k * near + j) * few
                    asc[tt, :, at_col : at_col + few] = row_of[:, k * few : (k + 1) * few]
                    taps[tt, k : k + 1, j * few : (j + 1) * few] = row_of[:, (3 + k) * few : (4 + k) * few]
                usc[tt, :, j * ups : (j + 1) * ups] = row_of[:, wide : wide + ups]
        for zs in range(nz):
            for yy in range(2):
                row_of = table[2 * zs + yy, 0]
                cols = slice(yy * outs, (yy + 1) * outs)
                oc[zs, :, cols] = row_of[:, wide + ups : wide + ups + outs]
                dc[zs, :, cols] = row_of[:, wide + ups + outs :]
    c = taps.shape[2]

    def hand_over(gs):
        here = pl.ds(off, rows)
        copy(hid.at[G + gs, here], hid.at[gs, here], sh, rh.at[gs], (r, 2 * (z - inward) + y, t)).start()

    def project_far(lo, hi):
        @pl.loop(lo, hi)
        def _(k):
            gs = nth(k)

            @pl.when(k == G - 1)
            def _():
                passed(G, rb)

            project(G, gs)
            hand_over(gs)

    @pl.when(outer)
    def _():
        swap(2)
        swap(3)
        spread(4, f)
        swapped(0)
        send_in(0, fy)
        swapped(4)
        spread(4, fy)
        copy(nrm.at[g], nrm.at[G + g], sn, rb.at[g], (r, 2 * (z + inward) + y, t)).start()
        spread(1, f)
        swapped(1)
        spread(1, fy)
        for s in (4, 1):
            both_to_siblings(s)
        spread(2, f)
        for i in range(2):
            arrived(detour[i], rt.at[i])
            ff = 2 * (z + inward) + y
            copy(detour[i], slot(2 + i, ff, t), st.at[i], rz.at[2 + i, ff], (r, fy, t)).start()
        def give_back(i):
            ff = 2 * (z + inward) + 1 - y
            arrived(slot(2 + i, ff, t), rz.at[2 + i, ff])
            send_in(2 + i, ff)
            to_siblings(2 + i, ff, slot(2 + i, ff, t))

        give_back(0)
        swapped(2)
        spread(2, fy)
        both_to_siblings(2)
        give_back(1)
        swapped(3)
        for ff in (f, fy):
            send(3, ff, across)
            send_in(3, ff)
        both_to_siblings(3)
        steps(4, 0, blocks)
        steps(1, 0, blocks)
        all_from_siblings(4)
        unpack()

    @pl.when(inner)
    def _():
        offer(0, rn)
        swapped(0)
        send_in(0, fy)
        both_to_siblings(0)
        inner_step(0, 3, 0)
        inner_step(0, 1, 0)
        for s in (4, 1):
            swapped(s)
            spread(s, fy)
            both_to_siblings(s)
        pass_on(0, rn, True)
        inner_step(0, 2, 0)
        inner_step(0, 1, 1)
        pass_on(0, rn, False)
        inner_step(0, 3, 1)
        arrived(nrm.at[G + g], rb.at[g])
        offer(G, rb)
        inner_step(0, 2, 1)
        for s in (2, 3):
            send_in(s, f)
        all_from_siblings(0)
        steps(4, 0, blocks)
        all_from_siblings(4)
        unpack()
        steps(1, 0, blocks)
        passed(0, rn)
        @pl.loop(0, G)
        def _(gs):
            project(0, gs)
    @pl.when(inner)
    def _():
        project(G, g)
        pass_on(G, rb, True)
        pass_on(G, rb, False)

    def pair(ref, i, zs):
        return ref.at[i, pl.ds(2 * zs, 2)]

    def legs(zs):
        even = zs % 2 == 0
        return jnp.where(even, gx, gy), jnp.where(even, gy, gx)

    def first_leg(zs):
        first, _ = legs(zs)
        copy(pair(p, gd, zs), pair(q, 1, zs), s1, r1.at[1, zs], member(first)).start()
        copy(pair(p, first, zs), pair(q, 0, zs), s1, r1.at[0, zs], member(first)).start()

    def own_leg(j, k):
        zs = 2 * j + k
        first, _ = legs(zs)
        copy(pair(p, first, zs), pair(q, 0, zs), s1, r1.at[0, zs], member(first)).start()

    def pass_leg(zs):
        first, _ = legs(zs)
        copy(pair(p, gd, zs), pair(q, 1, zs), s1, r1.at[1, zs], member(first)).start()

    pl.when(inner)(lambda: project_far(1, 3))

    @pl.loop(0, 2 * nz)
    def _(ff):
        from_siblings(1, ff)

    @pl.loop(0, G)
    def _(k):
        gs = nth((k + 1) % G)

        @pl.when(outer)
        def _():
            some = hid.at[gs, pl.ds(off, rows)]
            arrived(some, rh.at[gs])

        @pl.loop(0, nz // 2)
        def _(j):
            h = hid[gs, pl.ds(off, rows), :]
            for i in range(4):
                p[gs, 4 * j + i] = jnp.dot(h, WO[4 * j + i], preferred_element_type=f32).astype(bf16)

        @pl.when(outer & (k < 2))
        def _():
            pl.loop(0, nz // 2)(lambda j: own_leg(j, k))

        @pl.when(outer & (k == 2))
        def _():
            pl.loop(0, nz)(pass_leg)

    @pl.when(inner)
    def _():
        pl.loop(0, nz)(pass_leg)
        for k in range(2):
            pl.loop(0, nz // 2)(lambda j: own_leg(j, k))
        project_far(3, G)
        hand_over(g)
        inner_step(2, 1, 0)
        inner_step(2, 2, 0)

    @pl.loop(0, nz)
    def _(j):
        zs = place(j)
        _, second = legs(zs)
        arrived(pair(q, 1, zs), r1.at[1, zs])

        @pl.loop(0, rows // TILE)
        def _(k):
            at = pl.ds(pl.multiple_of(k * TILE, TILE), TILE)
            for yy in range(2):
                both = p[second, 2 * zs + yy, at, :].astype(f32) + q[1, 2 * zs + yy, at, :].astype(f32)
                p[second, 2 * zs + yy, at, :] = both.astype(bf16)

        copy(pair(p, second, zs), pair(q, 2, zs), s1, r1.at[2, zs], member(second)).start()

    @pl.when(inner)
    def _():
        swapped(2)
        send_in(2, fy)
        both_to_siblings(2)
        inner_step(2, 2, 1)

    pl.when(outer)(lambda: steps(2, 0, 1))
    @pl.loop(0, nz)
    def _(zs):
        for i in (0, 2):
            arrived(pair(q, i, zs), r1.at[i, zs])

    @pl.loop(0, rows // TILE)
    def _(i):
        at = pl.ds(pl.multiple_of(i * TILE, TILE), TILE)
        here = pl.ds(pl.multiple_of(t * rows + i * TILE, TILE), TILE)
        ssq = jnp.zeros((TILE, 1), f32)
        for ff in range(2 * nz):
            half = slice(ff % 2 * cw, (ff % 2 + 1) * cw)
            acc = p[g, ff, at, :].astype(f32) + q[0, ff, at, :].astype(f32) + q[2, ff, at, :].astype(f32)
            m = tok[here, ff * cw : (ff + 1) * cw].astype(f32) + acc * oc[ff // 2, :, half]
            mid32[ff // 2, at, half] = m
            ssq = ssq + jnp.sum(m * m, axis=-1, keepdims=True)
        inv = lax.rsqrt(ssq / D + norm_eps)
        for zs in range(nz):
            cols = slice(zs * pw, (zs + 1) * pw)
            mid[g, at, cols] = (mid32[zs, at, :] * inv * g2[:, cols]).astype(bf16)

    part = rows // 2

    def half_of(m, h):
        return mid.at[m, pl.ds(h * part, part)]

    for h in range(2):
        for m, way in ((gx, 1 - h), (gy, h)):
            copy(half_of(g, way), half_of(g, way), sa, ra.at[g, way], member(m)).start()
    @pl.when(outer)
    def _():
        steps(2, 2, 3)
        steps(2, 4, 5)


    @pl.when(inner)
    def _():
        inner_step(2, 1, 1)
        inner_step(3, 1, 0)
        swapped(3)
        send_in(3, fy)
        both_to_siblings(3)

    for m, n, h in ((gx, gy, 1), (gy, gx, 0)):
        arrived(half_of(m, h), ra.at[m, h])
        copy(half_of(m, h), half_of(m, h), sa, ra.at[m, h], member(n)).start()
    @pl.when(outer)
    def _():
        steps(2, 5, 6)
        steps(2, 3, 4)


    @pl.when(inner)
    def _():
        inner_step(2, 3, 0)
        inner_step(2, 3, 1)
        inner_step(3, 1, 1)

    all_from_siblings(2)
    u = usc.shape[2]
    arrived(p.at[pl.ds(0, G - 1)], s1)

    @pl.loop(0, G)
    def _(k):
        gs = nth(k)

        @pl.when((k == 1) | (k == G - 1))
        def _():
            arrived(half_of(gs, 0), ra.at[gs, 0])

        @pl.when(k > 1)
        def _():
            arrived(half_of(gs, 1), ra.at[gs, 1])

        x = mid[gs]
        for tt in range(T):
            upper = jnp.dot(x, WU[tt], preferred_element_type=f32) * usc[tt]
            act[gs, :, tt * u : (tt + 1) * u] = jnp.square(jnp.maximum(upper, 0.0)).astype(bf16)

    @pl.when(inner)
    def _():
        inner_step(3, 2, 0)

    def source(i):
        zs, yy = block(jnp.maximum(i - 2, 0))
        zs, yy = jnp.where(i < 2, z, zs), jnp.where(i < 2, (y + i) % 2, yy)
        return zs, yy, 2 * zs + yy

    def direct(i):
        return outer & (i > 5)

    def second_leg(i):
        _, _, ff = source(i)
        _, second = legs(ff)

        @pl.when(jnp.logical_not(direct(i)))
        def _():
            arrived(q.at[1, ff], r2.at[1, ff])

            @pl.loop(0, rows // TILE)
            def _(k):
                at = pl.ds(pl.multiple_of(k * TILE, TILE), TILE)
                both = p[second, ff, at, :].astype(f32) + q[1, ff, at, :].astype(f32)
                p[second, ff, at, :] = both.astype(bf16)

            copy(p.at[second, ff], q.at[2, ff], s2, r2.at[2, ff], member(second)).start()

    def finish(i):
        zs, yy, ff = source(i)
        wide = pl.ds(pl.multiple_of(yy * cw, cw), cw)
        cols = pl.ds(pl.multiple_of(ff * cw, cw), cw)

        def sum_up(slots):
            for m in slots:
                arrived(q.at[m, ff], r2.at[m, ff])

            @pl.loop(0, rows // TILE)
            def _(k):
                at = pl.ds(pl.multiple_of(k * TILE, TILE), TILE)
                acc = p[g, ff, at, :].astype(f32)
                for m in slots:
                    acc = acc + q[m, ff, at, :].astype(f32)
                fin[ff, at, :] = (mid32[zs, at, wide] + acc * dc[zs, :, wide]).astype(bf16)

        far = direct(i)
        pl.when(far)(lambda: sum_up((0, 1, 2)))
        pl.when(jnp.logical_not(far))(lambda: sum_up((0, 2)))
        mine = out.at[pl.ds(pl.multiple_of(t * rows, rows), rows), cols]
        for tt in siblings():
            copy(fin.at[ff], mine, so, ro, (r, f, tt)).start()
        pltpu.make_async_copy(fin.at[ff], mine, fo).start()

    @pl.loop(0, 2 * nz)
    def _(ff_at):
        _, _, ff = source(ff_at)

        @pl.when(ff_at > 1)
        def _():
            second_leg(ff_at - 2)

        @pl.when(outer & (ff_at > 1) & (ff_at != 3))
        def _():
            step(3, ff_at - 2)

        for at, near, late in ((3, 2, 1), (6, 3, 0), (7, 3, 1)):
            pl.when(inner & (ff_at == at))(functools.partial(inner_step, 3, near, late))

        from_siblings(3, ff)

        first, second = legs(ff)
        far = direct(ff_at)

        @pl.loop(0, G)
        def _(k):
            gs = jnp.where(k == 0, gd, jnp.where(k == 1, first, jnp.where(k == 2, second, g)))
            p[gs, ff] = jnp.dot(act[gs], WD[ff], preferred_element_type=f32).astype(bf16)

            @pl.when(k == 0)
            def _():
                to = member(jnp.where(far, gd, first))
                copy(p.at[gd, ff], q.at[1, ff], s2, r2.at[1, ff], to).start()

            @pl.when(k == 1)
            def _():
                copy(p.at[first, ff], q.at[0, ff], s2, r2.at[0, ff], member(first)).start()

            @pl.when(far & (k == 2))
            def _():
                copy(p.at[second, ff], q.at[2, ff], s2, r2.at[2, ff], member(second)).start()

        @pl.when(ff_at > 5)
        def _():
            finish(ff_at - 6)

    second_leg(2 * nz - 2)
    pl.loop(2, 4)(finish)
    second_leg(2 * nz - 1)
    pl.loop(4, 2 * nz)(finish)

    for s in range(5):
        if s in (2, 3):
            pl.when(outer)(functools.partial(arrived, slot(s, f, t), sy.at[s]))
        else:
            arrived(slot(s, f, t), sy.at[s])
        few_sent, many_sent = {0: (2, 4), 2: (5, 7), 3: (5, 7)}.get(s, (4, 8))

        @pl.when(outer)
        def _():
            arrived(part_of(s, t, few_sent), sz.at[s])

        @pl.when(inner)
        def _():
            arrived(part_of(s, t, many_sent), sz.at[s])

        def gone(s=s):
            for _ in siblings():
                arrived(part_of(s, t, 2 * nz), sd.at[s])

        if s == 0:
            pl.when(inner)(gone)
        else:
            gone()

    @pl.when(outer)
    def _():
        arrived(nrm.at[0], sn)

    @pl.when(inner)
    def _():
        arrived(nrm.at[pl.ds(0, 2 * (G - 1))], sn)
        arrived(hid.at[pl.ds(0, G), pl.ds(0, rows)], sh)

    for i in range(2):
        arrived(detour[i], st.at[i])
    arrived(mid.at[pl.ds(0, G - 1)], sa)
    arrived(p.at[pl.ds(0, G - 1)], s2)
    half = out.at[pl.ds(0, rows)]
    for _ in siblings():
        arrived(half, ro)
        arrived(fin, so)
    pltpu.make_async_copy(fin, fin, fo).wait()


def body(
    R, n_fs, T,
    tokens, mix_gain, value_weight, value_scale, inner_weight, inner_scale, outer_weight, outer_scale,
    conv_taps, out_weight, out_scale, mlp_gain, up_weight, up_scale, down_weight, down_scale,
):
    G, nz = 2 * R, n_fs // 2
    TOK, D = tokens.shape[1:]
    rows = TOK // T
    win = TOK if T == 1 else rows + HALO if T == 2 else rows + 2 * HALO
    r, f = lax.axis_index("rep"), lax.axis_index("fs")
    g = r * 2 + f % 2

    vs, us, os = value_scale.shape[0], up_scale.shape[0], out_scale.shape[0]
    inside = all(n % 128 == 0 for n in (vs, us, os))
    lined = inside and T == 2 and nz == 4 and R == 2
    c, u = conv_taps.shape[1] // G, up_weight.shape[1] // G
    if inside:
        scales = (value_scale, inner_scale, outer_scale, up_scale, out_scale, down_scale)
        wide = 128 if lined else us
        vectors = tuple(v.reshape(-1, wide) if v is up_scale else v[None] for v in scales) + (conv_taps,)
    else:
        tap = lax.dynamic_slice_in_dim(conv_taps, f * vs, vs, axis=1)
        packed = jnp.concatenate(
            [value_scale, inner_scale, outer_scale, tap[0], tap[1], tap[2], up_scale, out_scale, down_scale]
        )
        every = lax.all_gather(packed, ("tp", "fs"), axis=0, tiled=False).reshape(T, n_fs, -1)

        def block(v):
            return lax.dynamic_index_in_dim(v.reshape(T, G, -1), g, axis=1, keepdims=True)

        small = [block(every[:, :, i * vs : (i + 1) * vs]) for i in range(6)]
        asc = jnp.concatenate(small[:3], axis=2)
        taps = jnp.concatenate(small[3:], axis=1)
        usc = block(every[:, :, 6 * vs : 6 * vs + us])
        oc = every[0, :, 6 * vs + us : 6 * vs + us + os].reshape(nz, 1, -1)
        dc = every[0, :, 6 * vs + us + os :].reshape(nz, 1, -1)
        vectors = (asc, taps, usc, oc, dc)
    weights = (value_weight, inner_weight, outer_weight, out_weight, up_weight, down_weight)
    ka, ko, kd = value_weight.shape[0], out_weight.shape[0] // G, down_weight.shape[0] // G
    cw = out_weight.shape[1]
    rounded = [(ka, 3 * c), (ko, cw), (ka, u), (kd, cw)]
    staged = [(ka, 2 * c)] * 3 + [(2 * ko, cw), (ka, 2 * u), (2 * kd, cw)]
    gathered = ()
    if inside:
        L = 6 * vs + us + 2 * os
        small = [(1, L), (n_fs, T, 1, L), (T, 1, 3 * c), (T, 3, c), (T, 1, u), (nz, 1, 2 * cw), (nz, 1, 2 * cw)]
        gathered = tuple(pltpu.VMEM(shape, f32) for shape in small)
    pw = D // nz
    dma = pltpu.SemaphoreType.DMA
    vmem = pl.BlockSpec(memory_space=pltpu.VMEM)
    hbm = pl.BlockSpec(memory_space=pl.ANY)
    held = [
        pltpu.VMEM((T, D, 3 * c), bf16),
        pltpu.VMEM((n_fs, T * ko, cw), bf16),
        pltpu.VMEM((T, D, u), bf16),
        pltpu.VMEM((n_fs, T * kd, cw), bf16),
        pltpu.VMEM((2 * G if lined else G, win, D), bf16),
        pltpu.VMEM((2 * G if lined else G, win, T * ko), bf16),
    ]
    reading = [
        tuple(pltpu.VMEM(shape, f32) for shape in staged),
        tuple(pltpu.VMEM(shape, bf16) for shape in rounded),
        gathered,
    ]
    if lined:
        run = line_kernel
        limit = 65000000
        scratch = [
            *held,
            pltpu.VMEM((G, n_fs, rows, cw), bf16),
            pltpu.VMEM((G - 1, n_fs, rows, cw), bf16),
            pltpu.VMEM((nz, rows, pw), f32),
            pltpu.VMEM((G, rows, D), bf16),
            pltpu.VMEM((G, rows, T * kd), bf16),
            pltpu.VMEM((n_fs, rows, cw), bf16),
            *reading,
            tuple(pltpu.VMEM(shape, bf16) for shape in rounded[2:]),
            dma((5, n_fs)),
            dma((2, n_fs)),
            dma((3,)),
            dma((5,)),
            dma((5,)),
            dma((5,)),
            dma((6,)),
            dma((G + 1,)),
            dma((G + 1,)),
            dma((G,)),
            dma((2,)),
            dma,
            dma,
            dma((2,)),
            dma((G - 1, nz)),
            dma,
            dma((G, 2)),
            dma,
            dma((G - 1, n_fs)),
            dma,
            dma,
            dma,
            dma,
        ]
    else:
        run = kernel
        limit = 65000000
        scratch = [
            *held,
            pltpu.VMEM((G, nz, rows, pw), bf16),
            pltpu.VMEM((G, nz, rows, pw), bf16),
            pltpu.VMEM((nz, rows, pw), f32),
            pltpu.VMEM((G, rows, D), bf16),
            pltpu.VMEM((G, rows, T * kd), bf16),
            pltpu.VMEM((G, nz, rows, pw), bf16),
            pltpu.VMEM((G, nz, rows, pw), bf16),
            *reading,
            dma((5, n_fs)),
            dma((5, n_fs)),
            dma((5, n_fs, 2)),
            dma((5, n_fs)),
            dma((5,)),
            dma((6,)),
            dma((G,)),
            dma((G,)),
            dma((G,)),
            dma((G,)),
            dma((G,)),
            dma((G,)),
            dma((G, nz)),
            dma((G, nz)),
            dma((T,)),
            dma((T,)),
        ]
    result = pl.pallas_call(
        functools.partial(run, nz, G, T, win, rows, inside),
        out_shape=jax.ShapeDtypeStruct((TOK, D), bf16),
        in_specs=[vmem] * 3 + [(vmem,) * len(vectors), (hbm,) * 6],
        out_specs=hbm if lined else vmem,
        scratch_shapes=scratch,
        compiler_params=pltpu.CompilerParams(collective_id=0, has_side_effects=True, vmem_limit_bytes=limit),
    )(tokens[0], mix_gain[None], mlp_gain[None], vectors, weights)
    return result[None]


def solution(mesh):
    placed = (
        P(("rep", "fs"), None, None),
        P(),
        P("fs", "tp"),
        P(("tp", "fs")),
        P("fs", "tp"),
        P(("tp", "fs")),
        P("fs", "tp"),
        P(("tp", "fs")),
        P(None, "tp"),
        P("tp", "fs"),
        P("fs"),
        P(),
        P("fs", "tp"),
        P(("tp", "fs")),
        P("tp", "fs"),
        P("fs"),
    )
    sizes = (mesh.shape["rep"], mesh.shape["fs"], mesh.shape["tp"])
    return jax.shard_map(
        functools.partial(body, *sizes),
        mesh=mesh,
        in_specs=placed,
        out_specs=P(("rep", "fs"), None, None),
        check_vma=False,
    )
```
